128 devices in a mesh: fs: 16 (over z, x), tp: 8 (over y, core).
Axes of the slice: x: 4, y: 4, z: 4, core: 2. Of those that a mesh axis runs over, the one named last changes fastest.
Arguments:
- later_in: bfloat16 [16384, 2048], P('fs'), may hold values from -3 to 3
- earlier_in: bfloat16 [16384, 2048], P('fs'), may hold values from -3 to 3
- cotangent: bfloat16 [16384, 2048], P('fs'), may hold values from -6 to 6
- gate_weight: bfloat16 [2048, 5632], P('fs', 'tp'), may hold values from -0.125 to 0.125
- up_weight: bfloat16 [2048, 5632], P('fs', 'tp'), may hold values from -0.125 to 0.125
- down_weight: bfloat16 [2048, 5632], P('fs', 'tp'), may hold values from -0.078125 to 0.078125
- norm_gain: bfloat16 [2048], replicated, may hold values from 0.099609375 to 1.8984375
- gate_sum: float32 [2048, 5632], P('fs', 'tp'), may hold values from -96 to 96
- up_sum: float32 [2048, 5632], P('fs', 'tp'), may hold values from -96 to 96
- down_sum: float32 [2048, 5632], P('fs', 'tp'), may hold values from -96 to 96
- gain_sum: float32 [2048], replicated, may hold values from -192 to 192
Outputs:
- later_out: bfloat16 [16384, 2048], P(('fs', 'tp'))
- later_hidden: bfloat16 [16384, 5632], P('fs', 'tp')
- earlier_grad: bfloat16 [16384, 2048], P(('fs', 'tp'))
- gate_sum_new: float32 [2048, 5632], P('fs', 'tp')
- up_sum_new: float32 [2048, 5632], P('fs', 'tp')
- down_sum_new: float32 [2048, 5632], P('fs', 'tp')
- gain_sum_new: float32 [2048], replicated
The draws below stay inside these ranges and needn't reach their ends.
All inputs are finite; a program needn't handle non-finite values.
Results may differ from the reference program's by a relative error of at most 0.013.
Values may be sent and summed in bfloat16 or wider, within the bound.
A program may use at most 128 MiB of HBM per device.

```python
import jax
import jax.numpy as jnp
from jax import lax

D = 2048
FF = 5632
TOKENS = 16384
N_TP = 8


def raised(array, stream_key, source, target, blocks, factor):
    owner, partner = [(jnp.arange(array.shape[position]) // (array.shape[position] // blocks)).reshape([-1 if axis == position else 1 for axis in range(array.ndim)]) for position in (source, target)]
    chosen = jax.random.permutation(stream_key, blocks)[partner]
    strong = (owner == chosen) | (owner == (partner + blocks // 2) % blocks)
    return jnp.where(strong, factor * array, array)


def steps_of(own_key, shape, pieces, least, high):
    def one(axis_at, blocks):
        steps = jax.random.uniform(jax.random.fold_in(jax.random.fold_in(own_key, 6), axis_at), (blocks,), jnp.float32, least / len(pieces), high / len(pieces))
        return jnp.repeat(jnp.exp(steps), shape[axis_at] // blocks).reshape((-1,) + (1,) * (len(shape) - axis_at - 1))

    factor_of = one(*pieces[0])
    for cut in pieces[1:]:
        factor_of = factor_of * one(*cut)
    return factor_of


def centred(own_key, extent, spread, bound, cuts=(), dtype=jnp.bfloat16):
    drawn = spread * jax.random.normal(own_key, extent, jnp.float32)
    if cuts:
        drawn = drawn * steps_of(own_key, extent, cuts, -0.22, 0.18)
    return jnp.clip(drawn, -bound, bound).astype(dtype)


def bell_draw_with(stream_key, shape, scale, bound, shards, heavy, kind=jnp.bfloat16):
    array = scale * jax.random.normal(stream_key, shape, jnp.float32)
    if shards:
        array = array * steps_of(stream_key, shape, shards, -0.22, 0.18)
    return jnp.clip(raised(array, jax.random.fold_in(stream_key, 3), *heavy), -bound, bound).astype(kind)


def setup_inputs(seed: int = 0) -> dict:
    streams_of = jax.random.split(jax.random.key(seed), 12)
    return {
        "later_in": centred(streams_of[0], (TOKENS, D), 0.5, 3.0, ((0, 16),)),
        "earlier_in": centred(streams_of[1], (TOKENS, D), 0.5, 3.0, ((0, 16),)),
        "cotangent": bell_draw_with(streams_of[2], (TOKENS, D), 1.0, 6.0, ((0, 16),), (0, 1, 16, 2.0)),
        "gate_weight": centred(streams_of[3], (D, FF), D ** -0.5, 0.125, ((0, 16), (1, 8))),
        "up_weight": centred(streams_of[4], (D, FF), D ** -0.5, 0.125, ((0, 16), (1, 8))),
        "down_weight": centred(streams_of[5], (D, FF), FF ** -0.5, 0.078125, ((0, 16), (1, 8))),
        "norm_gain": jnp.clip(1.0 + 0.18 * jax.random.normal(streams_of[6], (D,), jnp.float32), 0.099609375, 1.8984375).astype(jnp.bfloat16),
        "gate_sum": centred(streams_of[7], (D, FF), 16.0, 96.0, ((0, 16), (1, 8)), jnp.float32),
        "up_sum": centred(streams_of[8], (D, FF), 16.0, 96.0, ((0, 16), (1, 8)), jnp.float32),
        "down_sum": centred(streams_of[9], (D, FF), 16.0, 96.0, ((0, 16), (1, 8)), jnp.float32),
        "gain_sum": centred(streams_of[10], (D,), 32.0, 192.0, (), jnp.float32),
    }


norm_floor = 0.05

def normalize(tokens_in, norm_gain):
    values = tokens_in.astype(jnp.float32)
    row_scale = jax.lax.rsqrt(lax.optimization_barrier(jnp.mean(values * values, axis=1, keepdims=True)) + norm_floor)
    unit_rows = values * row_scale
    normed = (unit_rows * norm_gain.astype(jnp.float32)).astype(jnp.bfloat16)
    return (row_scale, unit_rows, normed)

def rounded(partial_value):
    return jax.lax.optimization_barrier(partial_value.astype(jnp.bfloat16)).astype(jnp.float32)

def reference(later_in, earlier_in, cotangent, gate_weight, up_weight, down_weight, norm_gain, gate_sum, up_sum, down_sum, gain_sum):
    block_width = FF // N_TP
    gain_f = norm_gain.astype(jnp.float32)
    normed_later = normalize(later_in, norm_gain)[2]
    gate_later = jnp.dot(normed_later, gate_weight, preferred_element_type=jnp.float32)
    up_later = jnp.dot(normed_later, up_weight, preferred_element_type=jnp.float32)
    later_hidden = (jax.nn.silu(gate_later) * up_later).astype(jnp.bfloat16)
    branch_total = jnp.zeros(later_in.shape, jnp.float32)
    for block_index in range(N_TP):
        first = block_index * block_width
        partial_value = jnp.dot(later_hidden[:, first:first + block_width], down_weight[:, first:first + block_width].T, preferred_element_type=jnp.float32)
        branch_total = branch_total + rounded(partial_value)
    later_out = (later_in.astype(jnp.float32) + 0.5 * branch_total).astype(jnp.bfloat16)
    row_scale, unit_rows, normed = normalize(earlier_in, norm_gain)
    gate_pre = jnp.dot(normed, gate_weight, preferred_element_type=jnp.float32)
    up_pre = jnp.dot(normed, up_weight, preferred_element_type=jnp.float32)
    sigmoid_gate = jax.nn.sigmoid(gate_pre)
    activated = gate_pre * sigmoid_gate
    hidden_earlier = (activated * up_pre).astype(jnp.bfloat16)
    dhidden = jnp.dot(cotangent, down_weight, preferred_element_type=jnp.float32)
    dgate = (0.5 * dhidden * up_pre * sigmoid_gate * (1.0 + gate_pre * (1.0 - sigmoid_gate))).astype(jnp.bfloat16)
    dupper = (0.5 * dhidden * activated).astype(jnp.bfloat16)
    grad_total = jnp.zeros(earlier_in.shape, jnp.float32)
    dnormed_total = jnp.zeros(earlier_in.shape, jnp.float32)
    for block_index in range(N_TP):
        first = block_index * block_width
        dnormed_part = jnp.dot(dgate[:, first:first + block_width], gate_weight[:, first:first + block_width].T, preferred_element_type=jnp.float32) + jnp.dot(dupper[:, first:first + block_width], up_weight[:, first:first + block_width].T, preferred_element_type=jnp.float32)
        dnormed_total = dnormed_total + dnormed_part
        weighted = dnormed_part * gain_f
        branch_part = row_scale * (weighted - unit_rows * lax.optimization_barrier(jnp.mean(weighted * unit_rows, axis=1, keepdims=True)))
        grad_total = grad_total + rounded(branch_part)
    earlier_grad = (cotangent.astype(jnp.float32) + grad_total).astype(jnp.bfloat16)
    gate_sum_new = gate_sum + jnp.dot(normed.T, dgate, preferred_element_type=jnp.float32)
    up_sum_new = up_sum + jnp.dot(normed.T, dupper, preferred_element_type=jnp.float32)
    down_sum_new = down_sum + 0.5 * jnp.dot(cotangent.T, hidden_earlier, preferred_element_type=jnp.float32)
    gain_sum_new = gain_sum + lax.optimization_barrier(jnp.sum(dnormed_total * unit_rows, axis=0))
    return (later_out, later_hidden, earlier_grad, gate_sum_new, up_sum_new, down_sum_new, gain_sum_new)
```

```python
import functools

import jax
import jax.numpy as jnp
from jax import lax
from jax.experimental import pallas as pl
from jax.experimental.pallas import tpu as pltpu
from jax.sharding import Mesh
from jax.sharding import PartitionSpec as P

FS = ("z", "x")
TP = ("y", "c")
ALL = ("z", "x", "y", "c")
MESH = pl.DeviceIdType.MESH
BF = jnp.bfloat16
F32 = jnp.float32
CHUNK = 256
N_CHUNK = 3
WIDE = 3 * CHUNK
SHARD = 128
NORM_FLOOR = 0.05


def pack(w):
    rows, cols = w.shape
    w = jnp.pad(w, ((0, 0), (0, N_CHUNK * CHUNK - cols)))
    return w.reshape(rows, N_CHUNK, CHUNK).transpose(1, 0, 2)


class Gather:
    def __init__(self, w, send, recv):
        self.w, self.send, self.recv = w, send, recv
        self.mz, self.mx = lax.axis_index("z"), lax.axis_index("x")

    def owner(self, h, jf, js):
        dx, dz = (jf, js) if h == 0 else (js, jf)
        return lax.rem(self.mz + dz + 4, 4) * 4 + lax.rem(self.mx + dx + 4, 4)

    def copy(self, c, h, msg, jf, js, sub, axis, d):
        start = self.owner(h, jf, js) * SHARD + h * (SHARD // 2)
        size = SHARD // 2
        if sub is not None:
            size = SHARD // 4
            start = start + sub * size
        view = self.w.at[c, pl.ds(pl.multiple_of(start, 32), size), :]
        name = ("x", "z")[h] if axis == "f" else ("z", "x")[h]
        me = self.mx if name == "x" else self.mz
        return pltpu.make_async_remote_copy(
            src_ref=view,
            dst_ref=view,
            send_sem=self.send.at[c, h, msg],
            recv_sem=self.recv.at[c, h, msg],
            device_id={name: lax.rem(me + d + 4, 4)},
            device_id_type=MESH,
        )

    def m1(self, c, h, d):
        return self.copy(c, h, 0 if d > 0 else 1, 0, 0, None, "f", d)

    def r1(self, c, h, d):
        return self.copy(c, h, 0 if d > 0 else 1, -d, 0, None, "f", d)

    def m2(self, c, h, d):
        return self.copy(c, h, 2 if d > 0 else 3, -d, 0, 0 if d > 0 else 1, "f", d)

    def r2(self, c, h, d):
        return self.copy(c, h, 2 if d > 0 else 3, -2 * d, 0, 0 if d > 0 else 1, "f", d)

    def m3(self, c, h, j, d):
        return self.copy(c, h, 4 + 2 * (j % 4) + (0 if d > 0 else 1), j, 0, None, "s", d)

    def r3(self, c, h, j, d):
        return self.copy(c, h, 4 + 2 * (j % 4) + (0 if d > 0 else 1), j, -d, None, "s", d)

    def m4(self, c, h, j, d):
        return self.copy(c, h, 12 + 2 * (j % 4) + (0 if d > 0 else 1), j, -d, 0 if d > 0 else 1, "s", d)

    def r4(self, c, h, j, d):
        return self.copy(c, h, 12 + 2 * (j % 4) + (0 if d > 0 else 1), j, -2 * d, 0 if d > 0 else 1, "s", d)

    def t0(self, c):
        for h in (0, 1):
            for d in (1, -1):
                self.m1(c, h, d).start()
        for h in (0, 1):
            for d in (1, -1):
                self.m3(c, h, 0, d).start()

    def t1(self, c):
        for d in (1, -1):
            for h in (0, 1):
                self.r1(c, h, d).wait_recv()
                self.m2(c, h, d).start()
                for e in (1, -1):
                    self.m3(c, h, -d, e).start()

    def pass_on(self, c, js):
        for j in js:
            for d in (1, -1):
                for h in (0, 1):
                    self.r3(c, h, j, d).wait_recv()
                    self.m4(c, h, j, d).start()

    def t2(self, c):
        self.pass_on(c, (0,))

    def t3(self, c):
        for h in (0, 1):
            for d in (1, -1):
                self.r2(c, h, d).wait_recv()
            for e in (1, -1):
                self.m3(c, h, 2, e).start()

    def t4(self, c):
        self.pass_on(c, (-1, 1))

    def t5(self, c):
        self.pass_on(c, (2,))

    def t6(self, c):
        for h in (0, 1):
            for j in (0, -1, 1, 2):
                for d in (1, -1):
                    self.r4(c, h, j, d).wait_recv()

    def drain(self, c):
        for h in (0, 1):
            for d in (1, -1):
                self.m1(c, h, d).wait_send()
                self.m2(c, h, d).wait_send()
                for j in (0, -1, 1, 2):
                    self.m3(c, h, j, d).wait_send()
                    self.m4(c, h, j, d).wait_send()


def greet(peers):
    barrier = pltpu.get_barrier_semaphore()
    for peer in peers:
        pl.semaphore_signal(barrier, inc=1, device_id=peer, device_id_type=MESH)
    pl.semaphore_wait(barrier, len(peers))


def ring_peers(names):
    peers = []
    for name in names:
        me = lax.axis_index(name)
        for d in (1, 3):
            peers.append({name: lax.rem(me + d, 4)})
    return peers


def nn(a, b):
    return jnp.dot(a, b, preferred_element_type=F32)


def k1_body(
    later_in, earlier_in, cot_in, gain, w_own,
    w_out, hl_out, dg_out, du_out, g_out,
    w, nl, ne, net, cot, cott, hl, dg, du, he, g,
    in_sem, own_sem, send, recv, out_sem,
):
    tokens, width = nl.shape
    ins = [
        pltpu.make_async_copy(later_in, nl, in_sem.at[0]),
        pltpu.make_async_copy(earlier_in, ne, in_sem.at[1]),
        pltpu.make_async_copy(cot_in, cot, in_sem.at[2]),
    ]
    me = lax.axis_index("z") * 4 + lax.axis_index("x")
    own = [
        pltpu.make_async_copy(
            w_own.at[c], w.at[c, pl.ds(pl.multiple_of(me * SHARD, SHARD), SHARD), :], own_sem.at[c]
        )
        for c in range(N_CHUNK)
    ]
    for copy in own:
        copy.start()
    for copy in ins:
        copy.start()
    greet(ring_peers(("x", "z")))
    for copy in own:
        copy.wait()
    ring = Gather(w, send, recv)
    ring.t0(0)

    gain_row = gain[...].astype(F32)

    def norm_block(ref, i, turned):
        rows = pl.ds(pl.multiple_of(i * 128, 128), 128)
        v = ref[rows, :].astype(F32)
        unit = v * lax.rsqrt(jnp.mean(v * v, axis=1, keepdims=True) + NORM_FLOOR)
        normed = (unit * gain_row).astype(BF)
        ref[rows, :] = normed
        if turned is not None:
            turned[:, rows] = normed.T

    blocks = tokens // 128

    ins[0].wait()

    @pl.loop(0, blocks)
    def _(i):
        norm_block(nl, i, None)

    ring.t1(0)
    ins[1].wait()

    @pl.loop(0, blocks // 2)
    def _(i):
        norm_block(ne, i, net)

    ring.t2(0)

    @pl.loop(blocks // 2, blocks)
    def _(i):
        norm_block(ne, i, net)

    ring.t3(0)
    ring.t0(1)
    ins[2].wait()

    def turn_block(i):
        rows = pl.ds(pl.multiple_of(i * 128, 128), 128)
        cott[:, rows] = cot[rows, :].T

    @pl.loop(0, blocks // 2)
    def _(i):
        turn_block(i)

    ring.t4(0)
    ring.t1(1)

    @pl.loop(blocks // 2, blocks)
    def _(i):
        turn_block(i)

    ring.t5(0)
    ring.t2(1)
    ring.t6(0)

    tb = 256

    def later_item(c, i):
        rows = pl.ds(i * tb, tb)
        pre = nn(nl[rows, :], w[c, :, : 2 * CHUNK])
        gate, up = pre[:, :CHUNK], pre[:, CHUNK:]
        hl[c, rows, :] = (gate * jax.nn.sigmoid(gate) * up).astype(BF)

    def earlier_item(c, i):
        rows = pl.ds(i * tb, tb)
        pre = nn(ne[rows, :], w[c, :, : 2 * CHUNK])
        dh = 0.5 * nn(cot[rows, :], w[c, :, 2 * CHUNK :])
        gate, up = pre[:, :CHUNK], pre[:, CHUNK:]
        s = jax.nn.sigmoid(gate)
        act = gate * s
        he[rows, :] = (act * up).astype(BF)
        dg[c, rows, :] = (dh * up * s * (1.0 + gate * (1.0 - s))).astype(BF)
        du[c, rows, :] = (dh * act).astype(BF)

    def grad_item(c, i):
        rows = pl.ds(i * 512, 512)
        g[c, rows, :CHUNK] = nn(net[rows, :], dg[c]).astype(BF)
        g[c, rows, CHUNK : 2 * CHUNK] = nn(net[rows, :], du[c]).astype(BF)
        g[c, rows, 2 * CHUNK :] = (0.5 * nn(cott[rows, :], he[...])).astype(BF)

    @pl.loop(0, N_CHUNK)
    def _(c):
        ahead = [ring.t3, None, ring.t4, None, ring.t5, None, ring.t6]
        behind = [None, ring.t0, None, ring.t1, None, ring.t2, None]
        items = [functools.partial(earlier_item, c, i) for i in range(tokens // tb)]
        items += [functools.partial(later_item, c, i) for i in range(tokens // tb)]
        items += [functools.partial(grad_item, c, i) for i in range(width // 512)]
        slots = [1, 2, 4, 5, 7, 8, 11]
        for n, item in enumerate(items):
            item()
            if n in slots:
                k = slots.index(n)
                if ahead[k] is not None:

                    @pl.when(c < N_CHUNK - 1)
                    def _():
                        ahead[k](c + 1)

                else:

                    @pl.when(c < N_CHUNK - 2)
                    def _():
                        behind[k](c + 2)

    outs = [
        pltpu.make_async_copy(a, b, out_sem.at[i])
        for i, (a, b) in enumerate([(w, w_out), (hl, hl_out), (dg, dg_out), (du, du_out), (g, g_out)])
    ]
    for copy in outs:
        copy.start()
    for c in range(N_CHUNK):
        ring.drain(c)
    for copy in outs:
        copy.wait()


def k1(later_in, earlier_in, cot, gain, w_own):
    tokens, width = later_in.shape
    any_ = pl.BlockSpec(memory_space=pl.ANY)
    vm = pl.BlockSpec(memory_space=pltpu.VMEM)
    act = (N_CHUNK, tokens, CHUNK)
    full = (N_CHUNK, width, WIDE)
    return pl.pallas_call(
        k1_body,
        out_shape=[jax.ShapeDtypeStruct(s, BF) for s in (full, act, act, act, full)],
        in_specs=[any_, any_, any_, vm, any_],
        out_specs=[any_] * 5,
        scratch_shapes=[
            pltpu.VMEM(full, BF),
            pltpu.VMEM((tokens, width), BF),
            pltpu.VMEM((tokens, width), BF),
            pltpu.VMEM((width, tokens), BF),
            pltpu.VMEM((tokens, width), BF),
            pltpu.VMEM((width, tokens), BF),
            pltpu.VMEM(act, BF),
            pltpu.VMEM(act, BF),
            pltpu.VMEM(act, BF),
            pltpu.VMEM((tokens, CHUNK), BF),
            pltpu.VMEM(full, BF),
            pltpu.SemaphoreType.DMA((3,)),
            pltpu.SemaphoreType.DMA((N_CHUNK,)),
            pltpu.SemaphoreType.DMA((N_CHUNK, 2, 20)),
            pltpu.SemaphoreType.DMA((N_CHUNK, 2, 20)),
            pltpu.SemaphoreType.DMA((5,)),
        ],
        compiler_params=pltpu.CompilerParams(
            collective_id=0, has_side_effects=True, vmem_limit_bytes=64 * 1024 * 1024 - 65536
        ),
        name="gather_compute",
    )(later_in, earlier_in, cot, gain.reshape(1, width), w_own)


def unit_of(tokens_in):
    v = tokens_in.astype(F32)
    scale = lax.rsqrt(jnp.mean(v * v, axis=1, keepdims=True) + NORM_FLOOR)
    return scale, v * scale


def sum_at_owner(array, axis):
    n = lax.axis_size(axis)
    parts = array.reshape(n, array.shape[0] // n, *array.shape[1:])
    arrived = lax.all_to_all(parts, axis, split_axis=0, concat_axis=0, tiled=True)
    return arrived.astype(F32).sum(axis=0)


def local(later_in, earlier_in, cot, gate_w, up_w, down_w, gain, gate_sum, up_sum, down_sum, gain_sum):
    cols = gate_w.shape[1]
    w_own = jnp.concatenate([pack(gate_w), pack(up_w), pack(down_w)], axis=2)
    w, hl, dg, du, g = k1(later_in, earlier_in, cot, gain, w_own)
    hidden = hl.transpose(1, 0, 2).reshape(hl.shape[1], -1)
    nt = lambda a, b: lax.dot_general(a, b, (((0, 2), (0, 2)), ((), ())), preferred_element_type=F32)
    own = later_in.shape[0] // 8
    at = lax.axis_index(TP) * own
    rows = lambda a: lax.dynamic_slice_in_dim(a, at, own, 0).astype(F32)
    later_sum = lax.psum_scatter(
        nt(hl, w[:, :, 2 * CHUNK :]).astype(BF), TP, scatter_dimension=0, tiled=True
    ).astype(F32)
    later_out = (rows(later_in) + 0.5 * later_sum).astype(BF)
    gs = lax.psum_scatter(g, FS, scatter_dimension=1, tiled=True).astype(F32)
    dn = nt(dg, w[:, :, :CHUNK]) + nt(du, w[:, :, CHUNK : 2 * CHUNK])
    scale, unit = unit_of(earlier_in)
    gain_part = jnp.sum(dn * unit, axis=0)
    weighted = dn * gain.astype(F32)
    branch = scale * (weighted - unit * jnp.mean(weighted * unit, axis=1, keepdims=True))
    earlier_grad = (rows(cot) + sum_at_owner(branch.astype(BF), TP)).astype(BF)
    gain_new = gain_sum + lax.psum(gain_part, ALL)
    gs = gs.transpose(1, 0, 2).reshape(gs.shape[1], N_CHUNK, 3, CHUNK)
    pick = lambda k: gs[:, :, k, :].reshape(gs.shape[0], -1)[:, :cols]
    return (
        later_out, hidden[:, :cols], earlier_grad,
        gate_sum + pick(0), up_sum + pick(1), down_sum + pick(2), gain_new,
    )


def solution(mesh):
    torus = Mesh(mesh.devices.reshape(4, 4, 4, 2), ALL)
    return jax.shard_map(
        local,
        mesh=torus,
        in_specs=(P(FS, None),) * 3 + (P(FS, TP),) * 3 + (P(),) + (P(FS, TP),) * 3 + (P(),),
        out_specs=(P(ALL, None), P(FS, TP), P(ALL, None), P(FS, TP), P(FS, TP), P(FS, TP), P()),
        check_vma=False,
    )
```

```python
import functools

import jax
import jax.numpy as jnp
from jax import lax
from jax.experimental import pallas as pl
from jax.experimental.pallas import tpu as pltpu
from jax.sharding import Mesh
from jax.sharding import PartitionSpec as P

FS = ("z", "x")
TP = ("y", "c")
ALL = ("z", "x", "y", "c")
MESH = pl.DeviceIdType.MESH
BF = jnp.bfloat16
F32 = jnp.float32
CHUNK = 256
N_CHUNK = 3
WIDE = 3 * CHUNK
SHARD = 128
NORM_FLOOR = 0.05


def pack(w):
    rows, cols = w.shape
    w = jnp.pad(w, ((0, 0), (0, N_CHUNK * CHUNK - cols)))
    return w.reshape(rows, N_CHUNK, CHUNK).transpose(1, 0, 2)


class Gather:
    def __init__(self, w, send, recv):
        self.w, self.send, self.recv = w, send, recv
        self.mz, self.mx = lax.axis_index("z"), lax.axis_index("x")

    def owner(self, h, jf, js):
        dx, dz = (jf, js) if h == 0 else (js, jf)
        return lax.rem(self.mz + dz + 4, 4) * 4 + lax.rem(self.mx + dx + 4, 4)

    def copy(self, c, h, msg, jf, js, sub, axis, d):
        start = self.owner(h, jf, js) * SHARD + h * (SHARD // 2)
        size = SHARD // 2
        if sub is not None:
            size = SHARD // 4
            start = start + sub * size
        view = self.w.at[c, pl.ds(pl.multiple_of(start, 32), size), :]
        name = ("x", "z")[h] if axis == "f" else ("z", "x")[h]
        me = self.mx if name == "x" else self.mz
        return pltpu.make_async_remote_copy(
            src_ref=view,
            dst_ref=view,
            send_sem=self.send.at[c, h, msg],
            recv_sem=self.recv.at[c, h, msg],
            device_id={name: lax.rem(me + d + 4, 4)},
            device_id_type=MESH,
        )

    def m1(self, c, h, d):
        return self.copy(c, h, 0 if d > 0 else 1, 0, 0, None, "f", d)

    def r1(self, c, h, d):
        return self.copy(c, h, 0 if d > 0 else 1, -d, 0, None, "f", d)

    def m2(self, c, h, d):
        return self.copy(c, h, 2 if d > 0 else 3, -d, 0, 0 if d > 0 else 1, "f", d)

    def r2(self, c, h, d):
        return self.copy(c, h, 2 if d > 0 else 3, -2 * d, 0, 0 if d > 0 else 1, "f", d)

    def m3(self, c, h, j, d):
        return self.copy(c, h, 4 + 2 * (j % 4) + (0 if d > 0 else 1), j, 0, None, "s", d)

    def r3(self, c, h, j, d):
        return self.copy(c, h, 4 + 2 * (j % 4) + (0 if d > 0 else 1), j, -d, None, "s", d)

    def m4(self, c, h, j, d):
        return self.copy(c, h, 12 + 2 * (j % 4) + (0 if d > 0 else 1), j, -d, 0 if d > 0 else 1, "s", d)

    def r4(self, c, h, j, d):
        return self.copy(c, h, 12 + 2 * (j % 4) + (0 if d > 0 else 1), j, -2 * d, 0 if d > 0 else 1, "s", d)

    def t0(self, c):
        for h in (0, 1):
            for d in (1, -1):
                self.m1(c, h, d).start()
        for h in (0, 1):
            for d in (1, -1):
                self.m3(c, h, 0, d).start()

    def t1(self, c):
        for d in (1, -1):
            for h in (0, 1):
                self.r1(c, h, d).wait_recv()
                self.m2(c, h, d).start()
                for e in (1, -1):
                    self.m3(c, h, -d, e).start()

    def pass_on(self, c, js):
        for j in js:
            for d in (1, -1):
                for h in (0, 1):
                    self.r3(c, h, j, d).wait_recv()
                    self.m4(c, h, j, d).start()

    def t2(self, c):
        self.pass_on(c, (0,))

    def t3(self, c):
        for h in (0, 1):
            for d in (1, -1):
                self.r2(c, h, d).wait_recv()
            for e in (1, -1):
                self.m3(c, h, 2, e).start()

    def t4(self, c):
        self.pass_on(c, (-1, 1))

    def t5(self, c):
        self.pass_on(c, (2,))

    def t6(self, c):
        for h in (0, 1):
            for j in (0, -1, 1, 2):
                for d in (1, -1):
                    self.r4(c, h, j, d).wait_recv()

    def drain(self, c):
        for h in (0, 1):
            for d in (1, -1):
                self.m1(c, h, d).wait_send()
                self.m2(c, h, d).wait_send()
                for j in (0, -1, 1, 2):
                    self.m3(c, h, j, d).wait_send()
                    self.m4(c, h, j, d).wait_send()


def greet(peers):
    barrier = pltpu.get_barrier_semaphore()
    for peer in peers:
        pl.semaphore_signal(barrier, inc=1, device_id=peer, device_id_type=MESH)
    pl.semaphore_wait(barrier, len(peers))


def ring_peers(names):
    peers = []
    for name in names:
        me = lax.axis_index(name)
        for d in (1, 3):
            peers.append({name: lax.rem(me + d, 4)})
    return peers


def nn(a, b):
    return jnp.dot(a, b, preferred_element_type=F32)


def k1_body(
    later_in, earlier_in, cot_in, gain, w_own,
    w_out, hl_out, dg_out, du_out, g_out,
    w, nl, ne, net, cot, cott, hl, dg, du, he, g,
    in_sem, own_sem, send, recv, out_sem,
):
    tokens, width = nl.shape
    ins = [
        pltpu.make_async_copy(later_in, nl, in_sem.at[0]),
        pltpu.make_async_copy(earlier_in, ne, in_sem.at[1]),
        pltpu.make_async_copy(cot_in, cot, in_sem.at[2]),
    ]
    me = lax.axis_index("z") * 4 + lax.axis_index("x")
    own = [
        pltpu.make_async_copy(
            w_own.at[c], w.at[c, pl.ds(pl.multiple_of(me * SHARD, SHARD), SHARD), :], own_sem.at[c]
        )
        for c in range(N_CHUNK)
    ]
    for copy in own:
        copy.start()
    for copy in ins:
        copy.start()
    greet(ring_peers(("x", "z")))
    for copy in own:
        copy.wait()
    ring = Gather(w, send, recv)
    ring.t0(0)

    gain_row = gain[...].astype(F32)

    def norm_block(ref, i, turned):
        rows = pl.ds(pl.multiple_of(i * 128, 128), 128)
        v = ref[rows, :].astype(F32)
        unit = v * lax.rsqrt(jnp.mean(v * v, axis=1, keepdims=True) + NORM_FLOOR)
        normed = (unit * gain_row).astype(BF)
        ref[rows, :] = normed
        if turned is not None:
            turned[:, rows] = normed.T

    blocks = tokens // 128

    ins[0].wait()

    @pl.loop(0, blocks)
    def _(i):
        norm_block(nl, i, None)

    ring.t1(0)
    ins[1].wait()

    @pl.loop(0, blocks // 2)
    def _(i):
        norm_block(ne, i, net)

    ring.t2(0)

    @pl.loop(blocks // 2, blocks)
    def _(i):
        norm_block(ne, i, net)

    ring.t3(0)
    ring.t0(1)
    ins[2].wait()

    def turn_block(i):
        rows = pl.ds(pl.multiple_of(i * 128, 128), 128)
        cott[:, rows] = cot[rows, :].T

    @pl.loop(0, blocks // 2)
    def _(i):
        turn_block(i)

    ring.t4(0)
    ring.t1(1)

    @pl.loop(blocks // 2, blocks)
    def _(i):
        turn_block(i)

    ring.t5(0)
    ring.t2(1)
    ring.t6(0)

    tb = 256

    def later_item(c, i):
        rows = pl.ds(i * tb, tb)
        pre = nn(nl[rows, :], w[c, :, : 2 * CHUNK])
        gate, up = pre[:, :CHUNK], pre[:, CHUNK:]
        hl[c, rows, :] = (gate * jax.nn.sigmoid(gate) * up).astype(BF)

    def earlier_item(c, i):
        rows = pl.ds(i * tb, tb)
        pre = nn(ne[rows, :], w[c, :, : 2 * CHUNK])
        dh = 0.5 * nn(cot[rows, :], w[c, :, 2 * CHUNK :])
        gate, up = pre[:, :CHUNK], pre[:, CHUNK:]
        s = jax.nn.sigmoid(gate)
        act = gate * s
        he[rows, :] = (act * up).astype(BF)
        dg[c, rows, :] = (dh * up * s * (1.0 + gate * (1.0 - s))).astype(BF)
        du[c, rows, :] = (dh * act).astype(BF)

    def grad_item(c, i):
        rows = pl.ds(i * 512, 512)
        g[c, rows, :CHUNK] = nn(net[rows, :], dg[c]).astype(BF)
        g[c, rows, CHUNK : 2 * CHUNK] = nn(net[rows, :], du[c]).astype(BF)
        g[c, rows, 2 * CHUNK :] = (0.5 * nn(cott[rows, :], he[...])).astype(BF)

    @pl.loop(0, N_CHUNK)
    def _(c):
        ahead = [ring.t3, None, ring.t4, None, ring.t5, None, ring.t6]
        behind = [None, ring.t0, None, ring.t1, None, ring.t2, None]
        items = [functools.partial(earlier_item, c, i) for i in range(tokens // tb)]
        items += [functools.partial(later_item, c, i) for i in range(tokens // tb)]
        items += [functools.partial(grad_item, c, i) for i in range(width // 512)]
        slots = [1, 2, 4, 5, 7, 8, 11]
        for n, item in enumerate(items):
            item()
            if n in slots:
                k = slots.index(n)
                if ahead[k] is not None:

                    @pl.when(c < N_CHUNK - 1)
                    def _():
                        ahead[k](c + 1)

                else:

                    @pl.when(c < N_CHUNK - 2)
                    def _():
                        behind[k](c + 2)

    outs = [
        pltpu.make_async_copy(a, b, out_sem.at[i])
        for i, (a, b) in enumerate([(w, w_out), (hl, hl_out), (dg, dg_out), (du, du_out), (g, g_out)])
    ]
    for copy in outs:
        copy.start()
    for c in range(N_CHUNK):
        ring.drain(c)
    for copy in outs:
        copy.wait()


def k1(later_in, earlier_in, cot, gain, w_own):
    tokens, width = later_in.shape
    any_ = pl.BlockSpec(memory_space=pl.ANY)
    vm = pl.BlockSpec(memory_space=pltpu.VMEM)
    act = (N_CHUNK, tokens, CHUNK)
    full = (N_CHUNK, width, WIDE)
    return pl.pallas_call(
        k1_body,
        out_shape=[jax.ShapeDtypeStruct(s, BF) for s in (full, act, act, act, full)],
        in_specs=[any_, any_, any_, vm, any_],
        out_specs=[any_] * 5,
        scratch_shapes=[
            pltpu.VMEM(full, BF),
            pltpu.VMEM((tokens, width), BF),
            pltpu.VMEM((tokens, width), BF),
            pltpu.VMEM((width, tokens), BF),
            pltpu.VMEM((tokens, width), BF),
            pltpu.VMEM((width, tokens), BF),
            pltpu.VMEM(act, BF),
            pltpu.VMEM(act, BF),
            pltpu.VMEM(act, BF),
            pltpu.VMEM((tokens, CHUNK), BF),
            pltpu.VMEM(full, BF),
            pltpu.SemaphoreType.DMA((3,)),
            pltpu.SemaphoreType.DMA((N_CHUNK,)),
            pltpu.SemaphoreType.DMA((N_CHUNK, 2, 20)),
            pltpu.SemaphoreType.DMA((N_CHUNK, 2, 20)),
            pltpu.SemaphoreType.DMA((5,)),
        ],
        compiler_params=pltpu.CompilerParams(
            collective_id=0, has_side_effects=True, vmem_limit_bytes=64 * 1024 * 1024 - 65536
        ),
        name="gather_compute",
    )(later_in, earlier_in, cot, gain.reshape(1, width), w_own)


class Scatter:
    def __init__(self, g, r1, r2, r3, r4, send, recv, out):
        self.g, self.r = g, (r1, r2, r3, r4)
        self.send, self.recv, self.out = send, recv, out
        self.at = {"z": lax.axis_index("z"), "x": lax.axis_index("x")}

    def unit(self, c, h, jf, js=None, sub=None):
        r0, n = h * 64, 64
        if sub is not None:
            r0, n = r0 + sub * 32, 32
        fast, slow = (("x", "z"), ("z", "x"))[h]
        f = lax.rem(self.at[fast] + jf + 4, 4)
        s = slice(None) if js is None else lax.rem(self.at[slow] + js + 4, 4)
        where = (s, f) if h == 0 else (f, s)
        return self.g.at[(c, *where, slice(r0, r0 + n), slice(None))]

    def copy(self, stage, c, h, d, src):
        i = 0 if d > 0 else 1
        name = (("x", "z"), ("z", "x"))[h][stage // 2]
        m = stage * 2 + i
        return pltpu.make_async_remote_copy(
            src_ref=src,
            dst_ref=self.r[stage].at[c, h, i],
            send_sem=self.send.at[c, h, m],
            recv_sem=self.recv.at[c, h, m],
            device_id={name: lax.rem(self.at[name] + d + 4, 4)},
            device_id_type=MESH,
        )

    def c1(self, c, h, d):
        return self.copy(0, c, h, d, self.unit(c, h, 2, None, 0 if d > 0 else 1))

    def c2(self, c, h, d):
        return self.copy(1, c, h, d, self.unit(c, h, d))

    def c3(self, c, h, d):
        return self.copy(2, c, h, d, self.unit(c, h, 0, 2, 0 if d > 0 else 1))

    def c4(self, c, h, d):
        return self.copy(3, c, h, d, self.unit(c, h, 0, d))

    def s1(self, c):
        for h in (0, 1):
            for d in (1, -1):
                self.c1(c, h, d).start()

    def a1(self, c):
        for d in (1, -1):
            for h in (0, 1):
                i = 0 if d > 0 else 1
                self.c1(c, h, d).wait_recv()
                part = self.unit(c, h, d, None, i)
                for k in range(4):
                    part[k] = part[k] + self.r[0][c, h, i, k]
                self.c2(c, h, d).start()

    def a2(self, c):
        for h in (0, 1):
            for d in (1, -1):
                self.c2(c, h, d).wait_recv()
            whole = self.unit(c, h, 0)
            for k in range(4):
                whole[k] = (
                    whole[k].astype(F32) + self.r[1][c, h, 0, k].astype(F32) + self.r[1][c, h, 1, k].astype(F32)
                ).astype(BF)
            for d in (1, -1):
                self.c3(c, h, d).start()

    def a3(self, c):
        for d in (1, -1):
            for h in (0, 1):
                i = 0 if d > 0 else 1
                self.c3(c, h, d).wait_recv()
                part = self.unit(c, h, 0, d, i)
                part[...] = part[...] + self.r[2][c, h, i]
                self.c4(c, h, d).start()

    def a4(self, c):
        for h in (0, 1):
            for d in (1, -1):
                self.c4(c, h, d).wait_recv()
            own = self.unit(c, h, 0, 0)
            self.out[c, h * 64 : h * 64 + 64, :] = (
                own[...].astype(F32) + self.r[3][c, h, 0].astype(F32) + self.r[3][c, h, 1].astype(F32)
            )

    def drain(self, c):
        for h in (0, 1):
            for d in (1, -1):
                for copy in (self.c1, self.c2, self.c3, self.c4):
                    copy(c, h, d).wait_send()


class TokenScatter:
    def __init__(self, t, p, rc, q1, q2, send, recv, out):
        self.t, self.p, self.rc, self.q1, self.q2 = t, p, rc, q1, q2
        self.send, self.recv, self.out = send, recv, out
        self.y, self.c = lax.axis_index("y"), lax.axis_index("c")

    def to(self, k):
        return lax.rem(self.y + k + 4, 4)

    def pair(self, k):
        return pltpu.make_async_remote_copy(
            src_ref=self.p.at[self.to(k), 1 - self.c],
            dst_ref=self.rc.at[self.to(k)],
            send_sem=self.send.at[self.t, k % 4],
            recv_sem=self.recv.at[self.t, k % 4],
            device_id={"c": 1 - self.c},
            device_id_type=MESH,
        )

    def ring(self, src, dst, m, d):
        return pltpu.make_async_remote_copy(
            src_ref=src,
            dst_ref=dst,
            send_sem=self.send.at[self.t, m],
            recv_sem=self.recv.at[self.t, m],
            device_id={"y": self.to(d)},
            device_id_type=MESH,
        )

    def y1(self, d):
        i = 0 if d > 0 else 1
        return self.ring(self.p.at[self.to(2), self.c, i * 64 : i * 64 + 64], self.q1.at[self.t, i], 4 + i, d)

    def y2(self, d):
        i = 0 if d > 0 else 1
        return self.ring(self.p.at[self.to(d), self.c], self.q2.at[self.t, i], 6 + i, d)

    def share(self, k):
        self.pair(k).start()

    def join(self, k):
        self.pair(k).wait_recv()
        mine = self.p.at[self.to(k), self.c]
        mine[...] = mine[...] + self.rc[self.to(k)]

    def far(self):
        self.join(2)
        for d in (1, -1):
            self.y1(d).start()

    def near(self, d):
        i = 0 if d > 0 else 1
        self.join(d)
        self.y1(d).wait_recv()
        part = self.p.at[self.to(d), self.c, i * 64 : i * 64 + 64]
        part[...] = part[...] + self.q1[self.t, i]
        self.y2(d).start()

    def finish(self):
        self.join(0)
        for d in (1, -1):
            self.y2(d).wait_recv()
        self.out[...] = (
            self.p[self.y, self.c].astype(F32) + self.q2[self.t, 0].astype(F32) + self.q2[self.t, 1].astype(F32)
        )

    def drain(self):
        for k in (0, 1, 2, -1):
            self.pair(k).wait_send()
        for d in (1, -1):
            self.y1(d).wait_send()
            self.y2(d).wait_send()


def butterfly():
    steps = [("c", 1 - lax.axis_index("c"))]
    for name in ("y", "x", "z"):
        me = lax.axis_index(name)
        steps.append((name, me + 1 - 2 * lax.rem(me, 2)))
        steps.append((name, 3 - me))
    return steps


class GainSum:
    def __init__(self, mine, theirs, send, recv):
        self.mine, self.theirs, self.send, self.recv = mine, theirs, send, recv
        self.steps = butterfly()

    def copy(self, i):
        name, partner = self.steps[i]
        return pltpu.make_async_remote_copy(
            src_ref=self.mine.at[i],
            dst_ref=self.theirs.at[i],
            send_sem=self.send.at[i],
            recv_sem=self.recv.at[i],
            device_id={name: partner},
            device_id_type=MESH,
        )

    def start(self, i):
        self.copy(i).start()

    def end(self, i):
        self.copy(i).wait_recv()
        self.mine[i + 1] = self.mine[i] + self.theirs[i]

    def drain(self):
        for i in range(7):
            self.copy(i).wait_send()


def nt(a, b):
    return lax.dot_general(a, b, (((1,), (1,)), ((), ())), preferred_element_type=F32)


def k2_body(
    g_in, w_in, hl_in, dg_in, du_in, earlier_in, gain,
    gs_out, later_out, earlier_out, gain_out,
    g, w, hl, dg, du, x, p, rc, q1, q2, r1, r2, r3, r4, dn, gacc, gmine, gtheirs,
    in_sem, send, recv, tsend, trecv, gsend, grecv,
):
    loads = [pltpu.make_async_copy(g_in.at[c], g.at[c], in_sem.at[c]) for c in range(N_CHUNK)]
    loads += [
        pltpu.make_async_copy(a, b, in_sem.at[3 + i])
        for i, (a, b) in enumerate([(w_in, w), (hl_in, hl), (dg_in, dg), (du_in, du), (earlier_in, x)])
    ]
    for copy in loads:
        copy.start()
    greet(ring_peers(("x", "z", "y")) + [{"c": 1 - lax.axis_index("c")}])
    rs = Scatter(g, r1, r2, r3, r4, send, recv, gs_out)
    later = TokenScatter(0, p.at[0], rc.at[0], q1, q2, tsend, trecv, later_out)
    earlier = TokenScatter(1, p.at[1], rc.at[1], q1, q2, tsend, trecv, earlier_out)
    total = GainSum(gmine, gtheirs, gsend, grecv)
    gain_row = gain[...].astype(F32)
    y = lax.axis_index("y")

    def later_block(k):
        b = lax.rem(y + k + 4, 4)
        rows = pl.ds(pl.multiple_of(b * 256, 256), 256)
        out = nt(hl[0, rows, :], w[0, :, 2 * CHUNK :])
        for c in range(1, N_CHUNK):
            out = out + nt(hl[c, rows, :], w[c, :, 2 * CHUNK :])
        p[0, b, 0] = out[:128].astype(BF)
        p[0, b, 1] = out[128:].astype(BF)
        later.share(k)

    def earlier_block(k):
        b = lax.rem(y + k + 4, 4)
        rows = pl.ds(pl.multiple_of(b * 256, 256), 256)
        out = nt(dg[0, rows, :], w[0, :, :CHUNK])
        out = out + nt(du[0, rows, :], w[0, :, CHUNK : 2 * CHUNK])
        for c in range(1, N_CHUNK):
            out = out + nt(dg[c, rows, :], w[c, :, :CHUNK])
            out = out + nt(du[c, rows, :], w[c, :, CHUNK : 2 * CHUNK])
        dn[...] = out

        for half in (0, 1):

            @pl.loop(0, 8)
            def _(i):
                at = half * 128 + i * 16
                v = x[pl.ds(pl.multiple_of(b * 256 + at, 16), 16), :].astype(F32)
                scale = lax.rsqrt(jnp.mean(v * v, axis=1, keepdims=True) + NORM_FLOOR)
                unit = v * scale
                d = dn[pl.ds(pl.multiple_of(at, 16), 16), :]
                du_ = d * unit
                gacc[...] += du_[:8] + du_[8:]
                mean = jnp.mean(du_ * gain_row, axis=1, keepdims=True)
                branch = scale * (d * gain_row - unit * mean)
                p[1, b, half, pl.ds(pl.multiple_of(i * 16, 16), 16), :] = branch.astype(BF)

        earlier.share(k)

    gacc[...] = jnp.zeros_like(gacc)
    for c in (0, 1):
        loads[c].wait()
        rs.s1(c)
    loads[3].wait()
    loads[4].wait()
    later_block(2)
    rs.a1(0)
    loads[2].wait()
    rs.s1(2)
    later_block(1)
    rs.a1(1)
    later.far()
    later_block(-1)
    rs.a2(0)
    later_block(0)
    later.near(1)
    later.near(-1)
    rs.a1(2)
    for copy in loads[5:]:
        copy.wait()
    earlier_block(2)
    rs.a3(0)
    rs.a2(1)
    earlier_block(1)
    earlier.far()
    rs.a4(0)
    rs.a3(1)
    earlier_block(-1)
    rs.a2(2)
    earlier_block(0)
    later.finish()
    gmine[0] = jnp.sum(gacc[...], axis=0, keepdims=True)
    total.start(0)
    earlier.near(1)
    earlier.near(-1)
    total.end(0)
    total.start(1)
    rs.a4(1)
    rs.a3(2)
    for i in range(1, 6):
        total.end(i)
        total.start(i + 1)
    total.end(6)
    gain_out[...] = gmine[7]
    earlier.finish()
    rs.a4(2)
    for c in range(N_CHUNK):
        rs.drain(c)
    later.drain()
    earlier.drain()
    total.drain()


def k2(g, w, hl, dg, du, earlier_in, gain):
    tokens, width = earlier_in.shape
    any_ = pl.BlockSpec(memory_space=pl.ANY)
    vm = pl.BlockSpec(memory_space=pltpu.VMEM)
    act = (N_CHUNK, tokens, CHUNK)
    return pl.pallas_call(
        k2_body,
        out_shape=[
            jax.ShapeDtypeStruct((N_CHUNK, SHARD, WIDE), F32),
            jax.ShapeDtypeStruct((tokens // 8, width), F32),
            jax.ShapeDtypeStruct((tokens // 8, width), F32),
            jax.ShapeDtypeStruct((1, width), F32),
        ],
        in_specs=[any_] * 6 + [vm],
        out_specs=[vm] * 4,
        scratch_shapes=[
            pltpu.VMEM((N_CHUNK, 4, 4, SHARD, WIDE), BF),
            pltpu.VMEM((N_CHUNK, width, WIDE), BF),
            pltpu.VMEM(act, BF),
            pltpu.VMEM(act, BF),
            pltpu.VMEM(act, BF),
            pltpu.VMEM((tokens, width), BF),
            pltpu.VMEM((2, 4, 2, SHARD, width), BF),
            pltpu.VMEM((2, 4, SHARD, width), BF),
            pltpu.VMEM((2, 2, SHARD // 2, width), BF),
            pltpu.VMEM((2, 2, SHARD, width), BF),
            pltpu.VMEM((N_CHUNK, 2, 2, 4, SHARD // 4, WIDE), BF),
            pltpu.VMEM((N_CHUNK, 2, 2, 4, SHARD // 2, WIDE), BF),
            pltpu.VMEM((N_CHUNK, 2, 2, SHARD // 4, WIDE), BF),
            pltpu.VMEM((N_CHUNK, 2, 2, SHARD // 2, WIDE), BF),
            pltpu.VMEM((256, width), F32),
            pltpu.VMEM((8, width), F32),
            pltpu.VMEM((8, 1, width), F32),
            pltpu.VMEM((7, 1, width), F32),
            pltpu.SemaphoreType.DMA((8,)),
            pltpu.SemaphoreType.DMA((N_CHUNK, 2, 8)),
            pltpu.SemaphoreType.DMA((N_CHUNK, 2, 8)),
            pltpu.SemaphoreType.DMA((2, 8)),
            pltpu.SemaphoreType.DMA((2, 8)),
            pltpu.SemaphoreType.DMA((7,)),
            pltpu.SemaphoreType.DMA((7,)),
        ],
        compiler_params=pltpu.CompilerParams(
            collective_id=1, has_side_effects=True, vmem_limit_bytes=64 * 1024 * 1024 - 65536
        ),
        name="scatter_compute",
    )(g.reshape(N_CHUNK, 4, 4, SHARD, WIDE), w, hl, dg, du, earlier_in, gain.reshape(1, width))


def local(later_in, earlier_in, cot, gate_w, up_w, down_w, gain, gate_sum, up_sum, down_sum, gain_sum):
    cols = gate_w.shape[1]
    w_own = jnp.concatenate([pack(gate_w), pack(up_w), pack(down_w)], axis=2)
    w, hl, dg, du, g = k1(later_in, earlier_in, cot, gain, w_own)
    hidden = hl.transpose(1, 0, 2).reshape(hl.shape[1], -1)
    own = later_in.shape[0] // 8
    at = lax.axis_index(TP) * own
    rows = lambda a: lax.dynamic_slice_in_dim(a, at, own, 0).astype(F32)
    gs, later_sum, earlier_sum, gain_total = k2(g, w, hl, dg, du, earlier_in, gain)
    later_out = (rows(later_in) + 0.5 * later_sum).astype(BF)
    earlier_grad = (rows(cot) + earlier_sum).astype(BF)
    gain_new = gain_sum + gain_total[0]
    gs = gs.transpose(1, 0, 2).reshape(gs.shape[1], N_CHUNK, 3, CHUNK)
    pick = lambda k: gs[:, :, k, :].reshape(gs.shape[0], -1)[:, :cols]
    return (
        later_out, hidden[:, :cols], earlier_grad,
        gate_sum + pick(0), up_sum + pick(1), down_sum + pick(2), gain_new,
    )


def solution(mesh):
    torus = Mesh(mesh.devices.reshape(4, 4, 4, 2), ALL)
    return jax.shard_map(
        local,
        mesh=torus,
        in_specs=(P(FS, None),) * 3 + (P(FS, TP),) * 3 + (P(),) + (P(FS, TP),) * 3 + (P(),),
        out_specs=(P(ALL, None), P(FS, TP), P(ALL, None), P(FS, TP), P(FS, TP), P(FS, TP), P()),
        check_vma=False,
    )
```

```python
import functools

import jax
import jax.numpy as jnp
from jax import lax
from jax.experimental import pallas as pl
from jax.experimental.pallas import tpu as pltpu
from jax.sharding import Mesh
from jax.sharding import PartitionSpec as P

FS = ("z", "x")
TP = ("y", "c")
ALL = ("z", "x", "y", "c")
MESH = pl.DeviceIdType.MESH
BF = jnp.bfloat16
F32 = jnp.float32
CHUNK = 256
N_CHUNK = 3
WIDE = 3 * CHUNK
SHARD = 128
NORM_FLOOR = 0.05


class Gather:
    def __init__(self, w, send, recv):
        self.w, self.send, self.recv = w, send, recv
        self.mz, self.mx = lax.axis_index("z"), lax.axis_index("x")

    def owner(self, h, jf, js):
        dx, dz = (jf, js) if h == 0 else (js, jf)
        return lax.rem(self.mz + dz + 4, 4) * 4 + lax.rem(self.mx + dx + 4, 4)

    def copy(self, c, h, msg, jf, js, sub, axis, d):
        start = self.owner(h, jf, js) * SHARD + h * (SHARD // 2)
        size = SHARD // 2
        if sub is not None:
            size = SHARD // 4
            start = start + sub * size
        view = self.w.at[c, pl.ds(pl.multiple_of(start, 32), size), :]
        name = ("x", "z")[h] if axis == "f" else ("z", "x")[h]
        me = self.mx if name == "x" else self.mz
        return pltpu.make_async_remote_copy(
            src_ref=view,
            dst_ref=view,
            send_sem=self.send.at[c, h, msg],
            recv_sem=self.recv.at[c, h, msg],
            device_id={name: lax.rem(me + d + 4, 4)},
            device_id_type=MESH,
        )

    def m1(self, c, h, d):
        return self.copy(c, h, 0 if d > 0 else 1, 0, 0, None, "f", d)

    def r1(self, c, h, d):
        return self.copy(c, h, 0 if d > 0 else 1, -d, 0, None, "f", d)

    def m2(self, c, h, d):
        return self.copy(c, h, 2 if d > 0 else 3, -d, 0, 0 if d > 0 else 1, "f", d)

    def r2(self, c, h, d):
        return self.copy(c, h, 2 if d > 0 else 3, -2 * d, 0, 0 if d > 0 else 1, "f", d)

    def m3(self, c, h, j, d):
        return self.copy(c, h, 4 + 2 * (j % 4) + (0 if d > 0 else 1), j, 0, None, "s", d)

    def r3(self, c, h, j, d):
        return self.copy(c, h, 4 + 2 * (j % 4) + (0 if d > 0 else 1), j, -d, None, "s", d)

    def m4(self, c, h, j, d):
        return self.copy(c, h, 12 + 2 * (j % 4) + (0 if d > 0 else 1), j, -d, 0 if d > 0 else 1, "s", d)

    def r4(self, c, h, j, d):
        return self.copy(c, h, 12 + 2 * (j % 4) + (0 if d > 0 else 1), j, -2 * d, 0 if d > 0 else 1, "s", d)

    def t0(self, c):
        for h in (0, 1):
            for d in (1, -1):
                self.m1(c, h, d).start()
        for h in (0, 1):
            for d in (1, -1):
                self.m3(c, h, 0, d).start()

    def t1(self, c):
        for d in (1, -1):
            for h in (0, 1):
                self.r1(c, h, d).wait_recv()
                self.m2(c, h, d).start()
                for e in (1, -1):
                    self.m3(c, h, -d, e).start()

    def pass_on(self, c, js):
        for j in js:
            for d in (1, -1):
                for h in (0, 1):
                    self.r3(c, h, j, d).wait_recv()
                    self.m4(c, h, j, d).start()

    def t2(self, c):
        self.pass_on(c, (0,))

    def t3(self, c):
        for h in (0, 1):
            for d in (1, -1):
                self.r2(c, h, d).wait_recv()
            for e in (1, -1):
                self.m3(c, h, 2, e).start()

    def t4(self, c):
        self.pass_on(c, (-1, 1))

    def t5(self, c):
        self.pass_on(c, (2,))

    def t6(self, c):
        for h in (0, 1):
            for j in (0, -1, 1, 2):
                for d in (1, -1):
                    self.r4(c, h, j, d).wait_recv()

    def drain(self, c):
        for h in (0, 1):
            for d in (1, -1):
                self.m1(c, h, d).wait_send()
                self.m2(c, h, d).wait_send()
                for j in (0, -1, 1, 2):
                    self.m3(c, h, j, d).wait_send()
                    self.m4(c, h, j, d).wait_send()


def greet(peers):
    barrier = pltpu.get_barrier_semaphore()
    for peer in peers:
        pl.semaphore_signal(barrier, inc=1, device_id=peer, device_id_type=MESH)
    pl.semaphore_wait(barrier, len(peers))


def ring_peers(names):
    peers = []
    for name in names:
        me = lax.axis_index(name)
        for d in (1, 3):
            peers.append({name: lax.rem(me + d, 4)})
    return peers


def nn(a, b):
    return jnp.dot(a, b, preferred_element_type=F32)


class Scatter:
    def __init__(self, g, r1, r2, r3, r4, send, recv, out):
        self.g, self.r = g, (r1, r2, r3, r4)
        self.send, self.recv, self.out = send, recv, out
        self.at = {"z": lax.axis_index("z"), "x": lax.axis_index("x")}

    def unit(self, c, h, jf, js=None, sub=None):
        r0, n = h * 64, 64
        if sub is not None:
            r0, n = r0 + sub * 32, 32
        fast, slow = (("x", "z"), ("z", "x"))[h]
        f = lax.rem(self.at[fast] + jf + 4, 4)
        s = slice(None) if js is None else lax.rem(self.at[slow] + js + 4, 4)
        where = (s, f) if h == 0 else (f, s)
        return self.g.at[(c, *where, slice(r0, r0 + n), slice(None))]

    def copy(self, stage, c, h, d, src):
        i = 0 if d > 0 else 1
        name = (("x", "z"), ("z", "x"))[h][stage // 2]
        m = stage * 2 + i
        return pltpu.make_async_remote_copy(
            src_ref=src,
            dst_ref=self.r[stage].at[c, h, i],
            send_sem=self.send.at[c, h, m],
            recv_sem=self.recv.at[c, h, m],
            device_id={name: lax.rem(self.at[name] + d + 4, 4)},
            device_id_type=MESH,
        )

    def c1(self, c, h, d):
        return self.copy(0, c, h, d, self.unit(c, h, 2, None, 0 if d > 0 else 1))

    def c2(self, c, h, d):
        return self.copy(1, c, h, d, self.unit(c, h, d))

    def c3(self, c, h, d):
        return self.copy(2, c, h, d, self.unit(c, h, 0, 2, 0 if d > 0 else 1))

    def c4(self, c, h, d):
        return self.copy(3, c, h, d, self.unit(c, h, 0, d))

    def s1(self, c):
        for h in (0, 1):
            for d in (1, -1):
                self.c1(c, h, d).start()

    def a1(self, c):
        for d in (1, -1):
            for h in (0, 1):
                i = 0 if d > 0 else 1
                self.c1(c, h, d).wait_recv()
                part = self.unit(c, h, d, None, i)
                for k in range(4):
                    part[k] = part[k] + self.r[0][c, h, i, k]
                self.c2(c, h, d).start()

    def a2(self, c):
        for h in (0, 1):
            for d in (1, -1):
                self.c2(c, h, d).wait_recv()
            whole = self.unit(c, h, 0)
            for k in range(4):
                whole[k] = (
                    whole[k].astype(F32) + self.r[1][c, h, 0, k].astype(F32) + self.r[1][c, h, 1, k].astype(F32)
                ).astype(BF)
            for d in (1, -1):
                self.c3(c, h, d).start()

    def a3(self, c):
        for d in (1, -1):
            for h in (0, 1):
                i = 0 if d > 0 else 1
                self.c3(c, h, d).wait_recv()
                part = self.unit(c, h, 0, d, i)
                part[...] = part[...] + self.r[2][c, h, i]
                self.c4(c, h, d).start()

    def a4(self, c):
        for h in (0, 1):
            for d in (1, -1):
                self.c4(c, h, d).wait_recv()
            own = self.unit(c, h, 0, 0)
            done = own[...].astype(F32) + self.r[3][c, h, 0].astype(F32) + self.r[3][c, h, 1].astype(F32)
            at = slice(h * 64, h * 64 + 64)
            for k, out in enumerate(self.out):
                n = min(CHUNK, out.shape[1] - c * CHUNK)
                cols = slice(c * CHUNK, c * CHUNK + n)
                out[at, cols] = out[at, cols] + done[:, k * CHUNK : k * CHUNK + n]

    def drain(self, c):
        for h in (0, 1):
            for d in (1, -1):
                for copy in (self.c1, self.c2, self.c3, self.c4):
                    copy(c, h, d).wait_send()


class TokenScatter:
    def __init__(self, t, p, rc, q, credit, send, recv):
        self.t, self.p, self.rc, self.q, self.credit = t, p, rc, q, credit
        self.send, self.recv = send, recv
        self.y, self.c = lax.axis_index("y"), lax.axis_index("c")

    def to(self, k):
        return lax.rem(self.y + k + 4, 4)

    def rows(self, k, core, sub=None):
        start, n = (self.to(k) * 2 + core) * SHARD, SHARD
        if sub is not None:
            start, n = start + sub * (SHARD // 2), SHARD // 2
        return self.p.at[pl.ds(pl.multiple_of(start, SHARD // 2), n), :]

    def landed(self, k):
        start = self.t * 4 * SHARD + self.to(k) * SHARD
        return self.rc.at[pl.ds(pl.multiple_of(start, SHARD), SHARD), :]

    def q1(self, i):
        start = self.t * 3 * SHARD + i * (SHARD // 2)
        return self.q.at[start : start + SHARD // 2, :]

    def q2(self, i):
        start = self.t * 3 * SHARD + (1 + i) * SHARD
        return self.q.at[start : start + SHARD, :]

    def pair(self, k):
        return pltpu.make_async_remote_copy(
            src_ref=self.rows(k, 1 - self.c),
            dst_ref=self.landed(k),
            send_sem=self.send.at[self.t, k % 4],
            recv_sem=self.recv.at[self.t, k % 4],
            device_id={"c": 1 - self.c},
            device_id_type=MESH,
        )

    def ring(self, src, dst, m, d):
        return pltpu.make_async_remote_copy(
            src_ref=src,
            dst_ref=dst,
            send_sem=self.send.at[self.t, m],
            recv_sem=self.recv.at[self.t, m],
            device_id={"y": self.to(d)},
            device_id_type=MESH,
        )

    def y1(self, d):
        i = 0 if d > 0 else 1
        return self.ring(self.rows(2, self.c, i), self.q1(i), 4 + i, d)

    def y2(self, d):
        i = 0 if d > 0 else 1
        return self.ring(self.rows(d, self.c), self.q2(i), 6 + i, d)

    def share(self, k):
        if self.t == 0 and k == 2:
            pl.semaphore_wait(self.credit.at[0], 1)
        self.pair(k).start()

    def join(self, k):
        self.pair(k).wait_recv()
        mine = self.rows(k, self.c)
        mine[...] = mine[...] + self.landed(k)[...]

    def far(self):
        self.join(2)
        for d in (1, -1):
            if self.t == 0:
                pl.semaphore_wait(self.credit.at[1 if d > 0 else 2], 1)
            self.y1(d).start()

    def near(self, d):
        i = 0 if d > 0 else 1
        self.join(d)
        self.y1(d).wait_recv()
        part = self.rows(d, self.c, i)
        part[...] = part[...] + self.q1(i)[...]
        self.y2(d).start()

    def finish(self):
        self.join(0)
        for d in (1, -1):
            self.y2(d).wait_recv()
        return (
            self.rows(0, self.c)[...].astype(F32) + self.q2(0)[...].astype(F32) + self.q2(1)[...].astype(F32)
        )

    def drain(self):
        for k in (0, 1, 2, -1):
            self.pair(k).wait_send()
        for d in (1, -1):
            self.y1(d).wait_send()
            self.y2(d).wait_send()


def butterfly():
    steps = [("c", 1 - lax.axis_index("c"))]
    for name in ("y", "x", "z"):
        me = lax.axis_index(name)
        steps.append((name, me + 1 - 2 * lax.rem(me, 2)))
        steps.append((name, 3 - me))
    return steps


class GainSum:
    def __init__(self, mine, theirs, send, recv):
        self.mine, self.theirs, self.send, self.recv = mine, theirs, send, recv
        self.steps = butterfly()

    def copy(self, i):
        name, partner = self.steps[i]
        return pltpu.make_async_remote_copy(
            src_ref=self.mine.at[i],
            dst_ref=self.theirs.at[i],
            send_sem=self.send.at[i],
            recv_sem=self.recv.at[i],
            device_id={name: partner},
            device_id_type=MESH,
        )

    def start(self, i):
        self.copy(i).start()

    def end(self, i):
        self.copy(i).wait_recv()
        self.mine[i + 1] = self.mine[i] + self.theirs[i]

    def drain(self):
        for i in range(7):
            self.copy(i).wait_send()


def nt(a, b):
    return lax.dot_general(a, b, (((1,), (1,)), ((), ())), preferred_element_type=F32)


def sublayer(
    later_in, earlier_in, cot_in, gate_w, up_w, down_w, gain, gate_sum, up_sum, down_sum,
    later_out, hidden_out, earlier_out, gate_new, up_new, down_new, gain_out,
    w, g, nl, ne, cot, net, cott, hl, dg, du, he, r1, r2, r3, r4, dn, lrow, crow, gacc, gmine, gtheirs,
    in_sem, wsend, wrecv, send, recv, tsend, trecv, gsend, grecv, credit, out_sem,
):
    tokens, width = nl.shape
    half = width // 2
    z, x, y, c_me = (lax.axis_index(n) for n in ALL)
    me = z * 4 + x
    own_rows = pl.ds(pl.multiple_of((y * 2 + c_me) * SHARD, SHARD), SHARD)
    pairs = [
        (later_in, nl), (earlier_in, ne), (cot_in, cot),
        (gate_sum, gate_new), (up_sum, up_new), (down_sum, down_new),
        (later_in.at[own_rows, :], lrow), (cot_in.at[own_rows, :], crow),
    ]
    ins = [pltpu.make_async_copy(a, b, in_sem.at[i]) for i, (a, b) in enumerate(pairs)]
    ins[0].start()
    ins[1].start()
    mine = pl.ds(pl.multiple_of(me * SHARD, SHARD), SHARD)
    for k, ref in enumerate((gate_w, up_w, down_w)):
        cols = ref.shape[1]
        for c in range(N_CHUNK):
            n = min(CHUNK, cols - c * CHUNK)
            part = ref[:, c * CHUNK : c * CHUNK + n]
            if n < CHUNK:
                part = jnp.concatenate([part, jnp.zeros((SHARD, CHUNK - n), BF)], axis=1)
            w[c, mine, k * CHUNK : (k + 1) * CHUNK] = part
    greet(ring_peers(("x", "z", "y")) + [{"c": 1 - c_me}])
    ring = Gather(w, wsend, wrecv)
    ring.t0(0)
    for copy in ins[2:]:
        copy.start()
    rs = Scatter(g, r1, r2, r3, r4, send, recv, (gate_new, up_new, down_new))
    later = TokenScatter(0, nl, net, cot, credit, tsend, trecv)
    earlier = TokenScatter(1, ne, net, cot, credit, tsend, trecv)
    total = GainSum(gmine, gtheirs, gsend, grecv)

    gain_row = gain[...].astype(F32)

    def turn(ref, i):
        rows = pl.ds(pl.multiple_of(i * 128, 128), 128)
        return [ref[rows, j * half : (j + 1) * half].T for j in (0, 1)]

    def put(turned, ref, i):
        start = pl.multiple_of(i * 128, 128)
        flipped = turn(ref, i)
        turned[:, pl.ds(start, 128)] = flipped[0]
        turned[:, pl.ds(pl.multiple_of(start + tokens, 128), 128)] = flipped[1]

    def norm_block(ref, i):
        rows = pl.ds(pl.multiple_of(i * 64, 64), 64)
        v = ref[rows, :].astype(F32)
        unit = v * lax.rsqrt(jnp.mean(v * v, axis=1, keepdims=True) + NORM_FLOOR)
        ref[rows, :] = (unit * gain_row).astype(BF)

    blocks = tokens // 128

    def norms(ref, first, last):
        @pl.loop(first, last)
        def _(i):
            norm_block(ref, i)

    def turns(turned, ref, first, last):
        @pl.loop(first, last)
        def _(i):
            put(turned, ref, i)

    ins[0].wait()
    norms(nl, 0, blocks)
    ring.t1(0)
    norms(nl, blocks, 2 * blocks)
    ring.t2(0)
    ins[1].wait()
    norms(ne, 0, blocks)
    ring.t3(0)
    ring.t0(1)
    norms(ne, blocks, 2 * blocks)
    turns(net, ne, 0, blocks // 2)
    ring.t4(0)
    ring.t1(1)
    turns(net, ne, blocks // 2, blocks)
    ins[2].wait()
    turns(cott, cot, 0, blocks // 2)
    ring.t5(0)
    ring.t2(1)
    turns(cott, cot, blocks // 2, blocks)
    ring.t6(0)
    for copy in ins[3:]:
        copy.wait()

    tb = 256

    def later_item(c, i):
        rows = pl.ds(i * tb, tb)
        pre = nn(nl[rows, :], w[c, :, : 2 * CHUNK])
        gate, up = pre[:, :CHUNK], pre[:, CHUNK:]
        hl[c, rows, :] = (gate * jax.nn.sigmoid(gate) * up).astype(BF)

    def earlier_item(c, i):
        rows = pl.ds(i * tb, tb)
        pre = nn(ne[rows, :], w[c, :, : 2 * CHUNK])
        dh = 0.5 * nn(cot[rows, :], w[c, :, 2 * CHUNK :])
        gate, up = pre[:, :CHUNK], pre[:, CHUNK:]
        s = jax.nn.sigmoid(gate)
        act = gate * s
        he[rows, :] = (act * up).astype(BF)
        dg[c, rows, :] = (dh * up * s * (1.0 + gate * (1.0 - s))).astype(BF)
        du[c, rows, :] = (dh * act).astype(BF)

    def grad_item(c, i):
        rows = pl.ds((i % 2) * 512, 512)
        cols = pl.ds((i // 2) * tokens, tokens)
        shape = (4, SHARD, CHUNK)
        g[c, i, :, :, :CHUNK] = nn(net[rows, cols], dg[c]).astype(BF).reshape(shape)
        g[c, i, :, :, CHUNK : 2 * CHUNK] = nn(net[rows, cols], du[c]).astype(BF).reshape(shape)
        g[c, i, :, :, 2 * CHUNK :] = (0.5 * nn(cott[rows, cols], he[...])).astype(BF).reshape(shape)

    reload = pltpu.make_async_copy(earlier_in, cott, in_sem.at[8])

    def free():
        reload.start()
        pl.semaphore_signal(credit.at[0], inc=1, device_id={"c": 1 - c_me}, device_id_type=MESH)
        pl.semaphore_signal(credit.at[1], inc=1, device_id={"y": lax.rem(y + 3, 4)}, device_id_type=MESH)
        pl.semaphore_signal(credit.at[2], inc=1, device_id={"y": lax.rem(y + 1, 4)}, device_id_type=MESH)

    outs = [
        pltpu.make_async_copy(hl.at[c], hidden_out.at[:, c * CHUNK : (c + 1) * CHUNK], out_sem.at[c])
        for c in range(N_CHUNK)
    ]

    ticks = {
        0: {0: [ring.t3, 1], 1: [ring.t0, 2], 3: [ring.t4, 1], 4: [ring.t1, 2], 6: [ring.t5, 1], 7: [ring.t2, 2], 9: [ring.t6, 1]},
        1: {0: [ring.t3, 2], 3: [ring.t4, 2], 6: [ring.t5, 2], 8: [rs.s1, 0], 11: [ring.t6, 2]},
        2: {0: [rs.s1, 1], 4: [rs.a1, 0], 7: [rs.s1, 2], 10: [rs.a1, 1]},
    }

    @pl.loop(0, N_CHUNK)
    def _(c):
        items = [functools.partial(earlier_item, c, i) for i in range(tokens // tb)]
        items += [functools.partial(grad_item, c, i) for i in range(width // 512)]
        items += [functools.partial(later_item, c, i) for i in range(tokens // tb)]
        for n, item in enumerate(items):
            item()
            for when in range(N_CHUNK):
                todo = ticks[when].get(n)
                if todo is not None or (when == 2 and n == 7):

                    @pl.when(c == when)
                    def _():
                        if when == 2 and n == 7:
                            free()
                        if todo is not None:
                            todo[0](todo[1])

    for copy in outs:
        copy.start()

    def token_rows(b):
        return pl.ds(pl.multiple_of(b * 256, 256), 256)

    def later_block(k):
        b = lax.rem(y + k + 4, 4)
        rows = token_rows(b)

        @pl.loop(0, 4)
        def _(n):
            f = pl.ds(pl.multiple_of(n * 512, 512), 512)
            out = nt(hl[0, rows, :], w[0, f, 2 * CHUNK :])
            for c in range(1, N_CHUNK):
                out = out + nt(hl[c, rows, :], w[c, f, 2 * CHUNK :])
            nl[rows, f] = out.astype(BF)

        later.share(k)

    def earlier_block(k):
        b = lax.rem(y + k + 4, 4)
        rows = token_rows(b)

        @pl.loop(0, 4)
        def _(n):
            f = pl.ds(pl.multiple_of(n * 512, 512), 512)
            out = nt(dg[0, rows, :], w[0, f, :CHUNK])
            out = out + nt(du[0, rows, :], w[0, f, CHUNK : 2 * CHUNK])
            for c in range(1, N_CHUNK):
                out = out + nt(dg[c, rows, :], w[c, f, :CHUNK])
                out = out + nt(du[c, rows, :], w[c, f, CHUNK : 2 * CHUNK])
            dn[:, f] = out

        @pl.loop(0, 16)
        def _(i):
            at = pl.ds(pl.multiple_of(b * 256 + i * 16, 16), 16)
            v = cott[at, :].astype(F32)
            scale = lax.rsqrt(jnp.mean(v * v, axis=1, keepdims=True) + NORM_FLOOR)
            unit = v * scale
            d = dn[pl.ds(pl.multiple_of(i * 16, 16), 16), :]
            terms = d * unit
            gacc[...] += terms[:8] + terms[8:]
            mean = jnp.mean(terms * gain_row, axis=1, keepdims=True)
            ne[at, :] = (scale * (d * gain_row - unit * mean)).astype(BF)

        earlier.share(k)

    gacc[...] = jnp.zeros_like(gacc)
    later_block(2)
    later_block(1)
    later.far()
    reload.wait()
    earlier_block(2)
    later_block(-1)
    earlier.far()
    later_block(0)
    rs.a2(0)
    earlier_block(1)
    later.near(1)
    later.near(-1)
    rs.a1(2)
    earlier_block(-1)
    earlier.near(1)
    earlier.near(-1)
    earlier_block(0)
    gmine[0] = jnp.sum(gacc[...], axis=0, keepdims=True)
    total.start(0)
    rs.a2(1)
    rs.a3(0)
    total.end(0)
    total.start(1)
    later_out[...] = (lrow[...].astype(F32) + 0.5 * later.finish()).astype(BF)
    total.end(1)
    total.start(2)
    rs.a2(2)
    rs.a3(1)
    total.end(2)
    total.start(3)
    rs.a4(0)
    rs.a3(2)
    total.end(3)
    total.start(4)
    rs.a4(1)
    total.end(4)
    total.start(5)
    earlier_out[...] = (crow[...].astype(F32) + earlier.finish()).astype(BF)
    total.end(5)
    total.start(6)
    rs.a4(2)
    total.end(6)
    gain_out[...] = gmine[7]
    for c in range(N_CHUNK):
        ring.drain(c)
        rs.drain(c)
    later.drain()
    earlier.drain()
    total.drain()
    for copy in outs:
        copy.wait()


def run(later_in, earlier_in, cot, gate_w, up_w, down_w, gain, gate_sum, up_sum, down_sum):
    tokens, width = later_in.shape
    rows, cols = gate_w.shape
    any_ = pl.BlockSpec(memory_space=pl.ANY)
    vm = pl.BlockSpec(memory_space=pltpu.VMEM)
    act = (N_CHUNK, tokens, CHUNK)
    tok = (tokens, width)
    dma = pltpu.SemaphoreType.DMA
    return pl.pallas_call(
        sublayer,
        out_shape=[
            jax.ShapeDtypeStruct((tokens // 8, width), BF),
            jax.ShapeDtypeStruct((tokens, N_CHUNK * CHUNK), BF),
            jax.ShapeDtypeStruct((tokens // 8, width), BF),
            jax.ShapeDtypeStruct((rows, cols), F32),
            jax.ShapeDtypeStruct((rows, cols), F32),
            jax.ShapeDtypeStruct((rows, cols), F32),
            jax.ShapeDtypeStruct((1, width), F32),
        ],
        in_specs=[any_] * 3 + [vm] * 4 + [any_] * 3,
        out_specs=[vm, any_] + [vm] * 5,
        scratch_shapes=[
            pltpu.VMEM((N_CHUNK, width, WIDE), BF),
            pltpu.VMEM((N_CHUNK, 4, 4, SHARD, WIDE), BF),
            pltpu.VMEM(tok, BF),
            pltpu.VMEM(tok, BF),
            pltpu.VMEM(tok, BF),
            pltpu.VMEM(tok, BF),
            pltpu.VMEM(tok, BF),
            pltpu.VMEM(act, BF),
            pltpu.VMEM(act, BF),
            pltpu.VMEM(act, BF),
            pltpu.VMEM((tokens, CHUNK), BF),
            pltpu.VMEM((N_CHUNK, 2, 2, 4, SHARD // 4, WIDE), BF),
            pltpu.VMEM((N_CHUNK, 2, 2, 4, SHARD // 2, WIDE), BF),
            pltpu.VMEM((N_CHUNK, 2, 2, SHARD // 4, WIDE), BF),
            pltpu.VMEM((N_CHUNK, 2, 2, SHARD // 2, WIDE), BF),
            pltpu.VMEM((256, width), F32),
            pltpu.VMEM((SHARD, width), BF),
            pltpu.VMEM((SHARD, width), BF),
            pltpu.VMEM((8, width), F32),
            pltpu.VMEM((8, 1, width), F32),
            pltpu.VMEM((7, 1, width), F32),
            dma((9,)),
            dma((N_CHUNK, 2, 20)),
            dma((N_CHUNK, 2, 20)),
            dma((N_CHUNK, 2, 8)),
            dma((N_CHUNK, 2, 8)),
            dma((2, 8)),
            dma((2, 8)),
            dma((7,)),
            dma((7,)),
            pltpu.SemaphoreType.REGULAR((3,)),
            dma((N_CHUNK,)),
        ],
        compiler_params=pltpu.CompilerParams(
            collective_id=0, has_side_effects=True, vmem_limit_bytes=64 * 1024 * 1024 - 65536
        ),
        name="sublayer",
    )(later_in, earlier_in, cot, gate_w, up_w, down_w, gain.reshape(1, width), gate_sum, up_sum, down_sum)


def local(later_in, earlier_in, cot, gate_w, up_w, down_w, gain, gate_sum, up_sum, down_sum, gain_sum):
    later_out, hidden, earlier_grad, gate_new, up_new, down_new, gain_total = run(
        later_in, earlier_in, cot, gate_w, up_w, down_w, gain, gate_sum, up_sum, down_sum
    )
    return (
        later_out, hidden[:, : gate_w.shape[1]], earlier_grad,
        gate_new, up_new, down_new, gain_sum + gain_total[0],
    )


def solution(mesh):
    torus = Mesh(mesh.devices.reshape(4, 4, 4, 2), ALL)
    return jax.shard_map(
        local,
        mesh=torus,
        in_specs=(P(FS, None),) * 3 + (P(FS, TP),) * 3 + (P(),) + (P(FS, TP),) * 3 + (P(),),
        out_specs=(P(ALL, None), P(FS, TP), P(ALL, None), P(FS, TP), P(FS, TP), P(FS, TP), P()),
        check_vma=False,
    )
```

```python
import functools

import jax
import jax.numpy as jnp
from jax import lax
from jax.experimental import pallas as pl
from jax.experimental.pallas import tpu as pltpu
from jax.sharding import Mesh
from jax.sharding import PartitionSpec as P

FS = ("z", "x")
TP = ("y", "c")
ALL = ("z", "x", "y", "c")
MESH = pl.DeviceIdType.MESH
BF = jnp.bfloat16
F32 = jnp.float32
N_CHUNK = 2
CHUNK = 352
WIDE = 3 * CHUNK
HALF = WIDE // 2
CUT = 272
SHARD = 128
NORM_FLOOR = 0.05


def span(h, sub=None):
    at = h * HALF
    return slice(at + (CUT if sub == 1 else 0), at + (CUT if sub == 0 else HALF))


class Gather:
    def __init__(self, w, send, recv):
        self.w, self.send, self.recv = w, send, recv
        self.mz, self.mx = lax.axis_index("z"), lax.axis_index("x")

    def owner(self, h, jf, js):
        dx, dz = (jf, js) if h == 0 else (js, jf)
        return lax.rem(self.mz + dz + 4, 4) * 4 + lax.rem(self.mx + dx + 4, 4)

    def copy(self, c, h, msg, jf, js, sub, axis, d):
        view = self.w.at[
            c, span(h, sub), pl.ds(pl.multiple_of(self.owner(h, jf, js) * SHARD, SHARD), SHARD)
        ]
        name = ("x", "z")[h] if axis == "f" else ("z", "x")[h]
        me = self.mx if name == "x" else self.mz
        return pltpu.make_async_remote_copy(
            src_ref=view,
            dst_ref=view,
            send_sem=self.send.at[c, h, msg],
            recv_sem=self.recv.at[c, h, msg],
            device_id={name: lax.rem(me + d + 4, 4)},
            device_id_type=MESH,
        )

    def m1(self, c, h, d):
        return self.copy(c, h, 0 if d > 0 else 1, 0, 0, None, "f", d)

    def r1(self, c, h, d):
        return self.copy(c, h, 0 if d > 0 else 1, -d, 0, None, "f", d)

    def m2(self, c, h, d):
        return self.copy(c, h, 2 if d > 0 else 3, -d, 0, 0 if d > 0 else 1, "f", d)

    def r2(self, c, h, d):
        return self.copy(c, h, 2 if d > 0 else 3, -2 * d, 0, 0 if d > 0 else 1, "f", d)

    def m3(self, c, h, j, d):
        return self.copy(c, h, 4 + 2 * (j % 4) + (0 if d > 0 else 1), j, 0, None, "s", d)

    def r3(self, c, h, j, d):
        return self.copy(c, h, 4 + 2 * (j % 4) + (0 if d > 0 else 1), j, -d, None, "s", d)

    def m4(self, c, h, j, d):
        return self.copy(c, h, 12 + 2 * (j % 4) + (0 if d > 0 else 1), j, -d, 0 if d > 0 else 1, "s", d)

    def r4(self, c, h, j, d):
        return self.copy(c, h, 12 + 2 * (j % 4) + (0 if d > 0 else 1), j, -2 * d, 0 if d > 0 else 1, "s", d)

    def t0(self, c):
        for h in (0, 1):
            for d in (1, -1):
                self.m1(c, h, d).start()
        for h in (0, 1):
            for d in (1, -1):
                self.m3(c, h, 0, d).start()

    def t1(self, c):
        for d in (1, -1):
            for h in (0, 1):
                self.r1(c, h, d).wait_recv()
                self.m2(c, h, d).start()
                for e in (1, -1):
                    self.m3(c, h, -d, e).start()

    def pass_on(self, c, js):
        for j in js:
            for d in (1, -1):
                for h in (0, 1):
                    self.r3(c, h, j, d).wait_recv()
                    self.m4(c, h, j, d).start()

    def t2(self, c):
        self.pass_on(c, (0,))

    def t3(self, c):
        for h in (0, 1):
            for d in (1, -1):
                self.r2(c, h, d).wait_recv()
            for e in (1, -1):
                self.m3(c, h, 2, e).start()

    def t4(self, c):
        self.pass_on(c, (-1, 1))

    def t5(self, c):
        self.pass_on(c, (2,))

    def t6(self, c):
        for h in (0, 1):
            for j in (0, -1, 1, 2):
                for d in (1, -1):
                    self.r4(c, h, j, d).wait_recv()

    def drain(self, c):
        for h in (0, 1):
            for d in (1, -1):
                self.m1(c, h, d).wait_send()
                self.m2(c, h, d).wait_send()
                for j in (0, -1, 1, 2):
                    self.m3(c, h, j, d).wait_send()
                    self.m4(c, h, j, d).wait_send()


def greet(peers):
    barrier = pltpu.get_barrier_semaphore()
    for peer in peers:
        pl.semaphore_signal(barrier, inc=1, device_id=peer, device_id_type=MESH)
    pl.semaphore_wait(barrier, len(peers))


def ring_peers(names):
    peers = []
    for name in names:
        me = lax.axis_index(name)
        for d in (1, 3):
            peers.append({name: lax.rem(me + d, 4)})
    return peers


def nn(a, b):
    return jnp.dot(a, b, preferred_element_type=F32)


class Scatter:
    def __init__(self, g, r1, r2, r3, r4, send, recv, out):
        self.g, self.r = g, (r1, r2, r3, r4)
        self.send, self.recv, self.out = send, recv, out
        self.at = {"z": lax.axis_index("z"), "x": lax.axis_index("x")}

    def unit(self, c, h, jf, js=None, sub=None):
        fast, slow = (("x", "z"), ("z", "x"))[h]
        f = lax.rem(self.at[fast] + jf + 4, 4)
        s = slice(None) if js is None else lax.rem(self.at[slow] + js + 4, 4)
        where = (s, f) if h == 0 else (f, s)
        return self.g.at[(c, *where, span(h, sub), slice(None))]

    def landing(self, stage, c, h, i):
        ref = self.r[stage]
        if stage % 2:
            return ref.at[c, h, i]
        n = CUT if i == 0 else HALF - CUT
        return ref.at[c, h, i, :, :n] if stage == 0 else ref.at[c, h, i, :n]

    def copy(self, stage, c, h, d, src):
        i = 0 if d > 0 else 1
        name = (("x", "z"), ("z", "x"))[h][stage // 2]
        m = stage * 2 + i
        return pltpu.make_async_remote_copy(
            src_ref=src,
            dst_ref=self.landing(stage, c, h, i),
            send_sem=self.send.at[c, h, m],
            recv_sem=self.recv.at[c, h, m],
            device_id={name: lax.rem(self.at[name] + d + 4, 4)},
            device_id_type=MESH,
        )

    def c1(self, c, h, d):
        return self.copy(0, c, h, d, self.unit(c, h, 2, None, 0 if d > 0 else 1))

    def c2(self, c, h, d):
        return self.copy(1, c, h, d, self.unit(c, h, d))

    def c3(self, c, h, d):
        return self.copy(2, c, h, d, self.unit(c, h, 0, 2, 0 if d > 0 else 1))

    def c4(self, c, h, d):
        return self.copy(3, c, h, d, self.unit(c, h, 0, d))

    def s1(self, c):
        for h in (0, 1):
            for d in (1, -1):
                self.c1(c, h, d).start()

    def a1(self, c):
        for d in (1, -1):
            for h in (0, 1):
                i = 0 if d > 0 else 1
                self.c1(c, h, d).wait_recv()
                part = self.unit(c, h, d, None, i)
                for k in range(4):
                    part[k] = part[k] + self.landing(0, c, h, i)[k]
                self.c2(c, h, d).start()

    def a2(self, c):
        for h in (0, 1):
            for d in (1, -1):
                self.c2(c, h, d).wait_recv()
            whole = self.unit(c, h, 0)
            for k in range(4):
                whole[k] = (
                    whole[k].astype(F32) + self.r[1][c, h, 0, k].astype(F32) + self.r[1][c, h, 1, k].astype(F32)
                ).astype(BF)
            for d in (1, -1):
                self.c3(c, h, d).start()

    def a3(self, c):
        for d in (1, -1):
            for h in (0, 1):
                i = 0 if d > 0 else 1
                self.c3(c, h, d).wait_recv()
                part = self.unit(c, h, 0, d, i)
                part[...] = part[...] + self.landing(2, c, h, i)[...]
                self.c4(c, h, d).start()

    def a4(self, c):
        for h in (0, 1):
            for d in (1, -1):
                self.c4(c, h, d).wait_recv()
            own = self.unit(c, h, 0, 0)
            done = own[...].astype(F32) + self.r[3][c, h, 0].astype(F32) + self.r[3][c, h, 1].astype(F32)
            for k, out in enumerate(self.out):
                first, last = max(h * HALF, k * CHUNK), min((h + 1) * HALF, (k + 1) * CHUNK)
                if first < last:
                    at = slice(c * CHUNK + first - k * CHUNK, c * CHUNK + last - k * CHUNK)
                    out[at, :] = out[at, :] + done[first - h * HALF : last - h * HALF]

    def drain(self, c):
        for h in (0, 1):
            for d in (1, -1):
                for copy in (self.c1, self.c2, self.c3, self.c4):
                    copy(c, h, d).wait_send()


class TokenScatter:
    def __init__(self, t, p, rc, q, credit, send, recv):
        self.t, self.p, self.rc, self.q, self.credit = t, p, rc, q, credit
        self.send, self.recv = send, recv
        self.y, self.c = lax.axis_index("y"), lax.axis_index("c")

    def to(self, k):
        return lax.rem(self.y + k + 4, 4)

    def rows(self, k, core, sub=None):
        start, n = (self.to(k) * 2 + core) * SHARD, SHARD
        if sub is not None:
            start, n = start + sub * (SHARD // 2), SHARD // 2
        return self.p.at[pl.ds(pl.multiple_of(start, SHARD // 2), n), :]

    def landed(self, k):
        start = self.t * 4 * SHARD + self.to(k) * SHARD
        return self.rc.at[pl.ds(pl.multiple_of(start, SHARD), SHARD), :]

    def q1(self, i):
        start = self.t * 3 * SHARD + i * (SHARD // 2)
        return self.q.at[start : start + SHARD // 2, :]

    def q2(self, i):
        start = self.t * 3 * SHARD + (1 + i) * SHARD
        return self.q.at[start : start + SHARD, :]

    def pair(self, k):
        return pltpu.make_async_remote_copy(
            src_ref=self.rows(k, 1 - self.c),
            dst_ref=self.landed(k),
            send_sem=self.send.at[self.t, k % 4],
            recv_sem=self.recv.at[self.t, k % 4],
            device_id={"c": 1 - self.c},
            device_id_type=MESH,
        )

    def ring(self, src, dst, m, d):
        return pltpu.make_async_remote_copy(
            src_ref=src,
            dst_ref=dst,
            send_sem=self.send.at[self.t, m],
            recv_sem=self.recv.at[self.t, m],
            device_id={"y": self.to(d)},
            device_id_type=MESH,
        )

    def y1(self, d):
        i = 0 if d > 0 else 1
        return self.ring(self.rows(2, self.c, i), self.q1(i), 4 + i, d)

    def y2(self, d):
        i = 0 if d > 0 else 1
        return self.ring(self.rows(d, self.c), self.q2(i), 6 + i, d)

    def share(self, k):
        if self.t == 0 and k == 2:
            pl.semaphore_wait(self.credit.at[0], 1)
        self.pair(k).start()

    def join(self, k):
        self.pair(k).wait_recv()
        mine = self.rows(k, self.c)
        mine[...] = mine[...] + self.landed(k)[...]

    def far(self):
        self.join(2)
        for d in (1, -1):
            if self.t == 0:
                pl.semaphore_wait(self.credit.at[1 if d > 0 else 2], 1)
            self.y1(d).start()

    def near(self, d):
        i = 0 if d > 0 else 1
        self.join(d)
        self.y1(d).wait_recv()
        part = self.rows(d, self.c, i)
        part[...] = part[...] + self.q1(i)[...]
        self.y2(d).start()

    def finish(self):
        self.join(0)
        for d in (1, -1):
            self.y2(d).wait_recv()
        return (
            self.rows(0, self.c)[...].astype(F32) + self.q2(0)[...].astype(F32) + self.q2(1)[...].astype(F32)
        )

    def drain(self):
        for k in (0, 1, 2, -1):
            self.pair(k).wait_send()
        for d in (1, -1):
            self.y1(d).wait_send()
            self.y2(d).wait_send()


def butterfly():
    steps = [("c", 1 - lax.axis_index("c"))]
    for name in ("y", "x", "z"):
        me = lax.axis_index(name)
        steps.append((name, me + 1 - 2 * lax.rem(me, 2)))
        steps.append((name, 3 - me))
    return steps


class GainSum:
    def __init__(self, mine, theirs, send, recv):
        self.mine, self.theirs, self.send, self.recv = mine, theirs, send, recv
        self.steps = butterfly()

    def copy(self, i):
        name, partner = self.steps[i]
        return pltpu.make_async_remote_copy(
            src_ref=self.mine.at[i],
            dst_ref=self.theirs.at[i],
            send_sem=self.send.at[i],
            recv_sem=self.recv.at[i],
            device_id={name: partner},
            device_id_type=MESH,
        )

    def start(self, i):
        self.copy(i).start()

    def end(self, i):
        self.copy(i).wait_recv()
        self.mine[i + 1] = self.mine[i] + self.theirs[i]

    def drain(self):
        for i in range(7):
            self.copy(i).wait_send()


def sublayer(
    later_in, earlier_in, cot_in, gate_w, up_w, down_w, gain, gate_sum, up_sum, down_sum,
    later_out, hidden_out, earlier_out, gate_new, up_new, down_new, gain_out,
    w, g, nl, ne, cot, nlt, net, cott, hl, dx, he, hb, xb, r1, r2, r3, r4, dn, lrow, crow, gacc, gmine, gtheirs,
    in_sem, own_sem, wsend, wrecv, send, recv, tsend, trecv, gsend, grecv, credit, out_sem,
):
    tokens, width = nl.shape
    half = width // 2
    z, x, y, c_me = (lax.axis_index(n) for n in ALL)
    me = z * 4 + x
    own_rows = pl.ds(pl.multiple_of((y * 2 + c_me) * SHARD, SHARD), SHARD)
    mine = pl.ds(pl.multiple_of(me * SHARD, SHARD), SHARD)
    own = [
        pltpu.make_async_copy(
            ref.at[c * CHUNK : (c + 1) * CHUNK, :],
            w.at[c, k * CHUNK : (k + 1) * CHUNK, mine],
            own_sem.at[c, k],
        )
        for c in range(N_CHUNK)
        for k, ref in enumerate((gate_w, up_w, down_w))
    ]
    pairs = [
        (later_in, nl), (earlier_in, ne), (cot_in, cot),
        (gate_sum, gate_new), (up_sum, up_new), (down_sum, down_new),
        (later_in.at[own_rows, :], lrow), (cot_in.at[own_rows, :], crow),
    ]
    ins = [pltpu.make_async_copy(a, b, in_sem.at[i]) for i, (a, b) in enumerate(pairs)]
    for copy in own:
        copy.start()
    for copy in ins[:3]:
        copy.start()
    greet(ring_peers(("x", "z", "y")) + [{"c": 1 - c_me}])
    for copy in own:
        copy.wait()
    ring = Gather(w, wsend, wrecv)
    ring.t0(0)
    for copy in ins[3:]:
        copy.start()
    rs = Scatter(g, r1, r2, r3, r4, send, recv, (gate_new, up_new, down_new))
    later = TokenScatter(0, nl, net, cot, credit, tsend, trecv)
    earlier = TokenScatter(1, ne, net, cot, credit, tsend, trecv)
    total = GainSum(gmine, gtheirs, gsend, grecv)

    gain_row = gain[...].astype(F32)

    def turn_block(turned, ref, i):
        rows = pl.ds(pl.multiple_of(i * 128, 128), 128)
        for j in (0, 1):
            at = pl.ds(pl.multiple_of(i * 128 + j * tokens, 128), 128)
            turned[:, at] = ref[rows, j * half : (j + 1) * half].T

    def turned_cols(turned, i):
        return jnp.concatenate(
            [turned[:, j * tokens + i * 256 : j * tokens + (i + 1) * 256] for j in (0, 1)], axis=0
        )

    def norms(ref, first, last):
        @pl.loop(first, last)
        def _(i):
            rows = pl.ds(pl.multiple_of(i * 64, 64), 64)
            v = ref[rows, :].astype(F32)
            unit = v * lax.rsqrt(jnp.mean(v * v, axis=1, keepdims=True) + NORM_FLOOR)
            ref[rows, :] = (unit * gain_row).astype(BF)

    def turns(turned, ref, first, last):
        @pl.loop(first, last)
        def _(i):
            turn_block(turned, ref, i)

    blocks = tokens // 128

    ins[0].wait()
    norms(nl, 0, blocks)
    ring.t1(0)
    norms(nl, blocks, 2 * blocks)
    turns(nlt, nl, 0, blocks)
    ring.t2(0)
    ins[1].wait()
    norms(ne, 0, 2 * blocks)
    ring.t3(0)
    ring.t0(1)
    turns(net, ne, 0, blocks)
    ring.t4(0)
    ring.t1(1)
    ins[2].wait()
    turns(cott, cot, 0, blocks)
    ring.t5(0)
    ring.t2(1)
    for copy in ins[3:]:
        copy.wait()
    ring.t6(0)

    def tok_cols(i):
        return slice(i * 256, (i + 1) * 256)

    def later_item(c, i):
        pre = nn(w[c, : 2 * CHUNK, :], turned_cols(nlt, i))
        gate, up = pre[:CHUNK], pre[CHUNK:]
        hl[c * CHUNK : (c + 1) * CHUNK, tok_cols(i)] = (gate * jax.nn.sigmoid(gate) * up).astype(BF)

    def earlier_item(c, i):
        pre = nn(w[c, : 2 * CHUNK, :], turned_cols(net, i))
        dh = 0.5 * nn(w[c, 2 * CHUNK :, :], turned_cols(cott, i))
        gate, up = pre[:CHUNK], pre[CHUNK:]
        s = jax.nn.sigmoid(gate)
        act = gate * s
        he[:, tok_cols(i)] = (act * up).astype(BF)
        dx[c, :CHUNK, tok_cols(i)] = (dh * up * s * (1.0 + gate * (1.0 - s))).astype(BF)
        dx[c, CHUNK:, tok_cols(i)] = (dh * act).astype(BF)

    def grad_item(c, i):
        for j in (0, 1):
            cols = slice(i * 512 + j * 256, i * 512 + (j + 1) * 256)
            both = nn(dx[c], ne[:, cols]).astype(BF)
            down = (0.5 * nn(he[...], cot[:, cols])).astype(BF)
            for n in (0, 1):
                lanes = slice(n * SHARD, (n + 1) * SHARD)
                g[c, i, 2 * j + n, : 2 * CHUNK, :] = both[:, lanes]
                g[c, i, 2 * j + n, 2 * CHUNK :, :] = down[:, lanes]

    reload = pltpu.make_async_copy(earlier_in, cott, in_sem.at[8])

    def free():
        reload.start()
        pl.semaphore_signal(credit.at[0], inc=1, device_id={"c": 1 - c_me}, device_id_type=MESH)
        pl.semaphore_signal(credit.at[1], inc=1, device_id={"y": lax.rem(y + 3, 4)}, device_id_type=MESH)
        pl.semaphore_signal(credit.at[2], inc=1, device_id={"y": lax.rem(y + 1, 4)}, device_id_type=MESH)

    hidden = pltpu.make_async_copy(hl, hidden_out, out_sem)

    def token_cols(b):
        return pl.ds(pl.multiple_of(b * 256, 256), 256)

    def later_block(k):
        b = lax.rem(y + k + 4, 4)
        hb[...] = hl[:, token_cols(b)].T
        for n in range(width // 512):
            f = slice(n * 512, (n + 1) * 512)
            nl[token_cols(b), f] = nn(
                hb[...], jnp.concatenate([w[c, 2 * CHUNK :, f] for c in range(N_CHUNK)], axis=0)
            ).astype(BF)

    def earlier_block(k):
        b = lax.rem(y + k + 4, 4)
        for c in range(N_CHUNK):
            xb[c] = dx[c, :, token_cols(b)].T
        for n in range(width // 512):
            f = slice(n * 512, (n + 1) * 512)
            dn[:, f] = nn(xb[0], w[0, : 2 * CHUNK, f]) + nn(xb[1], w[1, : 2 * CHUNK, f])

        @pl.loop(0, 16)
        def _(i):
            at = pl.ds(pl.multiple_of(b * 256 + i * 16, 16), 16)
            v = cott[at, :].astype(F32)
            scale = lax.rsqrt(jnp.mean(v * v, axis=1, keepdims=True) + NORM_FLOOR)
            unit = v * scale
            d = dn[pl.ds(pl.multiple_of(i * 16, 16), 16), :]
            terms = d * unit
            gacc[...] += terms[:8] + terms[8:]
            mean = jnp.mean(terms * gain_row, axis=1, keepdims=True)
            ne[at, :] = (scale * (d * gain_row - unit * mean)).astype(BF)

        earlier.share(k)

    gacc[...] = jnp.zeros_like(gacc)
    for i in range(4):
        earlier_item(0, i)
        if i == 1:
            ring.t3(1)
    ring.t4(1)
    for i in range(4):
        grad_item(0, i)
        if i == 1:
            ring.t5(1)
    for i in range(4):
        later_item(0, i)
        if i == 1:
            rs.s1(0)
    ring.t6(1)
    for i in range(4):
        later_item(1, i)
    hidden.start()
    rs.a1(0)
    later_block(2)
    later_block(1)
    for i in range(4):
        earlier_item(1, i)
    rs.a2(0)
    for i in range(4):
        grad_item(1, i)
    free()
    rs.s1(1)
    later.share(2)
    later.share(1)
    later.far()
    reload.wait()
    earlier_block(2)
    later_block(-1)
    later.share(-1)
    earlier.far()
    later_block(0)
    later.share(0)
    rs.a3(0)
    earlier_block(1)
    later.near(1)
    later.near(-1)
    rs.a1(1)
    earlier_block(-1)
    earlier.near(1)
    earlier.near(-1)
    rs.a4(0)
    earlier_block(0)
    gmine[0] = jnp.sum(gacc[...], axis=0, keepdims=True)
    total.start(0)
    later_out[...] = (lrow[...].astype(F32) + 0.5 * later.finish()).astype(BF)
    total.end(0)
    total.start(1)
    rs.a2(1)
    total.end(1)
    total.start(2)
    rs.a3(1)
    total.end(2)
    total.start(3)
    earlier_out[...] = (crow[...].astype(F32) + earlier.finish()).astype(BF)
    total.end(3)
    total.start(4)
    rs.a4(1)
    for i in (4, 5):
        total.end(i)
        total.start(i + 1)
    total.end(6)
    gain_out[...] = gmine[7]
    for c in range(N_CHUNK):
        ring.drain(c)
        rs.drain(c)
    later.drain()
    earlier.drain()
    total.drain()
    hidden.wait()


def run(later_in, earlier_in, cot, gate_w, up_w, down_w, gain, gate_sum, up_sum, down_sum):
    tokens, width = later_in.shape
    cols, rows = gate_w.shape
    any_ = pl.BlockSpec(memory_space=pl.ANY)
    vm = pl.BlockSpec(memory_space=pltpu.VMEM)
    tok = (tokens, width)
    dma = pltpu.SemaphoreType.DMA
    return pl.pallas_call(
        sublayer,
        out_shape=[
            jax.ShapeDtypeStruct((tokens // 8, width), BF),
            jax.ShapeDtypeStruct((cols, tokens), BF),
            jax.ShapeDtypeStruct((tokens // 8, width), BF),
            jax.ShapeDtypeStruct((cols, rows), F32),
            jax.ShapeDtypeStruct((cols, rows), F32),
            jax.ShapeDtypeStruct((cols, rows), F32),
            jax.ShapeDtypeStruct((1, width), F32),
        ],
        in_specs=[any_] * 6 + [vm] + [any_] * 3,
        out_specs=[vm, any_] + [vm] * 5,
        scratch_shapes=[
            pltpu.VMEM((N_CHUNK, WIDE, width), BF),
            pltpu.VMEM((N_CHUNK, 4, 4, WIDE, SHARD), BF),
            *[pltpu.VMEM(tok, BF)] * 6,
            pltpu.VMEM((N_CHUNK * CHUNK, tokens), BF),
            pltpu.VMEM((N_CHUNK, 2 * CHUNK, tokens), BF),
            pltpu.VMEM((CHUNK, tokens), BF),
            pltpu.VMEM((256, 2 * CHUNK), BF),
            pltpu.VMEM((N_CHUNK, 256, 2 * CHUNK), BF),
            pltpu.VMEM((N_CHUNK, 2, 2, 4, CUT, SHARD), BF),
            pltpu.VMEM((N_CHUNK, 2, 2, 4, HALF, SHARD), BF),
            pltpu.VMEM((N_CHUNK, 2, 2, CUT, SHARD), BF),
            pltpu.VMEM((N_CHUNK, 2, 2, HALF, SHARD), BF),
            pltpu.VMEM((256, width), F32),
            pltpu.VMEM((SHARD, width), BF),
            pltpu.VMEM((SHARD, width), BF),
            pltpu.VMEM((8, width), F32),
            pltpu.VMEM((8, 1, width), F32),
            pltpu.VMEM((7, 1, width), F32),
            dma((9,)),
            dma((N_CHUNK, 3)),
            dma((N_CHUNK, 2, 20)),
            dma((N_CHUNK, 2, 20)),
            dma((N_CHUNK, 2, 8)),
            dma((N_CHUNK, 2, 8)),
            dma((2, 8)),
            dma((2, 8)),
            dma((7,)),
            dma((7,)),
            pltpu.SemaphoreType.REGULAR((3,)),
            dma,
        ],
        compiler_params=pltpu.CompilerParams(
            collective_id=0, has_side_effects=True, vmem_limit_bytes=64 * 1024 * 1024 - 65536
        ),
        name="sublayer",
    )(later_in, earlier_in, cot, gate_w, up_w, down_w, gain.reshape(1, width), gate_sum, up_sum, down_sum)


def local(later_in, earlier_in, cot, gate_w, up_w, down_w, gain, gate_sum, up_sum, down_sum, gain_sum):
    later_out, hidden, earlier_grad, gate_new, up_new, down_new, gain_total = run(
        later_in, earlier_in, cot, gate_w.T, up_w.T, down_w.T, gain, gate_sum.T, up_sum.T, down_sum.T
    )
    return (
        later_out, hidden.T, earlier_grad,
        gate_new.T, up_new.T, down_new.T, gain_sum + gain_total[0],
    )


def solution(mesh):
    torus = Mesh(mesh.devices.reshape(4, 4, 4, 2), ALL)
    return jax.shard_map(
        local,
        mesh=torus,
        in_specs=(P(FS, None),) * 3 + (P(FS, TP),) * 3 + (P(),) + (P(FS, TP),) * 3 + (P(),),
        out_specs=(P(ALL, None), P(FS, TP), P(ALL, None), P(FS, TP), P(FS, TP), P(FS, TP), P()),
        check_vma=False,
    )
```

```python
import functools

import jax
import jax.numpy as jnp
from jax import lax
from jax.experimental import pallas as pl
from jax.experimental.pallas import tpu as pltpu
from jax.sharding import Mesh
from jax.sharding import PartitionSpec as P

FS = ("z", "x")
TP = ("y", "c")
ALL = ("z", "x", "y", "c")
MESH = pl.DeviceIdType.MESH
BF = jnp.bfloat16
F32 = jnp.float32
SIZES = (192, 256, 256)
STARTS = (0, 192, 448)
N_CHUNK = 3
SHARD = 128
NORM_FLOOR = 0.05


def half_of(c):
    return SIZES[c] * 3 // 2


def span(c, h, sub=None):
    n = half_of(c)
    at = h * n
    return slice(at + (n // 2 if sub == 1 else 0), at + (n // 2 if sub == 0 else n))


class Gather:
    def __init__(self, w, send, recv):
        self.w, self.send, self.recv = w, send, recv
        self.mz, self.mx = lax.axis_index("z"), lax.axis_index("x")

    def owner(self, h, jf, js):
        dx, dz = (jf, js) if h == 0 else (js, jf)
        return lax.rem(self.mz + dz + 4, 4) * 4 + lax.rem(self.mx + dx + 4, 4)

    def copy(self, c, h, msg, jf, js, sub, axis, d):
        view = self.w[c].at[
            span(c, h, sub), pl.ds(pl.multiple_of(self.owner(h, jf, js) * SHARD, SHARD), SHARD)
        ]
        name = ("x", "z")[h] if axis == "f" else ("z", "x")[h]
        me = self.mx if name == "x" else self.mz
        return pltpu.make_async_remote_copy(
            src_ref=view,
            dst_ref=view,
            send_sem=self.send.at[c, h, msg],
            recv_sem=self.recv.at[c, h, msg],
            device_id={name: lax.rem(me + d + 4, 4)},
            device_id_type=MESH,
        )

    def m1(self, c, h, d):
        return self.copy(c, h, 0 if d > 0 else 1, 0, 0, None, "f", d)

    def r1(self, c, h, d):
        return self.copy(c, h, 0 if d > 0 else 1, -d, 0, None, "f", d)

    def m2(self, c, h, d):
        return self.copy(c, h, 2 if d > 0 else 3, -d, 0, 0 if d > 0 else 1, "f", d)

    def r2(self, c, h, d):
        return self.copy(c, h, 2 if d > 0 else 3, -2 * d, 0, 0 if d > 0 else 1, "f", d)

    def m3(self, c, h, j, d):
        return self.copy(c, h, 4 + 2 * (j % 4) + (0 if d > 0 else 1), j, 0, None, "s", d)

    def r3(self, c, h, j, d):
        return self.copy(c, h, 4 + 2 * (j % 4) + (0 if d > 0 else 1), j, -d, None, "s", d)

    def m4(self, c, h, j, d):
        return self.copy(c, h, 12 + 2 * (j % 4) + (0 if d > 0 else 1), j, -d, 0 if d > 0 else 1, "s", d)

    def r4(self, c, h, j, d):
        return self.copy(c, h, 12 + 2 * (j % 4) + (0 if d > 0 else 1), j, -2 * d, 0 if d > 0 else 1, "s", d)

    def t0(self, c):
        for h in (0, 1):
            for d in (1, -1):
                self.m1(c, h, d).start()
        for h in (0, 1):
            for d in (1, -1):
                self.m3(c, h, 0, d).start()

    def t1(self, c):
        for d in (1, -1):
            for h in (0, 1):
                self.r1(c, h, d).wait_recv()
                self.m2(c, h, d).start()
                for e in (1, -1):
                    self.m3(c, h, -d, e).start()

    def pass_on(self, c, js):
        for j in js:
            for d in (1, -1):
                for h in (0, 1):
                    self.r3(c, h, j, d).wait_recv()
                    self.m4(c, h, j, d).start()

    def t2(self, c):
        self.pass_on(c, (0,))

    def t3(self, c):
        for h in (0, 1):
            for d in (1, -1):
                self.r2(c, h, d).wait_recv()
            for e in (1, -1):
                self.m3(c, h, 2, e).start()

    def t4(self, c):
        self.pass_on(c, (-1, 1))

    def t5(self, c):
        self.pass_on(c, (2,))

    def t6(self, c):
        for h in (0, 1):
            for j in (0, -1, 1, 2):
                for d in (1, -1):
                    self.r4(c, h, j, d).wait_recv()

    def drain(self, c):
        for h in (0, 1):
            for d in (1, -1):
                self.m1(c, h, d).wait_send()
                self.m2(c, h, d).wait_send()
                for j in (0, -1, 1, 2):
                    self.m3(c, h, j, d).wait_send()
                    self.m4(c, h, j, d).wait_send()


def greet(peers):
    barrier = pltpu.get_barrier_semaphore()
    for peer in peers:
        pl.semaphore_signal(barrier, inc=1, device_id=peer, device_id_type=MESH)
    pl.semaphore_wait(barrier, len(peers))


def ring_peers(names):
    peers = []
    for name in names:
        me = lax.axis_index(name)
        for d in (1, 3):
            peers.append({name: lax.rem(me + d, 4)})
    return peers


def nn(a, b):
    return jnp.dot(a, b, preferred_element_type=F32)


class Scatter:
    def __init__(self, g, r, send, recv, out):
        self.g, self.r = g, r
        self.send, self.recv, self.out = send, recv, out
        self.at = {"z": lax.axis_index("z"), "x": lax.axis_index("x")}

    def unit(self, c, h, jf, js=None, sub=None):
        fast, slow = (("x", "z"), ("z", "x"))[h]
        f = lax.rem(self.at[fast] + jf + 4, 4)
        s = slice(None) if js is None else lax.rem(self.at[slow] + js + 4, 4)
        where = (s, f) if h == 0 else (f, s)
        return self.g[c].at[(*where, span(c, h, sub), slice(None))]

    def landing(self, stage, c, h, i):
        return self.r[c][stage].at[h, i]

    def copy(self, stage, c, h, d, src):
        i = 0 if d > 0 else 1
        name = (("x", "z"), ("z", "x"))[h][stage // 2]
        m = stage * 2 + i
        return pltpu.make_async_remote_copy(
            src_ref=src,
            dst_ref=self.landing(stage, c, h, i),
            send_sem=self.send.at[c, h, m],
            recv_sem=self.recv.at[c, h, m],
            device_id={name: lax.rem(self.at[name] + d + 4, 4)},
            device_id_type=MESH,
        )

    def c1(self, c, h, d):
        return self.copy(0, c, h, d, self.unit(c, h, 2, None, 0 if d > 0 else 1))

    def c2(self, c, h, d):
        return self.copy(1, c, h, d, self.unit(c, h, d))

    def c3(self, c, h, d):
        return self.copy(2, c, h, d, self.unit(c, h, 0, 2, 0 if d > 0 else 1))

    def c4(self, c, h, d):
        return self.copy(3, c, h, d, self.unit(c, h, 0, d))

    def s1(self, c):
        for h in (0, 1):
            for d in (1, -1):
                self.c1(c, h, d).start()

    def a1(self, c):
        for d in (1, -1):
            for h in (0, 1):
                i = 0 if d > 0 else 1
                self.c1(c, h, d).wait_recv()
                part = self.unit(c, h, d, None, i)
                for k in range(4):
                    part[k] = part[k] + self.landing(0, c, h, i)[k]
                self.c2(c, h, d).start()

    def a2(self, c):
        for h in (0, 1):
            for d in (1, -1):
                self.c2(c, h, d).wait_recv()
            whole = self.unit(c, h, 0)
            for k in range(4):
                whole[k] = (
                    whole[k].astype(F32)
                    + self.landing(1, c, h, 0)[k].astype(F32)
                    + self.landing(1, c, h, 1)[k].astype(F32)
                ).astype(BF)
            for d in (1, -1):
                self.c3(c, h, d).start()

    def a3(self, c):
        for d in (1, -1):
            for h in (0, 1):
                i = 0 if d > 0 else 1
                self.c3(c, h, d).wait_recv()
                part = self.unit(c, h, 0, d, i)
                part[...] = part[...] + self.landing(2, c, h, i)[...]
                self.c4(c, h, d).start()

    def a4(self, c):
        for h in (0, 1):
            for d in (1, -1):
                self.c4(c, h, d).wait_recv()
            own = self.unit(c, h, 0, 0)
            done = (
                own[...].astype(F32)
                + self.landing(3, c, h, 0)[...].astype(F32)
                + self.landing(3, c, h, 1)[...].astype(F32)
            )
            n, size = half_of(c), SIZES[c]
            for k, out in enumerate(self.out):
                first, last = max(h * n, k * size), min((h + 1) * n, (k + 1) * size)
                if first < last:
                    at = slice(STARTS[c] + first - k * size, STARTS[c] + last - k * size)
                    out[at, :] = out[at, :] + done[first - h * n : last - h * n]

    def drain(self, c):
        for h in (0, 1):
            for d in (1, -1):
                for copy in (self.c1, self.c2, self.c3, self.c4):
                    copy(c, h, d).wait_send()


class TokenScatter:
    def __init__(self, t, p, buf, credit, send, recv):
        self.t, self.p, self.buf, self.credit = t, p, buf, credit
        self.send, self.recv = send, recv
        self.y, self.c = lax.axis_index("y"), lax.axis_index("c")

    def to(self, k):
        return lax.rem(self.y + k + 4, 4)

    def rows(self, k, core, sub=None):
        start, n = (self.to(k) * 2 + core) * SHARD, SHARD
        if sub is not None:
            start, n = start + sub * (SHARD // 2), SHARD // 2
        return self.p.at[pl.ds(pl.multiple_of(start, SHARD // 2), n), :]

    def landed(self, k):
        return self.buf.at[pl.ds(pl.multiple_of(self.to(k) * SHARD, SHARD), SHARD), :]

    def q1(self, i):
        start = 4 * SHARD + i * (SHARD // 2)
        return self.buf.at[start : start + SHARD // 2, :]

    def q2(self, i):
        start = (5 + i) * SHARD
        return self.buf.at[start : start + SHARD, :]

    def ready(self):
        for i, peer in enumerate(({"c": 1 - self.c}, {"y": self.to(-1)}, {"y": self.to(1)})):
            pl.semaphore_signal(self.credit.at[self.t, i], inc=1, device_id=peer, device_id_type=MESH)

    def pair(self, k):
        return pltpu.make_async_remote_copy(
            src_ref=self.rows(k, 1 - self.c),
            dst_ref=self.landed(k),
            send_sem=self.send.at[self.t, k % 4],
            recv_sem=self.recv.at[self.t, k % 4],
            device_id={"c": 1 - self.c},
            device_id_type=MESH,
        )

    def ring(self, src, dst, m, d):
        return pltpu.make_async_remote_copy(
            src_ref=src,
            dst_ref=dst,
            send_sem=self.send.at[self.t, m],
            recv_sem=self.recv.at[self.t, m],
            device_id={"y": self.to(d)},
            device_id_type=MESH,
        )

    def y1(self, d):
        i = 0 if d > 0 else 1
        return self.ring(self.rows(2, self.c, i), self.q1(i), 4 + i, d)

    def y2(self, d):
        i = 0 if d > 0 else 1
        return self.ring(self.rows(d, self.c), self.q2(i), 6 + i, d)

    def share(self, k):
        if k == 2:
            pl.semaphore_wait(self.credit.at[self.t, 0], 1)
        self.pair(k).start()

    def join(self, k):
        self.pair(k).wait_recv()
        mine = self.rows(k, self.c)
        mine[...] = mine[...] + self.landed(k)[...]

    def far(self):
        self.join(2)
        for d in (1, -1):
            pl.semaphore_wait(self.credit.at[self.t, 1 if d > 0 else 2], 1)
            self.y1(d).start()

    def near(self, d):
        i = 0 if d > 0 else 1
        self.join(d)
        self.y1(d).wait_recv()
        part = self.rows(d, self.c, i)
        part[...] = part[...] + self.q1(i)[...]
        self.y2(d).start()

    def finish(self):
        self.join(0)
        for d in (1, -1):
            self.y2(d).wait_recv()
        return (
            self.rows(0, self.c)[...].astype(F32) + self.q2(0)[...].astype(F32) + self.q2(1)[...].astype(F32)
        )

    def drain(self):
        for k in (0, 1, 2, -1):
            self.pair(k).wait_send()
        for d in (1, -1):
            self.y1(d).wait_send()
            self.y2(d).wait_send()


def butterfly():
    steps = [("c", 1 - lax.axis_index("c"))]
    for name in ("y", "x", "z"):
        me = lax.axis_index(name)
        steps.append((name, me + 1 - 2 * lax.rem(me, 2)))
        steps.append((name, 3 - me))
    return steps


class GainSum:
    def __init__(self, mine, theirs, send, recv):
        self.mine, self.theirs, self.send, self.recv = mine, theirs, send, recv
        self.steps = butterfly()

    def copy(self, i):
        name, partner = self.steps[i]
        return pltpu.make_async_remote_copy(
            src_ref=self.mine.at[i],
            dst_ref=self.theirs.at[i],
            send_sem=self.send.at[i],
            recv_sem=self.recv.at[i],
            device_id={name: partner},
            device_id_type=MESH,
        )

    def start(self, i):
        self.copy(i).start()

    def end(self, i):
        self.copy(i).wait_recv()
        self.mine[i + 1] = self.mine[i] + self.theirs[i]

    def drain(self):
        for i in range(7):
            self.copy(i).wait_send()


def sublayer(
    later_in, earlier_in, cot_in, gate_w, up_w, down_w, gain, gate_sum, up_sum, down_sum,
    later_out, hidden_out, earlier_out, gate_new, up_new, down_new, gain_out,
    w, g, r, nl, ne, cot, nlt, net, cott, hl, dx, he, hb, xb, dn, lrow, crow, gacc, gmine, gtheirs,
    in_sem, own_sem, wsend, wrecv, send, recv, tsend, trecv, gsend, grecv, credit, out_sem,
):
    tokens, width = nl.shape
    half = width // 2
    z, x, y, c_me = (lax.axis_index(n) for n in ALL)
    me = z * 4 + x
    own_rows = pl.ds(pl.multiple_of((y * 2 + c_me) * SHARD, SHARD), SHARD)
    mine = pl.ds(pl.multiple_of(me * SHARD, SHARD), SHARD)
    own = [
        pltpu.make_async_copy(
            ref.at[STARTS[c] : STARTS[c] + SIZES[c], :],
            w[c].at[k * SIZES[c] : (k + 1) * SIZES[c], mine],
            own_sem.at[c, k],
        )
        for c in range(N_CHUNK)
        for k, ref in enumerate((gate_w, up_w, down_w))
    ]
    pairs = [
        (later_in, nl), (earlier_in, ne), (cot_in, cot),
        (gate_sum, gate_new), (up_sum, up_new), (down_sum, down_new),
        (later_in.at[own_rows, :], lrow), (cot_in.at[own_rows, :], crow),
    ]
    ins = [pltpu.make_async_copy(a, b, in_sem.at[i]) for i, (a, b) in enumerate(pairs)]
    for copy in own:
        copy.start()
    for copy in ins[:3]:
        copy.start()
    greet(ring_peers(("x", "z", "y")) + [{"c": 1 - c_me}])
    for copy in own:
        copy.wait()
    ring = Gather(w, wsend, wrecv)
    ring.t0(0)
    for copy in ins[3:]:
        copy.start()
    rs = Scatter(g, r, send, recv, (gate_new, up_new, down_new))
    later = TokenScatter(0, nl, nlt, credit, tsend, trecv)
    earlier = TokenScatter(1, ne, net, credit, tsend, trecv)
    total = GainSum(gmine, gtheirs, gsend, grecv)

    gain_row = gain[...].astype(F32)

    def turn_block(turned, ref, i):
        rows = pl.ds(pl.multiple_of(i * 128, 128), 128)
        for j in (0, 1):
            at = pl.ds(pl.multiple_of(i * 128 + j * tokens, 128), 128)
            turned[:, at] = ref[rows, j * half : (j + 1) * half].T

    def tok(i):
        return pl.ds(pl.multiple_of(i * 256, 256), 256)

    def turned_cols(turned, i):
        return jnp.concatenate(
            [turned[:, pl.ds(pl.multiple_of(i * 256 + j * tokens, 256), 256)] for j in (0, 1)], axis=0
        )

    def norms(ref, first, last):
        @pl.loop(first, last)
        def _(i):
            rows = pl.ds(pl.multiple_of(i * 64, 64), 64)
            v = ref[rows, :].astype(F32)
            unit = v * lax.rsqrt(jnp.mean(v * v, axis=1, keepdims=True) + NORM_FLOOR)
            ref[rows, :] = (unit * gain_row).astype(BF)

    def turns(turned, ref, first, last):
        @pl.loop(first, last)
        def _(i):
            turn_block(turned, ref, i)

    blocks = tokens // 128

    def looped(item, c, first, count):
        @pl.loop(first, first + count)
        def _(i):
            item(c, i)

    def later_item(c, i):
        n = SIZES[c]
        pre = nn(w[c][: 2 * n, :], turned_cols(nlt, i))
        gate, up = pre[:n], pre[n:]
        hl[STARTS[c] : STARTS[c] + n, tok(i)] = (gate * jax.nn.sigmoid(gate) * up).astype(BF)

    def earlier_item(c, i):
        n = SIZES[c]
        pre = nn(w[c][: 2 * n, :], turned_cols(net, i))
        dh = 0.5 * nn(w[c][2 * n :, :], turned_cols(cott, i))
        gate, up = pre[:n], pre[n:]
        s = jax.nn.sigmoid(gate)
        act = gate * s
        he[:n, tok(i)] = (act * up).astype(BF)
        dx[c][:n, tok(i)] = (dh * up * s * (1.0 + gate * (1.0 - s))).astype(BF)
        dx[c][n:, tok(i)] = (dh * act).astype(BF)

    def grad_item(c, i):
        n = SIZES[c]
        for j in (0, 1):
            cols = pl.ds(pl.multiple_of(i * 512 + j * 256, 256), 256)
            both = nn(dx[c][...], ne[:, cols]).astype(BF)
            down = (0.5 * nn(he[:n, :], cot[:, cols])).astype(BF)
            for m in (0, 1):
                lanes = slice(m * SHARD, (m + 1) * SHARD)
                g[c][i, 2 * j + m, : 2 * n, :] = both[:, lanes]
                g[c][i, 2 * j + m, 2 * n :, :] = down[:, lanes]

    L = functools.partial(looped, later_item)
    E = functools.partial(looped, earlier_item)
    G = functools.partial(looped, grad_item)

    reload = pltpu.make_async_copy(earlier_in, cott, in_sem.at[8])
    hidden = pltpu.make_async_copy(hl, hidden_out, out_sem)

    def features(n):
        return pl.ds(pl.multiple_of(n * 512, 512), 512)

    def later_block(k):
        b = lax.rem(y + k + 4, 4)
        hb[...] = hl[:, tok(b)].T

        @pl.loop(0, width // 512)
        def _(n):
            f = features(n)
            rows = [w[c][2 * SIZES[c] :, f] for c in range(N_CHUNK)]
            nl[tok(b), f] = nn(hb[...], jnp.concatenate(rows, axis=0)).astype(BF)

        later.share(k)

    def earlier_block(k):
        b = lax.rem(y + k + 4, 4)
        for c in range(N_CHUNK):
            xb[:, 2 * STARTS[c] : 2 * (STARTS[c] + SIZES[c])] = dx[c][:, tok(b)].T

        @pl.loop(0, width // 512)
        def _(n):
            f = features(n)
            rows = [w[c][: 2 * SIZES[c], f] for c in range(N_CHUNK)]
            dn[:, f] = nn(xb[...], jnp.concatenate(rows, axis=0))

        @pl.loop(0, 16)
        def _(i):
            at = pl.ds(pl.multiple_of(b * 256 + i * 16, 16), 16)
            v = cott[at, :].astype(F32)
            scale = lax.rsqrt(jnp.mean(v * v, axis=1, keepdims=True) + NORM_FLOOR)
            unit = v * scale
            d = dn[pl.ds(pl.multiple_of(i * 16, 16), 16), :]
            terms = d * unit
            gacc[...] += terms[:8] + terms[8:]
            mean = jnp.mean(terms * gain_row, axis=1, keepdims=True)
            ne[at, :] = (scale * (d * gain_row - unit * mean)).astype(BF)

        earlier.share(k)

    ins[0].wait()
    norms(nl, 0, blocks)
    ring.t1(0)
    norms(nl, blocks, 2 * blocks)
    turns(nlt, nl, 0, blocks // 2)
    ring.t2(0)
    turns(nlt, nl, blocks // 2, blocks)
    ring.t3(0)
    ring.t0(1)
    ins[1].wait()
    norms(ne, 0, 2 * blocks)
    ring.t4(0)
    turns(net, ne, 0, blocks)
    ring.t5(0)
    ring.t1(1)
    ins[2].wait()
    turns(cott, cot, 0, blocks)
    gacc[...] = jnp.zeros_like(gacc)
    for copy in ins[3:]:
        copy.wait()
    ring.t6(0)

    E(0, 0, 2)
    ring.t2(1)
    E(0, 2, 2)
    ring.t3(1)
    ring.t0(2)
    G(0, 0, 2)
    ring.t4(1)
    G(0, 2, 2)
    ring.t5(1)
    ring.t1(2)
    L(0, 0, 4)
    ring.t6(1)

    E(1, 0, 2)
    ring.t2(2)
    E(1, 2, 2)
    ring.t3(2)
    rs.s1(0)
    G(1, 0, 2)
    ring.t4(2)
    G(1, 2, 2)
    ring.t5(2)
    rs.s1(1)
    L(1, 0, 4)
    rs.a1(0)
    ring.t6(2)

    L(2, 0, 4)
    later.ready()
    hidden.start()
    later_block(2)
    later_block(1)
    rs.a1(1)
    later.far()
    E(2, 0, 2)
    rs.a2(0)
    E(2, 2, 2)
    earlier.ready()
    reload.start()
    G(2, 0, 4)
    rs.s1(2)
    later_block(-1)
    rs.a3(0)
    later_block(0)
    later.near(1)
    later.near(-1)
    reload.wait()
    earlier_block(2)
    rs.a1(2)
    rs.a2(1)
    earlier_block(1)
    earlier.far()
    rs.a4(0)
    earlier_block(-1)
    rs.a3(1)
    earlier_block(0)
    gmine[0] = jnp.sum(gacc[...], axis=0, keepdims=True)
    total.start(0)
    total.end(0)
    total.start(1)
    later_out[...] = (lrow[...].astype(F32) + 0.5 * later.finish()).astype(BF)
    total.end(1)
    total.start(2)
    earlier.near(1)
    earlier.near(-1)
    total.end(2)
    total.start(3)
    rs.a2(2)
    total.end(3)
    total.start(4)
    rs.a3(2)
    rs.a4(1)
    total.end(4)
    total.start(5)
    rs.a4(2)
    total.end(5)
    total.start(6)
    earlier_out[...] = (crow[...].astype(F32) + earlier.finish()).astype(BF)
    total.end(6)
    gain_out[...] = gmine[7]
    for c in range(N_CHUNK):
        ring.drain(c)
        rs.drain(c)
    later.drain()
    earlier.drain()
    total.drain()
    hidden.wait()


def run(later_in, earlier_in, cot, gate_w, up_w, down_w, gain, gate_sum, up_sum, down_sum):
    tokens, width = later_in.shape
    cols, rows = gate_w.shape
    any_ = pl.BlockSpec(memory_space=pl.ANY)
    vm = pl.BlockSpec(memory_space=pltpu.VMEM)
    tok = (tokens, width)
    dma = pltpu.SemaphoreType.DMA
    return pl.pallas_call(
        sublayer,
        out_shape=[
            jax.ShapeDtypeStruct((tokens // 8, width), BF),
            jax.ShapeDtypeStruct((cols, tokens), BF),
            jax.ShapeDtypeStruct((tokens // 8, width), BF),
            jax.ShapeDtypeStruct((cols, rows), F32),
            jax.ShapeDtypeStruct((cols, rows), F32),
            jax.ShapeDtypeStruct((cols, rows), F32),
            jax.ShapeDtypeStruct((1, width), F32),
        ],
        in_specs=[any_] * 6 + [vm] + [any_] * 3,
        out_specs=[vm, any_] + [vm] * 5,
        scratch_shapes=[
            [pltpu.VMEM((3 * n, width), BF) for n in SIZES],
            [pltpu.VMEM((4, 4, 3 * n, SHARD), BF) for n in SIZES],
            [
                [
                    pltpu.VMEM((2, 2, 4, half_of(c) // 2, SHARD), BF),
                    pltpu.VMEM((2, 2, 4, half_of(c), SHARD), BF),
                    pltpu.VMEM((2, 2, half_of(c) // 2, SHARD), BF),
                    pltpu.VMEM((2, 2, half_of(c), SHARD), BF),
                ]
                for c in range(N_CHUNK)
            ],
            *[pltpu.VMEM(tok, BF)] * 6,
            pltpu.VMEM((cols, tokens), BF),
            [pltpu.VMEM((2 * n, tokens), BF) for n in SIZES],
            pltpu.VMEM((max(SIZES), tokens), BF),
            pltpu.VMEM((256, cols), BF),
            pltpu.VMEM((256, 2 * cols), BF),
            pltpu.VMEM((256, width), F32),
            pltpu.VMEM((SHARD, width), BF),
            pltpu.VMEM((SHARD, width), BF),
            pltpu.VMEM((8, width), F32),
            pltpu.VMEM((8, 1, width), F32),
            pltpu.VMEM((7, 1, width), F32),
            dma((9,)),
            dma((N_CHUNK, 3)),
            dma((N_CHUNK, 2, 20)),
            dma((N_CHUNK, 2, 20)),
            dma((N_CHUNK, 2, 8)),
            dma((N_CHUNK, 2, 8)),
            dma((2, 8)),
            dma((2, 8)),
            dma((7,)),
            dma((7,)),
            pltpu.SemaphoreType.REGULAR((2, 3)),
            dma,
        ],
        compiler_params=pltpu.CompilerParams(
            collective_id=0, has_side_effects=True, vmem_limit_bytes=64 * 1024 * 1024 - 65536
        ),
        name="sublayer",
    )(later_in, earlier_in, cot, gate_w, up_w, down_w, gain.reshape(1, width), gate_sum, up_sum, down_sum)


def local(later_in, earlier_in, cot, gate_w, up_w, down_w, gain, gate_sum, up_sum, down_sum, gain_sum):
    later_out, hidden, earlier_grad, gate_new, up_new, down_new, gain_total = run(
        later_in, earlier_in, cot, gate_w.T, up_w.T, down_w.T, gain, gate_sum.T, up_sum.T, down_sum.T
    )
    return (
        later_out, hidden.T, earlier_grad,
        gate_new.T, up_new.T, down_new.T, gain_sum + gain_total[0],
    )


def solution(mesh):
    torus = Mesh(mesh.devices.reshape(4, 4, 4, 2), ALL)
    return jax.shard_map(
        local,
        mesh=torus,
        in_specs=(P(FS, None),) * 3 + (P(FS, TP),) * 3 + (P(),) + (P(FS, TP),) * 3 + (P(),),
        out_specs=(P(ALL, None), P(FS, TP), P(ALL, None), P(FS, TP), P(FS, TP), P(FS, TP), P()),
        check_vma=False,
    )
```

```python
import functools

import jax
import jax.numpy as jnp
from jax import lax
from jax.experimental import pallas as pl
from jax.experimental.pallas import tpu as pltpu
from jax.sharding import Mesh
from jax.sharding import PartitionSpec as P

FS = ("z", "x")
TP = ("y", "c")
ALL = ("z", "x", "y", "c")
MESH = pl.DeviceIdType.MESH
BF = jnp.bfloat16
F32 = jnp.float32
SIZES = (192, 256, 256)
STARTS = (0, 192, 448)
N_CHUNK = 3
SHARD = 128
NORM_FLOOR = 0.05


def half_of(c):
    return SIZES[c] * 3 // 2


def span(c, h, sub=None):
    n = half_of(c)
    at = h * n
    return slice(at + (n // 2 if sub == 1 else 0), at + (n // 2 if sub == 0 else n))


class Gather:
    def __init__(self, w, send, recv):
        self.w, self.send, self.recv = w, send, recv
        self.mz, self.mx = lax.axis_index("z"), lax.axis_index("x")

    def owner(self, h, jf, js):
        dx, dz = (jf, js) if h == 0 else (js, jf)
        return lax.rem(self.mz + dz + 4, 4) * 4 + lax.rem(self.mx + dx + 4, 4)

    def copy(self, c, h, msg, jf, js, sub, axis, d):
        view = self.w[c].at[
            span(c, h, sub), pl.ds(pl.multiple_of(self.owner(h, jf, js) * SHARD, SHARD), SHARD)
        ]
        name = ("x", "z")[h] if axis == "f" else ("z", "x")[h]
        me = self.mx if name == "x" else self.mz
        return pltpu.make_async_remote_copy(
            src_ref=view,
            dst_ref=view,
            send_sem=self.send.at[c, h, msg],
            recv_sem=self.recv.at[c, h, msg],
            device_id={name: lax.rem(me + d + 4, 4)},
            device_id_type=MESH,
        )

    def m1(self, c, h, d):
        return self.copy(c, h, 0 if d > 0 else 1, 0, 0, None, "f", d)

    def r1(self, c, h, d):
        return self.copy(c, h, 0 if d > 0 else 1, -d, 0, None, "f", d)

    def m2(self, c, h, d):
        return self.copy(c, h, 2 if d > 0 else 3, -d, 0, 0 if d > 0 else 1, "f", d)

    def r2(self, c, h, d):
        return self.copy(c, h, 2 if d > 0 else 3, -2 * d, 0, 0 if d > 0 else 1, "f", d)

    def m3(self, c, h, j, d):
        return self.copy(c, h, 4 + 2 * (j % 4) + (0 if d > 0 else 1), j, 0, None, "s", d)

    def r3(self, c, h, j, d):
        return self.copy(c, h, 4 + 2 * (j % 4) + (0 if d > 0 else 1), j, -d, None, "s", d)

    def m4(self, c, h, j, d):
        return self.copy(c, h, 12 + 2 * (j % 4) + (0 if d > 0 else 1), j, -d, 0 if d > 0 else 1, "s", d)

    def r4(self, c, h, j, d):
        return self.copy(c, h, 12 + 2 * (j % 4) + (0 if d > 0 else 1), j, -2 * d, 0 if d > 0 else 1, "s", d)

    def t0(self, c):
        for h in (0, 1):
            for d in (1, -1):
                self.m1(c, h, d).start()
        for h in (0, 1):
            for d in (1, -1):
                self.m3(c, h, 0, d).start()

    def t1(self, c, h, d):
        self.r1(c, h, d).wait_recv()
        self.m2(c, h, d).start()
        for e in (1, -1):
            self.m3(c, h, -d, e).start()

    def t3(self, c, h):
        for d in (1, -1):
            self.r2(c, h, d).wait_recv()
        for e in (1, -1):
            self.m3(c, h, 2, e).start()

    def hand(self, c, h, j, d):
        self.r3(c, h, j, d).wait_recv()
        self.m4(c, h, j, d).start()

    def t6(self, c):
        for h in (0, 1):
            for j in (0, -1, 1, 2):
                for d in (1, -1):
                    self.r4(c, h, j, d).wait_recv()

    def drain(self, c):
        for h in (0, 1):
            for d in (1, -1):
                self.m1(c, h, d).wait_send()
                self.m2(c, h, d).wait_send()
                for j in (0, -1, 1, 2):
                    self.m3(c, h, j, d).wait_send()
                    self.m4(c, h, j, d).wait_send()


def greet(peers):
    barrier = pltpu.get_barrier_semaphore()
    for peer in peers:
        pl.semaphore_signal(barrier, inc=1, device_id=peer, device_id_type=MESH)
    pl.semaphore_wait(barrier, len(peers))


def ring_peers(names):
    peers = []
    for name in names:
        me = lax.axis_index(name)
        for d in (1, 3):
            peers.append({name: lax.rem(me + d, 4)})
    return peers


def nn(a, b):
    return jnp.dot(a, b, preferred_element_type=F32)


class Scatter:
    def __init__(self, g, r, send, recv, out):
        self.g, self.r = g, r
        self.send, self.recv, self.out = send, recv, out
        self.at = {"z": lax.axis_index("z"), "x": lax.axis_index("x")}

    def unit(self, c, h, jf, js=None, sub=None):
        fast, slow = (("x", "z"), ("z", "x"))[h]
        f = lax.rem(self.at[fast] + jf + 4, 4)
        s = slice(None) if js is None else lax.rem(self.at[slow] + js + 4, 4)
        where = (s, f) if h == 0 else (f, s)
        return self.g[c].at[(*where, span(c, h, sub), slice(None))]

    def landing(self, stage, c, h, i):
        return self.r[c][stage].at[h, i]

    def copy(self, stage, c, h, d, src):
        i = 0 if d > 0 else 1
        name = (("x", "z"), ("z", "x"))[h][stage // 2]
        m = stage * 2 + i
        return pltpu.make_async_remote_copy(
            src_ref=src,
            dst_ref=self.landing(stage, c, h, i),
            send_sem=self.send.at[c, h, m],
            recv_sem=self.recv.at[c, h, m],
            device_id={name: lax.rem(self.at[name] + d + 4, 4)},
            device_id_type=MESH,
        )

    def c1(self, c, h, d):
        return self.copy(0, c, h, d, self.unit(c, h, 2, None, 0 if d > 0 else 1))

    def c2(self, c, h, d):
        return self.copy(1, c, h, d, self.unit(c, h, d))

    def c3(self, c, h, d):
        return self.copy(2, c, h, d, self.unit(c, h, 0, 2, 0 if d > 0 else 1))

    def c4(self, c, h, d):
        return self.copy(3, c, h, d, self.unit(c, h, 0, d))

    def s1(self, c):
        for h in (0, 1):
            for d in (1, -1):
                self.c1(c, h, d).start()

    def a1(self, c, h, d):
        i = 0 if d > 0 else 1
        self.c1(c, h, d).wait_recv()
        part = self.unit(c, h, d, None, i)
        for k in range(4):
            part[k] = part[k] + self.landing(0, c, h, i)[k]
        self.c2(c, h, d).start()

    def a2(self, c, h):
        for d in (1, -1):
            self.c2(c, h, d).wait_recv()
        whole = self.unit(c, h, 0)
        for k in range(4):
            whole[k] = (
                whole[k].astype(F32)
                + self.landing(1, c, h, 0)[k].astype(F32)
                + self.landing(1, c, h, 1)[k].astype(F32)
            ).astype(BF)
        for d in (1, -1):
            self.c3(c, h, d).start()

    def a3(self, c, h, d):
        i = 0 if d > 0 else 1
        self.c3(c, h, d).wait_recv()
        part = self.unit(c, h, 0, d, i)
        part[...] = part[...] + self.landing(2, c, h, i)[...]
        self.c4(c, h, d).start()

    def a4(self, c, h):
        for d in (1, -1):
            self.c4(c, h, d).wait_recv()
        own = self.unit(c, h, 0, 0)
        done = (
            own[...].astype(F32)
            + self.landing(3, c, h, 0)[...].astype(F32)
            + self.landing(3, c, h, 1)[...].astype(F32)
        )
        n, size = half_of(c), SIZES[c]
        for k, out in enumerate(self.out):
            first, last = max(h * n, k * size), min((h + 1) * n, (k + 1) * size)
            if first < last:
                at = slice(STARTS[c] + first - k * size, STARTS[c] + last - k * size)
                out[at, :] = out[at, :] + done[first - h * n : last - h * n]

    def drain(self, c):
        for h in (0, 1):
            for d in (1, -1):
                for copy in (self.c1, self.c2, self.c3, self.c4):
                    copy(c, h, d).wait_send()


class TokenScatter:
    def __init__(self, t, p, buf, credit, send, recv):
        self.t, self.p, self.buf, self.credit = t, p, buf, credit
        self.send, self.recv = send, recv
        self.y, self.c = lax.axis_index("y"), lax.axis_index("c")

    def to(self, k):
        return lax.rem(self.y + k + 4, 4)

    def rows(self, k, core, sub=None):
        start, n = (self.to(k) * 2 + core) * SHARD, SHARD
        if sub is not None:
            start, n = start + sub * (SHARD // 2), SHARD // 2
        return self.p.at[pl.ds(pl.multiple_of(start, SHARD // 2), n), :]

    def landed(self, k):
        return self.buf.at[pl.ds(pl.multiple_of(self.to(k) * SHARD, SHARD), SHARD), :]

    def q1(self, i):
        start = 4 * SHARD + i * (SHARD // 2)
        return self.buf.at[start : start + SHARD // 2, :]

    def q2(self, i):
        start = (5 + i) * SHARD
        return self.buf.at[start : start + SHARD, :]

    def ready(self):
        for i, peer in enumerate(({"c": 1 - self.c}, {"y": self.to(-1)}, {"y": self.to(1)})):
            pl.semaphore_signal(self.credit.at[self.t, i], inc=1, device_id=peer, device_id_type=MESH)

    def pair(self, k):
        return pltpu.make_async_remote_copy(
            src_ref=self.rows(k, 1 - self.c),
            dst_ref=self.landed(k),
            send_sem=self.send.at[self.t, k % 4],
            recv_sem=self.recv.at[self.t, k % 4],
            device_id={"c": 1 - self.c},
            device_id_type=MESH,
        )

    def ring(self, src, dst, m, d):
        return pltpu.make_async_remote_copy(
            src_ref=src,
            dst_ref=dst,
            send_sem=self.send.at[self.t, m],
            recv_sem=self.recv.at[self.t, m],
            device_id={"y": self.to(d)},
            device_id_type=MESH,
        )

    def y1(self, d):
        i = 0 if d > 0 else 1
        return self.ring(self.rows(2, self.c, i), self.q1(i), 4 + i, d)

    def y2(self, d):
        i = 0 if d > 0 else 1
        return self.ring(self.rows(d, self.c), self.q2(i), 6 + i, d)

    def share(self, k):
        if k == 2:
            pl.semaphore_wait(self.credit.at[self.t, 0], 1)
        self.pair(k).start()

    def join(self, k):
        self.pair(k).wait_recv()
        mine = self.rows(k, self.c)
        mine[...] = mine[...] + self.landed(k)[...]

    def far(self):
        self.join(2)
        for d in (1, -1):
            pl.semaphore_wait(self.credit.at[self.t, 1 if d > 0 else 2], 1)
            self.y1(d).start()

    def near(self, d):
        i = 0 if d > 0 else 1
        self.join(d)
        self.y1(d).wait_recv()
        part = self.rows(d, self.c, i)
        part[...] = part[...] + self.q1(i)[...]
        self.y2(d).start()

    def finish(self):
        self.join(0)
        for d in (1, -1):
            self.y2(d).wait_recv()
        return (
            self.rows(0, self.c)[...].astype(F32) + self.q2(0)[...].astype(F32) + self.q2(1)[...].astype(F32)
        )

    def drain(self):
        for k in (0, 1, 2, -1):
            self.pair(k).wait_send()
        for d in (1, -1):
            self.y1(d).wait_send()
            self.y2(d).wait_send()


class GainSum:
    AXES = (("c", 2), ("x", 4), ("z", 4), ("y", 4))

    def __init__(self, rows, send, recv):
        self.rows, self.send, self.recv = rows, send, recv

    def copy(self, i, d, arriving):
        name, n = self.AXES[i]
        me = lax.axis_index(name)
        src = lax.rem(me + n - d, n) if arriving else me
        return pltpu.make_async_remote_copy(
            src_ref=self.rows.at[i, src],
            dst_ref=self.rows.at[i, src],
            send_sem=self.send.at[i, d],
            recv_sem=self.recv.at[i, d],
            device_id={name: lax.rem(me + d, n)},
            device_id_type=MESH,
        )

    def start(self, i, row):
        name, n = self.AXES[i]
        self.rows[i, lax.axis_index(name)] = row
        for d in range(1, n):
            self.copy(i, d, False).start()

    def end(self, i):
        n = self.AXES[i][1]
        for d in range(1, n):
            self.copy(i, d, True).wait_recv()
        row = self.rows[i, 0]
        for k in range(1, n):
            row = row + self.rows[i, k]
        return row

    def drain(self):
        for i, (_, n) in enumerate(self.AXES):
            for d in range(1, n):
                self.copy(i, d, False).wait_send()


def sublayer(
    later_in, earlier_in, cot_in, gate_w, up_w, down_w, gain, gate_sum, up_sum, down_sum,
    later_out, hidden_out, earlier_out, gate_new, up_new, down_new, gain_out,
    w, g, r, nl, ne, cot, nlt, net, cott, hl, dx, he, hb, xb, dn, lrow, crow, gacc, grows,
    in_sem, own_sem, wsend, wrecv, send, recv, tsend, trecv, gsend, grecv, credit, out_sem,
):
    tokens, width = nl.shape
    half = width // 2
    z, x, y, c_me = (lax.axis_index(n) for n in ALL)
    me = z * 4 + x
    own_rows = pl.ds(pl.multiple_of((y * 2 + c_me) * SHARD, SHARD), SHARD)
    mine = pl.ds(pl.multiple_of(me * SHARD, SHARD), SHARD)
    own = [
        pltpu.make_async_copy(
            ref.at[STARTS[c] : STARTS[c] + SIZES[c], :],
            w[c].at[k * SIZES[c] : (k + 1) * SIZES[c], mine],
            own_sem.at[c, k],
        )
        for c in range(N_CHUNK)
        for k, ref in enumerate((gate_w, up_w, down_w))
    ]
    pairs = [
        (later_in, nl), (earlier_in, ne), (cot_in, cot),
        (gate_sum, gate_new), (up_sum, up_new), (down_sum, down_new),
        (later_in.at[own_rows, :], lrow), (cot_in.at[own_rows, :], crow),
    ]
    ins = [pltpu.make_async_copy(a, b, in_sem.at[i]) for i, (a, b) in enumerate(pairs)]
    for copy in own:
        copy.start()
    for copy in ins[:3]:
        copy.start()
    across = [{n: lax.rem(lax.axis_index(n) + 2, 4)} for n in ("x", "z", "y")]
    greet(ring_peers(("x", "z", "y")) + [{"c": 1 - c_me}] + across)
    for copy in own:
        copy.wait()
    ring = Gather(w, wsend, wrecv)
    ring.t0(0)
    for copy in ins[3:]:
        copy.start()
    rs = Scatter(g, r, send, recv, (gate_new, up_new, down_new))
    later = TokenScatter(0, nl, nlt, credit, tsend, trecv)
    earlier = TokenScatter(1, ne, net, credit, tsend, trecv)
    total = GainSum(grows, gsend, grecv)

    gain_row = gain[...].astype(F32)

    def turn_block(turned, ref, i):
        rows = pl.ds(pl.multiple_of(i * 128, 128), 128)
        for j in (0, 1):
            at = pl.ds(pl.multiple_of(i * 128 + j * tokens, 128), 128)
            turned[:, at] = ref[rows, j * half : (j + 1) * half].T

    def tok(i):
        return pl.ds(pl.multiple_of(i * 256, 256), 256)

    def turned_cols(turned, i):
        return jnp.concatenate(
            [turned[:, pl.ds(pl.multiple_of(i * 256 + j * tokens, 256), 256)] for j in (0, 1)], axis=0
        )

    def norms(ref, first, last):
        @pl.loop(first, last)
        def _(i):
            rows = pl.ds(pl.multiple_of(i * 64, 64), 64)
            v = ref[rows, :].astype(F32)
            unit = v * lax.rsqrt(jnp.mean(v * v, axis=1, keepdims=True) + NORM_FLOOR)
            ref[rows, :] = (unit * gain_row).astype(BF)

    def turns(turned, ref, first, last):
        @pl.loop(first, last)
        def _(i):
            turn_block(turned, ref, i)

    blocks = tokens // 128

    def looped(item, c, first, count):
        @pl.loop(first, first + count)
        def _(i):
            item(c, i)

    def later_item(c, i):
        n = SIZES[c]
        pre = nn(w[c][: 2 * n, :], turned_cols(nlt, i))
        gate, up = pre[:n], pre[n:]
        hl[STARTS[c] : STARTS[c] + n, tok(i)] = (gate * jax.nn.sigmoid(gate) * up).astype(BF)

    def earlier_item(c, i):
        n = SIZES[c]
        pre = nn(w[c][: 2 * n, :], turned_cols(net, i))
        dh = 0.5 * nn(w[c][2 * n :, :], turned_cols(cott, i))
        gate, up = pre[:n], pre[n:]
        s = jax.nn.sigmoid(gate)
        act = gate * s
        he[:n, tok(i)] = (act * up).astype(BF)
        dx[c][:n, tok(i)] = (dh * up * s * (1.0 + gate * (1.0 - s))).astype(BF)
        dx[c][n:, tok(i)] = (dh * act).astype(BF)

    def grad_item(c, i):
        n = SIZES[c]
        for j in (0, 1):
            cols = pl.ds(pl.multiple_of(i * 512 + j * 256, 256), 256)
            both = nn(dx[c][...], ne[:, cols]).astype(BF)
            down = (0.5 * nn(he[:n, :], cot[:, cols])).astype(BF)
            for m in (0, 1):
                lanes = slice(m * SHARD, (m + 1) * SHARD)
                g[c][i, 2 * j + m, : 2 * n, :] = both[:, lanes]
                g[c][i, 2 * j + m, 2 * n :, :] = down[:, lanes]

    L = functools.partial(looped, later_item)
    E = functools.partial(looped, earlier_item)
    G = functools.partial(looped, grad_item)

    reload = pltpu.make_async_copy(earlier_in, cott, in_sem.at[8])
    hidden = pltpu.make_async_copy(hl, hidden_out, out_sem)

    def features(n):
        return pl.ds(pl.multiple_of(n * 512, 512), 512)

    def later_block(k):
        b = lax.rem(y + k + 4, 4)
        hb[...] = hl[:, tok(b)].T

        @pl.loop(0, width // 512)
        def _(n):
            f = features(n)
            rows = [w[c][2 * SIZES[c] :, f] for c in range(N_CHUNK)]
            nl[tok(b), f] = nn(hb[...], jnp.concatenate(rows, axis=0)).astype(BF)

        later.share(k)

    def earlier_block(k):
        b = lax.rem(y + k + 4, 4)
        for c in range(N_CHUNK):
            xb[:, 2 * STARTS[c] : 2 * (STARTS[c] + SIZES[c])] = dx[c][:, tok(b)].T

        @pl.loop(0, width // 512)
        def _(n):
            f = features(n)
            rows = [w[c][: 2 * SIZES[c], f] for c in range(N_CHUNK)]
            dn[:, f] = nn(xb[...], jnp.concatenate(rows, axis=0))

        @pl.loop(0, 16)
        def _(i):
            at = pl.ds(pl.multiple_of(b * 256 + i * 16, 16), 16)
            v = cott[at, :].astype(F32)
            scale = lax.rsqrt(jnp.mean(v * v, axis=1, keepdims=True) + NORM_FLOOR)
            unit = v * scale
            d = dn[pl.ds(pl.multiple_of(i * 16, 16), 16), :]
            terms = d * unit
            gacc[...] += terms[:8] + terms[8:]
            mean = jnp.mean(terms * gain_row, axis=1, keepdims=True)
            ne[at, :] = (scale * (d * gain_row - unit * mean)).astype(BF)

        earlier.share(k)

    def gain_step(i):
        row = total.end(i - 1) if i else jnp.sum(gacc[...], axis=0, keepdims=True)
        if i < 4:
            total.start(i, row)
        else:
            gain_out[...] = row

    def later_end():
        later_out[...] = (lrow[...].astype(F32) + 0.5 * later.finish()).astype(BF)

    def earlier_end():
        earlier_out[...] = (crow[...].astype(F32) + earlier.finish()).astype(BF)

    gacc[...] = jnp.zeros_like(gacc)
    ins[0].wait()
    norms(nl, 0, blocks)
    norms(nl, blocks, 2 * blocks)
    ins[1].wait()
    norms(ne, 0, blocks)
    ring.t1(0,0,1)
    ring.t1(0,0,-1)
    ring.t1(0,1,1)
    ring.t1(0,1,-1)
    turns(nlt, nl, 0, blocks // 2)
    ring.hand(0,0,0,1)
    ring.hand(0,0,0,-1)
    ring.hand(0,1,0,1)
    ring.hand(0,1,0,-1)
    turns(nlt, nl, blocks // 2, blocks)
    ring.t3(0,0)
    ring.hand(0,0,-1,1)
    ring.hand(0,0,-1,-1)
    norms(ne, blocks, 2 * blocks)
    ring.hand(0,0,1,1)
    ring.hand(0,0,1,-1)
    ring.hand(0,1,-1,1)
    ring.hand(0,1,-1,-1)
    ring.t3(0,1)
    ring.hand(0,1,1,1)
    ring.hand(0,1,1,-1)
    ring.t0(1)
    turns(net, ne, 0, blocks // 2)
    turns(net, ne, blocks // 2, blocks)
    ring.hand(0,0,2,1)
    ring.hand(0,0,2,-1)
    ins[2].wait()
    turns(cott, cot, 0, blocks // 2)
    ring.t1(1,1,1)
    ring.t1(1,1,-1)
    ring.hand(0,1,2,1)
    ring.hand(0,1,2,-1)
    turns(cott, cot, blocks // 2, blocks)
    ring.t1(1,0,1)
    ring.t1(1,0,-1)
    ring.hand(1,0,0,1)
    ring.hand(1,0,0,-1)
    ring.hand(1,1,0,1)
    ring.hand(1,1,0,-1)
    ring.t3(1,1)
    ring.hand(1,1,-1,1)
    ring.hand(1,1,-1,-1)
    ring.hand(1,0,-1,-1)
    ring.hand(1,0,-1,1)
    ring.hand(1,1,1,1)
    ring.hand(1,1,1,-1)
    ring.t6(0)
    L(0, 3, 1)
    ring.hand(1,0,1,1)
    ring.hand(1,0,1,-1)
    E(0, 0, 1)
    ring.t3(1,0)
    ring.t0(2)
    L(0, 0, 1)
    L(0, 2, 1)
    E(0, 1, 1)
    L(0, 1, 1)
    E(0, 2, 1)
    ring.hand(1,1,2,1)
    ring.hand(1,1,2,-1)
    E(0, 3, 1)
    G(0, 1, 1)
    G(0, 0, 1)
    ring.hand(1,0,2,1)
    ring.hand(1,0,2,-1)
    G(0, 2, 2)
    ring.t1(2,1,1)
    ring.t1(2,1,-1)
    ring.t1(2,0,1)
    ring.t1(2,0,-1)
    ring.hand(2,0,0,1)
    ring.hand(2,0,0,-1)
    ring.hand(2,1,0,1)
    ring.hand(2,1,0,-1)
    for copy in ins[3:]:
        copy.wait()
    ring.t6(1)
    E(1, 0, 1)
    ring.t3(2,1)
    L(1, 0, 1)
    E(1, 2, 1)
    ring.hand(2,1,-1,1)
    ring.hand(2,1,-1,-1)
    L(1, 3, 1)
    ring.hand(2,0,-1,1)
    ring.hand(2,0,-1,-1)
    L(1, 1, 1)
    E(1, 3, 1)
    ring.hand(2,0,1,1)
    ring.hand(2,0,1,-1)
    ring.hand(2,1,1,1)
    ring.hand(2,1,1,-1)
    L(1, 2, 1)
    ring.t3(2,0)
    rs.s1(0)
    E(1, 1, 1)
    G(1, 1, 2)
    ring.hand(2,1,2,1)
    ring.hand(2,1,2,-1)
    G(1, 0, 1)
    G(1, 3, 1)
    ring.hand(2,0,2,1)
    ring.hand(2,0,2,-1)
    rs.s1(1)
    rs.a1(0,1,1)
    rs.a1(0,0,1)
    rs.a1(0,0,-1)
    rs.a1(0,1,-1)
    ring.t6(2)
    E(2, 3, 1)
    L(2, 1, 1)
    E(2, 1, 1)
    L(2, 0, 1)
    L(2, 3, 1)
    rs.a1(1,1,1)
    rs.a1(1,0,1)
    rs.a1(1,0,-1)
    rs.a1(1,1,-1)
    L(2, 2, 1)
    later.ready()
    hidden.start()
    E(2, 0, 1)
    E(2, 2, 1)
    earlier.ready()
    reload.start()
    G(2, 3, 1)
    G(2, 2, 1)
    later_block(2)
    rs.a2(0,0)
    rs.a2(0,1)
    later.far()
    G(2, 0, 2)
    rs.s1(2)
    reload.wait()
    earlier_block(2)
    later_block(-1)
    rs.a2(1,0)
    rs.a3(0,0,1)
    earlier.far()
    rs.a3(0,0,-1)
    rs.a3(0,1,1)
    rs.a3(0,1,-1)
    rs.a2(1,1)
    later.near(-1)
    later_block(1)
    rs.a1(2,1,1)
    rs.a1(2,0,1)
    rs.a1(2,0,-1)
    rs.a3(1,0,1)
    rs.a3(1,0,-1)
    rs.a1(2,1,-1)
    rs.a4(0,1)
    later.near(1)
    earlier_block(-1)
    rs.a3(1,1,1)
    rs.a3(1,1,-1)
    rs.a4(0,0)
    earlier_block(1)
    earlier.near(-1)
    earlier_block(0)
    earlier.near(1)
    gain_step(0)
    rs.a2(2,0)
    rs.a2(2,1)
    gain_step(1)
    rs.a4(1,0)
    rs.a4(1,1)
    later_block(0)
    rs.a3(2,0,-1)
    rs.a3(2,0,1)
    rs.a3(2,1,-1)
    rs.a3(2,1,1)
    later_end()
    gain_step(2)
    rs.a4(2,0)
    rs.a4(2,1)
    gain_step(3)
    earlier_end()
    gain_step(4)
    for c in range(N_CHUNK):
        ring.drain(c)
        rs.drain(c)
    later.drain()
    earlier.drain()
    total.drain()
    hidden.wait()


def run(later_in, earlier_in, cot, gate_w, up_w, down_w, gain, gate_sum, up_sum, down_sum):
    tokens, width = later_in.shape
    cols, rows = gate_w.shape
    any_ = pl.BlockSpec(memory_space=pl.ANY)
    vm = pl.BlockSpec(memory_space=pltpu.VMEM)
    tok = (tokens, width)
    dma = pltpu.SemaphoreType.DMA
    return pl.pallas_call(
        sublayer,
        out_shape=[
            jax.ShapeDtypeStruct((tokens // 8, width), BF),
            jax.ShapeDtypeStruct((cols, tokens), BF),
            jax.ShapeDtypeStruct((tokens // 8, width), BF),
            jax.ShapeDtypeStruct((cols, rows), F32),
            jax.ShapeDtypeStruct((cols, rows), F32),
            jax.ShapeDtypeStruct((cols, rows), F32),
            jax.ShapeDtypeStruct((1, width), F32),
        ],
        in_specs=[any_] * 6 + [vm] + [any_] * 3,
        out_specs=[vm, any_] + [vm] * 5,
        scratch_shapes=[
            [pltpu.VMEM((3 * n, width), BF) for n in SIZES],
            [pltpu.VMEM((4, 4, 3 * n, SHARD), BF) for n in SIZES],
            [
                [
                    pltpu.VMEM((2, 2, 4, half_of(c) // 2, SHARD), BF),
                    pltpu.VMEM((2, 2, 4, half_of(c), SHARD), BF),
                    pltpu.VMEM((2, 2, half_of(c) // 2, SHARD), BF),
                    pltpu.VMEM((2, 2, half_of(c), SHARD), BF),
                ]
                for c in range(N_CHUNK)
            ],
            *[pltpu.VMEM(tok, BF)] * 6,
            pltpu.VMEM((cols, tokens), BF),
            [pltpu.VMEM((2 * n, tokens), BF) for n in SIZES],
            pltpu.VMEM((max(SIZES), tokens), BF),
            pltpu.VMEM((256, cols), BF),
            pltpu.VMEM((256, 2 * cols), BF),
            pltpu.VMEM((256, width), F32),
            pltpu.VMEM((SHARD, width), BF),
            pltpu.VMEM((SHARD, width), BF),
            pltpu.VMEM((8, width), F32),
            pltpu.VMEM((4, 4, 1, width), F32),
            dma((9,)),
            dma((N_CHUNK, 3)),
            dma((N_CHUNK, 2, 20)),
            dma((N_CHUNK, 2, 20)),
            dma((N_CHUNK, 2, 8)),
            dma((N_CHUNK, 2, 8)),
            dma((2, 8)),
            dma((2, 8)),
            dma((4, 4)),
            dma((4, 4)),
            pltpu.SemaphoreType.REGULAR((2, 3)),
            dma,
        ],
        compiler_params=pltpu.CompilerParams(
            collective_id=0, has_side_effects=True, vmem_limit_bytes=64 * 1024 * 1024 - 65536
        ),
        name="sublayer",
    )(later_in, earlier_in, cot, gate_w, up_w, down_w, gain.reshape(1, width), gate_sum, up_sum, down_sum)


def local(later_in, earlier_in, cot, gate_w, up_w, down_w, gain, gate_sum, up_sum, down_sum, gain_sum):
    later_out, hidden, earlier_grad, gate_new, up_new, down_new, gain_total = run(
        later_in, earlier_in, cot, gate_w.T, up_w.T, down_w.T, gain, gate_sum.T, up_sum.T, down_sum.T
    )
    return (
        later_out, hidden.T, earlier_grad,
        gate_new.T, up_new.T, down_new.T, gain_sum + gain_total[0],
    )


def solution(mesh):
    torus = Mesh(mesh.devices.reshape(4, 4, 4, 2), ALL)
    return jax.shard_map(
        local,
        mesh=torus,
        in_specs=(P(FS, None),) * 3 + (P(FS, TP),) * 3 + (P(),) + (P(FS, TP),) * 3 + (P(),),
        out_specs=(P(ALL, None), P(FS, TP), P(ALL, None), P(FS, TP), P(FS, TP), P(FS, TP), P()),
        check_vma=False,
    )
```

```python
import functools

import jax
import jax.numpy as jnp
from jax import lax
from jax.experimental import pallas as pl
from jax.experimental.pallas import tpu as pltpu
from jax.sharding import Mesh
from jax.sharding import PartitionSpec as P

FS = ("z", "x")
TP = ("y", "c")
ALL = ("z", "x", "y", "c")
MESH = pl.DeviceIdType.MESH
BF = jnp.bfloat16
F32 = jnp.float32
SIZES = (192, 256, 256)
STARTS = (0, 192, 448)
N_CHUNK = 3
SHARD = 128
NORM_FLOOR = 0.05


def half_of(c):
    return SIZES[c] * 3 // 2


def span(c, h, sub=None):
    n = half_of(c)
    at = h * n
    return slice(at + (n // 2 if sub == 1 else 0), at + (n // 2 if sub == 0 else n))


class Gather:
    def __init__(self, w, send, recv):
        self.w, self.send, self.recv = w, send, recv
        self.mz, self.mx = lax.axis_index("z"), lax.axis_index("x")

    def owner(self, h, jf, js):
        dx, dz = (jf, js) if h == 0 else (js, jf)
        return lax.rem(self.mz + dz + 4, 4) * 4 + lax.rem(self.mx + dx + 4, 4)

    def copy(self, c, h, msg, jf, js, sub, axis, d):
        view = self.w[c].at[
            span(c, h, sub), pl.ds(pl.multiple_of(self.owner(h, jf, js) * SHARD, SHARD), SHARD)
        ]
        name = ("x", "z")[h] if axis == "f" else ("z", "x")[h]
        me = self.mx if name == "x" else self.mz
        return pltpu.make_async_remote_copy(
            src_ref=view,
            dst_ref=view,
            send_sem=self.send.at[c, h, msg],
            recv_sem=self.recv.at[c, h, msg],
            device_id={name: lax.rem(me + d + 4, 4)},
            device_id_type=MESH,
        )

    def m1(self, c, h, d):
        return self.copy(c, h, 0 if d > 0 else 1, 0, 0, None, "f", d)

    def r1(self, c, h, d):
        return self.copy(c, h, 0 if d > 0 else 1, -d, 0, None, "f", d)

    def m2(self, c, h, d):
        return self.copy(c, h, 2 if d > 0 else 3, -d, 0, 0 if d > 0 else 1, "f", d)

    def r2(self, c, h, d):
        return self.copy(c, h, 2 if d > 0 else 3, -2 * d, 0, 0 if d > 0 else 1, "f", d)

    def m3(self, c, h, j, d):
        return self.copy(c, h, 4 + 2 * (j % 4) + (0 if d > 0 else 1), j, 0, None, "s", d)

    def r3(self, c, h, j, d):
        return self.copy(c, h, 4 + 2 * (j % 4) + (0 if d > 0 else 1), j, -d, None, "s", d)

    def m4(self, c, h, j, d):
        return self.copy(c, h, 12 + 2 * (j % 4) + (0 if d > 0 else 1), j, -d, 0 if d > 0 else 1, "s", d)

    def r4(self, c, h, j, d):
        return self.copy(c, h, 12 + 2 * (j % 4) + (0 if d > 0 else 1), j, -2 * d, 0 if d > 0 else 1, "s", d)

    def t0(self, c):
        for h in (0, 1):
            for d in (1, -1):
                self.m1(c, h, d).start()
        for h in (0, 1):
            for d in (1, -1):
                self.m3(c, h, 0, d).start()

    def t1(self, c, h, d):
        self.r1(c, h, d).wait_recv()
        self.m2(c, h, d).start()
        for e in (1, -1):
            self.m3(c, h, -d, e).start()

    def t3(self, c, h):
        for d in (1, -1):
            self.r2(c, h, d).wait_recv()
        for e in (1, -1):
            self.m3(c, h, 2, e).start()

    def hand(self, c, h, j, d):
        self.r3(c, h, j, d).wait_recv()
        self.m4(c, h, j, d).start()

    def t6(self, c):
        for h in (0, 1):
            for j in (0, -1, 1, 2):
                for d in (1, -1):
                    self.r4(c, h, j, d).wait_recv()

    def drain(self, c):
        for h in (0, 1):
            for d in (1, -1):
                self.m1(c, h, d).wait_send()
                self.m2(c, h, d).wait_send()
                for j in (0, -1, 1, 2):
                    self.m3(c, h, j, d).wait_send()
                    self.m4(c, h, j, d).wait_send()


def greet(peers):
    barrier = pltpu.get_barrier_semaphore()
    for peer in peers:
        pl.semaphore_signal(barrier, inc=1, device_id=peer, device_id_type=MESH)
    pl.semaphore_wait(barrier, len(peers))


def ring_peers(names):
    peers = []
    for name in names:
        me = lax.axis_index(name)
        for d in (1, 3):
            peers.append({name: lax.rem(me + d, 4)})
    return peers


def nn(a, b):
    return jnp.dot(a, b, preferred_element_type=F32)


class Scatter:
    def __init__(self, g, r, send, recv, out):
        self.g, self.r = g, r
        self.send, self.recv, self.out = send, recv, out
        self.at = {"z": lax.axis_index("z"), "x": lax.axis_index("x")}

    def unit(self, c, h, jf, js=None, sub=None):
        fast, slow = (("x", "z"), ("z", "x"))[h]
        f = lax.rem(self.at[fast] + jf + 4, 4)
        s = slice(None) if js is None else lax.rem(self.at[slow] + js + 4, 4)
        where = (s, f) if h == 0 else (f, s)
        return self.g[c].at[(*where, span(c, h, sub), slice(None))]

    def landing(self, stage, c, h, i):
        return self.r[c][stage].at[h, i]

    def copy(self, stage, c, h, d, src):
        i = 0 if d > 0 else 1
        name = (("x", "z"), ("z", "x"))[h][stage // 2]
        m = stage * 2 + i
        return pltpu.make_async_remote_copy(
            src_ref=src,
            dst_ref=self.landing(stage, c, h, i),
            send_sem=self.send.at[c, h, m],
            recv_sem=self.recv.at[c, h, m],
            device_id={name: lax.rem(self.at[name] + d + 4, 4)},
            device_id_type=MESH,
        )

    def c1(self, c, h, d):
        return self.copy(0, c, h, d, self.unit(c, h, 2, None, 0 if d > 0 else 1))

    def c2(self, c, h, d):
        return self.copy(1, c, h, d, self.unit(c, h, d))

    def c3(self, c, h, d):
        return self.copy(2, c, h, d, self.unit(c, h, 0, 2, 0 if d > 0 else 1))

    def c4(self, c, h, d):
        return self.copy(3, c, h, d, self.unit(c, h, 0, d))

    def s1(self, c):
        for h in (0, 1):
            for d in (1, -1):
                self.c1(c, h, d).start()

    def a1(self, c, h, d):
        i = 0 if d > 0 else 1
        self.c1(c, h, d).wait_recv()
        part = self.unit(c, h, d, None, i)
        for k in range(4):
            part[k] = part[k] + self.landing(0, c, h, i)[k]
        self.c2(c, h, d).start()

    def a2(self, c, h):
        for d in (1, -1):
            self.c2(c, h, d).wait_recv()
        whole = self.unit(c, h, 0)
        for k in range(4):
            whole[k] = (
                whole[k].astype(F32)
                + self.landing(1, c, h, 0)[k].astype(F32)
                + self.landing(1, c, h, 1)[k].astype(F32)
            ).astype(BF)
        for d in (1, -1):
            self.c3(c, h, d).start()

    def a3(self, c, h, d):
        i = 0 if d > 0 else 1
        self.c3(c, h, d).wait_recv()
        part = self.unit(c, h, 0, d, i)
        part[...] = part[...] + self.landing(2, c, h, i)[...]
        self.c4(c, h, d).start()

    def a4(self, c, h):
        for d in (1, -1):
            self.c4(c, h, d).wait_recv()
        own = self.unit(c, h, 0, 0)
        done = (
            own[...].astype(F32)
            + self.landing(3, c, h, 0)[...].astype(F32)
            + self.landing(3, c, h, 1)[...].astype(F32)
        )
        n, size = half_of(c), SIZES[c]
        for k, out in enumerate(self.out):
            first, last = max(h * n, k * size), min((h + 1) * n, (k + 1) * size)
            if first < last:
                at = slice(STARTS[c] + first - k * size, STARTS[c] + last - k * size)
                out[at, :] = out[at, :] + done[first - h * n : last - h * n]

    def drain(self, c):
        for h in (0, 1):
            for d in (1, -1):
                for copy in (self.c1, self.c2, self.c3, self.c4):
                    copy(c, h, d).wait_send()


class TokenScatter:
    def __init__(self, t, p, buf, credit, send, recv):
        self.t, self.p, self.buf, self.credit = t, p, buf, credit
        self.send, self.recv = send, recv
        self.y, self.c = lax.axis_index("y"), lax.axis_index("c")

    def to(self, k):
        return lax.rem(self.y + k + 4, 4)

    def rows(self, k, core, sub=None):
        start, n = (self.to(k) * 2 + core) * SHARD, SHARD
        if sub is not None:
            start, n = start + sub * (SHARD // 2), SHARD // 2
        return self.p.at[pl.ds(pl.multiple_of(start, SHARD // 2), n), :]

    def landed(self, k):
        return self.buf.at[pl.ds(pl.multiple_of(self.to(k) * SHARD, SHARD), SHARD), :]

    def q1(self, i):
        start = 4 * SHARD + i * (SHARD // 2)
        return self.buf.at[start : start + SHARD // 2, :]

    def q2(self, i):
        start = (5 + i) * SHARD
        return self.buf.at[start : start + SHARD, :]

    def ready(self):
        for i, peer in enumerate(({"c": 1 - self.c}, {"y": self.to(-1)}, {"y": self.to(1)})):
            pl.semaphore_signal(self.credit.at[self.t, i], inc=1, device_id=peer, device_id_type=MESH)

    def pair(self, k):
        return pltpu.make_async_remote_copy(
            src_ref=self.rows(k, 1 - self.c),
            dst_ref=self.landed(k),
            send_sem=self.send.at[self.t, k % 4],
            recv_sem=self.recv.at[self.t, k % 4],
            device_id={"c": 1 - self.c},
            device_id_type=MESH,
        )

    def ring(self, src, dst, m, d):
        return pltpu.make_async_remote_copy(
            src_ref=src,
            dst_ref=dst,
            send_sem=self.send.at[self.t, m],
            recv_sem=self.recv.at[self.t, m],
            device_id={"y": self.to(d)},
            device_id_type=MESH,
        )

    def y1(self, d):
        i = 0 if d > 0 else 1
        return self.ring(self.rows(2, self.c, i), self.q1(i), 4 + i, d)

    def y2(self, d):
        i = 0 if d > 0 else 1
        return self.ring(self.rows(d, self.c), self.q2(i), 6 + i, d)

    def share(self, k):
        if k == 2:
            pl.semaphore_wait(self.credit.at[self.t, 0], 1)
        self.pair(k).start()

    def join(self, k):
        self.pair(k).wait_recv()
        mine = self.rows(k, self.c)
        mine[...] = mine[...] + self.landed(k)[...]

    def far(self):
        self.join(2)
        for d in (1, -1):
            pl.semaphore_wait(self.credit.at[self.t, 1 if d > 0 else 2], 1)
            self.y1(d).start()

    def near(self, d):
        i = 0 if d > 0 else 1
        self.join(d)
        self.y1(d).wait_recv()
        part = self.rows(d, self.c, i)
        part[...] = part[...] + self.q1(i)[...]
        self.y2(d).start()

    def finish(self):
        self.join(0)
        for d in (1, -1):
            self.y2(d).wait_recv()
        return (
            self.rows(0, self.c)[...].astype(F32) + self.q2(0)[...].astype(F32) + self.q2(1)[...].astype(F32)
        )

    def drain(self):
        for k in (0, 1, 2, -1):
            self.pair(k).wait_send()
        for d in (1, -1):
            self.y1(d).wait_send()
            self.y2(d).wait_send()


class GainSum:
    AXES = (("c", 2), ("x", 4), ("z", 4), ("y", 4))

    def __init__(self, rows, send, recv):
        self.rows, self.send, self.recv = rows, send, recv

    def copy(self, i, d, arriving):
        name, n = self.AXES[i]
        me = lax.axis_index(name)
        src = lax.rem(me + n - d, n) if arriving else me
        return pltpu.make_async_remote_copy(
            src_ref=self.rows.at[i, src],
            dst_ref=self.rows.at[i, src],
            send_sem=self.send.at[i, d],
            recv_sem=self.recv.at[i, d],
            device_id={name: lax.rem(me + d, n)},
            device_id_type=MESH,
        )

    def start(self, i, row):
        name, n = self.AXES[i]
        self.rows[i, lax.axis_index(name)] = row
        for d in range(1, n):
            self.copy(i, d, False).start()

    def end(self, i):
        n = self.AXES[i][1]
        for d in range(1, n):
            self.copy(i, d, True).wait_recv()
        row = self.rows[i, 0]
        for k in range(1, n):
            row = row + self.rows[i, k]
        return row

    def drain(self):
        for i, (_, n) in enumerate(self.AXES):
            for d in range(1, n):
                self.copy(i, d, False).wait_send()


def sublayer(
    later_in, earlier_in, cot_in, gate_w, up_w, down_w, gain, gate_sum, up_sum, down_sum,
    later_out, hidden_out, earlier_out, gate_new, up_new, down_new, gain_out,
    w, g, r, nl, ne, cot, nlt, net, cott, hl, dx, he, hb, xb, dn, lrow, crow, gacc, grows,
    in_sem, own_sem, wsend, wrecv, send, recv, tsend, trecv, gsend, grecv, credit, out_sem,
):
    tokens, width = nl.shape
    half = width // 2
    z, x, y, c_me = (lax.axis_index(n) for n in ALL)
    me = z * 4 + x
    own_rows = pl.ds(pl.multiple_of((y * 2 + c_me) * SHARD, SHARD), SHARD)
    mine = pl.ds(pl.multiple_of(me * SHARD, SHARD), SHARD)
    own = [
        pltpu.make_async_copy(
            ref.at[STARTS[c] : STARTS[c] + SIZES[c], :],
            w[c].at[k * SIZES[c] : (k + 1) * SIZES[c], mine],
            own_sem.at[c, k],
        )
        for c in range(N_CHUNK)
        for k, ref in enumerate((gate_w, up_w, down_w))
    ]
    pairs = [
        (later_in, nl), (earlier_in, ne), (cot_in, cot),
        (gate_sum, gate_new), (up_sum, up_new), (down_sum, down_new),
        (later_in.at[own_rows, :], lrow), (cot_in.at[own_rows, :], crow),
    ]
    ins = [pltpu.make_async_copy(a, b, in_sem.at[i]) for i, (a, b) in enumerate(pairs)]
    for copy in own:
        copy.start()
    for copy in ins[:3]:
        copy.start()
    across = [{n: lax.rem(lax.axis_index(n) + 2, 4)} for n in ("x", "z", "y")]
    greet(ring_peers(("x", "z", "y")) + [{"c": 1 - c_me}] + across)
    for copy in own:
        copy.wait()
    ring = Gather(w, wsend, wrecv)
    ring.t0(0)
    for copy in ins[3:]:
        copy.start()
    rs = Scatter(g, r, send, recv, (gate_new, up_new, down_new))
    later = TokenScatter(0, nl, nlt, credit, tsend, trecv)
    earlier = TokenScatter(1, ne, net, credit, tsend, trecv)
    total = GainSum(grows, gsend, grecv)

    gain_row = gain[...].astype(F32).reshape(1, width)

    def turn_block(turned, ref, i):
        rows = pl.ds(pl.multiple_of(i * 128, 128), 128)
        for j in (0, 1):
            at = pl.ds(pl.multiple_of(i * 128 + j * tokens, 128), 128)
            turned[:, at] = ref[rows, j * half : (j + 1) * half].T

    def tok(i):
        return pl.ds(pl.multiple_of(i * 256, 256), 256)

    def turned_cols(turned, i):
        return jnp.concatenate(
            [turned[:, pl.ds(pl.multiple_of(i * 256 + j * tokens, 256), 256)] for j in (0, 1)], axis=0
        )

    def norms(ref, first, last):
        @pl.loop(first, last)
        def _(i):
            rows = pl.ds(pl.multiple_of(i * 64, 64), 64)
            v = ref[rows, :].astype(F32)
            unit = v * lax.rsqrt(jnp.mean(v * v, axis=1, keepdims=True) + NORM_FLOOR)
            ref[rows, :] = (unit * gain_row).astype(BF)

    def turns(turned, ref, first, last):
        @pl.loop(first, last)
        def _(i):
            turn_block(turned, ref, i)

    blocks = tokens // 128

    def looped(item, c, first, count):
        @pl.loop(first, first + count)
        def _(i):
            item(c, i)

    def later_item(c, i):
        n = SIZES[c]
        pre = nn(w[c][: 2 * n, :], turned_cols(nlt, i))
        gate, up = pre[:n], pre[n:]
        hl[STARTS[c] : STARTS[c] + n, tok(i)] = (gate * jax.nn.sigmoid(gate) * up).astype(BF)

    def earlier_item(c, i):
        n = SIZES[c]
        pre = nn(w[c][: 2 * n, :], turned_cols(net, i))
        dh = 0.5 * nn(w[c][2 * n :, :], turned_cols(cott, i))
        gate, up = pre[:n], pre[n:]
        s = jax.nn.sigmoid(gate)
        act = gate * s
        he[:n, tok(i)] = (act * up).astype(BF)
        dx[c][:n, tok(i)] = (dh * up * s * (1.0 + gate * (1.0 - s))).astype(BF)
        dx[c][n:, tok(i)] = (dh * act).astype(BF)

    def grad_item(c, i):
        n = SIZES[c]
        for j in (0, 1):
            cols = pl.ds(pl.multiple_of(i * 512 + j * 256, 256), 256)
            both = nn(dx[c][...], ne[:, cols]).astype(BF)
            down = (0.5 * nn(he[:n, :], cot[:, cols])).astype(BF)
            for m in (0, 1):
                lanes = slice(m * SHARD, (m + 1) * SHARD)
                g[c][i, 2 * j + m, : 2 * n, :] = both[:, lanes]
                g[c][i, 2 * j + m, 2 * n :, :] = down[:, lanes]

    L = functools.partial(looped, later_item)
    E = functools.partial(looped, earlier_item)
    G = functools.partial(looped, grad_item)

    reload = pltpu.make_async_copy(earlier_in, cott, in_sem.at[8])
    hidden = pltpu.make_async_copy(hl, hidden_out, out_sem)

    def features(n):
        return pl.ds(pl.multiple_of(n * 512, 512), 512)

    def later_block(k):
        b = lax.rem(y + k + 4, 4)
        hb[...] = hl[:, tok(b)].T

        @pl.loop(0, width // 512)
        def _(n):
            f = features(n)
            rows = [w[c][2 * SIZES[c] :, f] for c in range(N_CHUNK)]
            nl[tok(b), f] = nn(hb[...], jnp.concatenate(rows, axis=0)).astype(BF)

        later.share(k)

    def earlier_block(k):
        b = lax.rem(y + k + 4, 4)
        for c in range(N_CHUNK):
            xb[:, 2 * STARTS[c] : 2 * (STARTS[c] + SIZES[c])] = dx[c][:, tok(b)].T

        @pl.loop(0, width // 512)
        def _(n):
            f = features(n)
            rows = [w[c][: 2 * SIZES[c], f] for c in range(N_CHUNK)]
            dn[:, f] = nn(xb[...], jnp.concatenate(rows, axis=0))

        @pl.loop(0, 16)
        def _(i):
            at = pl.ds(pl.multiple_of(b * 256 + i * 16, 16), 16)
            v = cott[at, :].astype(F32)
            scale = lax.rsqrt(jnp.mean(v * v, axis=1, keepdims=True) + NORM_FLOOR)
            unit = v * scale
            d = dn[pl.ds(pl.multiple_of(i * 16, 16), 16), :]
            terms = d * unit
            gacc[...] += terms[:8] + terms[8:]
            mean = jnp.mean(terms * gain_row, axis=1, keepdims=True)
            ne[at, :] = (scale * (d * gain_row - unit * mean)).astype(BF)

        earlier.share(k)

    def gain_step(i):
        row = total.end(i - 1) if i else jnp.sum(gacc[...], axis=0, keepdims=True)
        if i < 4:
            total.start(i, row)
        else:
            gain_out[...] = row

    def later_end():
        later_out[...] = (lrow[...].astype(F32) + 0.5 * later.finish()).astype(BF)

    def earlier_end():
        earlier_out[...] = (crow[...].astype(F32) + earlier.finish()).astype(BF)

    gacc[...] = jnp.zeros_like(gacc)
    ins[2].wait()
    turns(cott, cot, 0, blocks // 2)
    turns(cott, cot, blocks // 2, blocks)
    ring.t1(0,0,1)
    ring.t1(0,0,-1)
    ring.t1(0,1,1)
    ring.t1(0,1,-1)
    ins[0].wait()
    norms(nl, 0, blocks)
    ring.hand(0,0,0,1)
    ring.hand(0,0,0,-1)
    ring.hand(0,1,0,1)
    ring.hand(0,1,0,-1)
    norms(nl, blocks, 2 * blocks)
    ring.t3(0,0)
    ins[1].wait()
    norms(ne, 0, blocks)
    ring.hand(0,0,-1,1)
    ring.hand(0,0,-1,-1)
    ring.hand(0,1,-1,1)
    ring.hand(0,1,-1,-1)
    norms(ne, blocks, 2 * blocks)
    ring.t3(0,1)
    ring.t0(1)
    ring.hand(0,0,1,1)
    ring.hand(0,0,1,-1)
    ring.hand(0,1,1,1)
    ring.hand(0,1,1,-1)
    turns(net, ne, 0, blocks // 2)
    ring.hand(0,0,2,1)
    ring.hand(0,0,2,-1)
    turns(net, ne, blocks // 2, blocks)
    ring.hand(0,1,2,1)
    ring.hand(0,1,2,-1)
    turns(nlt, nl, 0, blocks // 2)
    ring.t1(1,0,1)
    ring.t1(1,0,-1)
    ring.t1(1,1,1)
    ring.t1(1,1,-1)
    turns(nlt, nl, blocks // 2, blocks)
    ring.hand(1,0,0,1)
    ring.hand(1,0,0,-1)
    ring.hand(1,1,0,1)
    ring.hand(1,1,0,-1)
    ring.t6(0)
    E(0, 3, 1)
    E(0, 1, 1)
    ring.t3(1,0)
    ring.hand(1,0,-1,1)
    ring.hand(1,0,-1,-1)
    E(0, 0, 1)
    E(0, 2, 1)
    ring.hand(1,0,1,1)
    ring.hand(1,0,1,-1)
    ring.hand(1,1,-1,1)
    ring.hand(1,1,-1,-1)
    G(0, 2, 1)
    ring.t3(1,1)
    ring.t0(2)
    G(0, 0, 1)
    ring.hand(1,1,1,1)
    ring.hand(1,1,1,-1)
    L(0, 2, 1)
    G(0, 3, 1)
    L(0, 1, 1)
    L(0, 3, 1)
    ring.hand(1,0,2,1)
    ring.hand(1,0,2,-1)
    L(0, 0, 1)
    G(0, 1, 1)
    ring.hand(1,1,2,1)
    ring.hand(1,1,2,-1)
    ring.t1(2,0,-1)
    ring.t1(2,0,1)
    ring.t1(2,1,-1)
    ring.t1(2,1,1)
    ring.hand(2,1,0,-1)
    ring.hand(2,1,0,1)
    ring.hand(2,0,0,-1)
    ring.hand(2,0,0,1)
    for copy in ins[3:]:
        copy.wait()
    ring.t6(1)
    L(1, 0, 1)
    E(1, 3, 1)
    ring.t3(2,0)
    ring.hand(2,0,1,1)
    ring.hand(2,0,1,-1)
    L(1, 2, 2)
    ring.hand(2,0,-1,1)
    ring.hand(2,0,-1,-1)
    ring.hand(2,1,1,1)
    ring.hand(2,1,1,-1)
    E(1, 0, 1)
    ring.t3(2,1)
    rs.s1(0)
    E(1, 2, 1)
    ring.hand(2,1,-1,1)
    ring.hand(2,1,-1,-1)
    E(1, 1, 1)
    G(1, 2, 1)
    ring.hand(2,0,2,1)
    ring.hand(2,0,2,-1)
    G(1, 0, 1)
    G(1, 3, 1)
    ring.hand(2,1,2,1)
    ring.hand(2,1,2,-1)
    G(1, 1, 1)
    rs.s1(1)
    L(1, 1, 1)
    rs.a1(0,0,-1)
    rs.a1(0,0,1)
    rs.a1(0,1,1)
    rs.a1(0,1,-1)
    ring.t6(2)
    L(2, 3, 1)
    E(2, 3, 1)
    L(2, 2, 1)
    L(2, 0, 2)
    later.ready()
    hidden.start()
    rs.a1(1,1,1)
    rs.a1(1,0,1)
    rs.a1(1,0,-1)
    rs.a1(1,1,-1)
    later_block(2)
    later_block(1)
    later_block(-1)
    later.far()
    E(2, 0, 1)
    rs.a2(0,1)
    rs.a2(0,0)
    E(2, 1, 2)
    earlier.ready()
    reload.start()
    G(2, 0, 1)
    G(2, 2, 1)
    G(2, 1, 1)
    later.near(1)
    later.near(-1)
    rs.a2(1,1)
    rs.a2(1,0)
    rs.a3(0,0,1)
    rs.a3(0,0,-1)
    rs.a3(0,1,1)
    rs.a3(0,1,-1)
    G(2, 3, 1)
    rs.s1(2)
    reload.wait()
    earlier_block(2)
    rs.a3(1,0,1)
    rs.a3(1,0,-1)
    rs.a3(1,1,1)
    rs.a3(1,1,-1)
    rs.a4(0,0)
    rs.a4(0,1)
    earlier_block(-1)
    earlier.far()
    rs.a1(2,0,1)
    rs.a1(2,0,-1)
    rs.a1(2,1,1)
    rs.a1(2,1,-1)
    rs.a4(1,0)
    rs.a4(1,1)
    earlier_block(1)
    earlier_block(0)
    earlier.near(1)
    earlier.near(-1)
    gain_step(0)
    later_block(0)
    gain_step(1)
    rs.a2(2,0)
    rs.a2(2,1)
    later_end()
    gain_step(2)
    rs.a3(2,0,-1)
    rs.a3(2,0,1)
    rs.a3(2,1,-1)
    rs.a3(2,1,1)
    gain_step(3)
    rs.a4(2,0)
    rs.a4(2,1)
    earlier_end()
    gain_step(4)
    for c in range(N_CHUNK):
        ring.drain(c)
        rs.drain(c)
    later.drain()
    earlier.drain()
    total.drain()
    hidden.wait()


def run(later_in, earlier_in, cot, gate_w, up_w, down_w, gain, gate_sum, up_sum, down_sum):
    tokens, width = later_in.shape
    cols, rows = gate_w.shape
    any_ = pl.BlockSpec(memory_space=pl.ANY)
    vm = pl.BlockSpec(memory_space=pltpu.VMEM)
    tok = (tokens, width)
    dma = pltpu.SemaphoreType.DMA
    return pl.pallas_call(
        sublayer,
        out_shape=[
            jax.ShapeDtypeStruct((tokens // 8, width), BF),
            jax.ShapeDtypeStruct((cols, tokens), BF),
            jax.ShapeDtypeStruct((tokens // 8, width), BF),
            jax.ShapeDtypeStruct((cols, rows), F32),
            jax.ShapeDtypeStruct((cols, rows), F32),
            jax.ShapeDtypeStruct((cols, rows), F32),
            jax.ShapeDtypeStruct((1, width), F32),
        ],
        in_specs=[any_] * 6 + [vm] + [any_] * 3,
        out_specs=[vm, any_] + [vm] * 5,
        scratch_shapes=[
            [pltpu.VMEM((3 * n, width), BF) for n in SIZES],
            [pltpu.VMEM((4, 4, 3 * n, SHARD), BF) for n in SIZES],
            [
                [
                    pltpu.VMEM((2, 2, 4, half_of(c) // 2, SHARD), BF),
                    pltpu.VMEM((2, 2, 4, half_of(c), SHARD), BF),
                    pltpu.VMEM((2, 2, half_of(c) // 2, SHARD), BF),
                    pltpu.VMEM((2, 2, half_of(c), SHARD), BF),
                ]
                for c in range(N_CHUNK)
            ],
            *[pltpu.VMEM(tok, BF)] * 6,
            pltpu.VMEM((cols, tokens), BF),
            [pltpu.VMEM((2 * n, tokens), BF) for n in SIZES],
            pltpu.VMEM((max(SIZES), tokens), BF),
            pltpu.VMEM((256, cols), BF),
            pltpu.VMEM((256, 2 * cols), BF),
            pltpu.VMEM((256, width), F32),
            pltpu.VMEM((SHARD, width), BF),
            pltpu.VMEM((SHARD, width), BF),
            pltpu.VMEM((8, width), F32),
            pltpu.VMEM((4, 4, 1, width), F32),
            dma((9,)),
            dma((N_CHUNK, 3)),
            dma((N_CHUNK, 2, 20)),
            dma((N_CHUNK, 2, 20)),
            dma((N_CHUNK, 2, 8)),
            dma((N_CHUNK, 2, 8)),
            dma((2, 8)),
            dma((2, 8)),
            dma((4, 4)),
            dma((4, 4)),
            pltpu.SemaphoreType.REGULAR((2, 3)),
            dma,
        ],
        compiler_params=pltpu.CompilerParams(
            collective_id=0, has_side_effects=True, vmem_limit_bytes=64 * 1024 * 1024 - 65536
        ),
        name="sublayer",
    )(later_in, earlier_in, cot, gate_w, up_w, down_w, gain, gate_sum, up_sum, down_sum)


def deliver_body(*refs):
    n = (len(refs) - 2) // 3
    srcs, outs, bufs = refs[:n], refs[n : 2 * n], refs[2 * n : 3 * n]
    in_sem, out_sem = refs[-2:]
    ins = [pltpu.make_async_copy(a, b, in_sem.at[i]) for i, (a, b) in enumerate(zip(srcs, bufs))]
    for copy in ins:
        copy.start()
    puts = [pltpu.make_async_copy(a, b, out_sem.at[i]) for i, (a, b) in enumerate(zip(bufs, outs))]
    for copy, put in zip(ins, puts):
        copy.wait()
        put.start()
    for put in puts:
        put.wait()


def deliver(arrays):
    any_ = pl.BlockSpec(memory_space=pl.ANY)
    n = len(arrays)
    return pl.pallas_call(
        deliver_body,
        out_shape=[jax.ShapeDtypeStruct(a.shape, a.dtype) for a in arrays],
        in_specs=[any_] * n,
        out_specs=[any_] * n,
        scratch_shapes=[pltpu.VMEM(a.shape, a.dtype) for a in arrays]
        + [pltpu.SemaphoreType.DMA((n,)), pltpu.SemaphoreType.DMA((n,))],
        compiler_params=pltpu.CompilerParams(vmem_limit_bytes=64 * 1024 * 1024 - 65536),
        name="deliver",
    )(*arrays)


def local(later_in, earlier_in, cot, gate_w, up_w, down_w, gain, gate_sum, up_sum, down_sum, gain_sum):
    *parts, gain_total = run(
        later_in, earlier_in, cot, gate_w.T, up_w.T, down_w.T, gain, gate_sum.T, up_sum.T, down_sum.T
    )
    later_out, hidden, earlier_grad, gate_new, up_new, down_new = deliver(parts)
    return (
        later_out, hidden.T, earlier_grad,
        gate_new.T, up_new.T, down_new.T, gain_sum + gain_total[0],
    )


def solution(mesh):
    torus = Mesh(mesh.devices.reshape(4, 4, 4, 2), ALL)
    return jax.shard_map(
        local,
        mesh=torus,
        in_specs=(P(FS, None),) * 3 + (P(FS, TP),) * 3 + (P(),) + (P(FS, TP),) * 3 + (P(),),
        out_specs=(P(ALL, None), P(FS, TP), P(ALL, None), P(FS, TP), P(FS, TP), P(FS, TP), P()),
        check_vma=False,
    )
```

```python
import functools

import jax
import jax.numpy as jnp
from jax import lax
from jax.experimental import pallas as pl
from jax.experimental.pallas import tpu as pltpu
from jax.sharding import Mesh
from jax.sharding import PartitionSpec as P

FS = ("z", "x")
TP = ("y", "c")
ALL = ("z", "x", "y", "c")
MESH = pl.DeviceIdType.MESH
BF = jnp.bfloat16
F32 = jnp.float32
SIZES = (256, 320, 128)
STARTS = (0, 256, 576)
N_CHUNK = 3
SHARD = 128
NORM_FLOOR = 0.05


def half_of(c):
    return SIZES[c] * 3 // 2


def span(c, h, sub=None):
    n = half_of(c)
    at = h * n
    return slice(at + (n // 2 if sub == 1 else 0), at + (n // 2 if sub == 0 else n))


class Gather:
    def __init__(self, w, send, recv):
        self.w, self.send, self.recv = w, send, recv
        self.mz, self.mx = lax.axis_index("z"), lax.axis_index("x")

    def owner(self, h, jf, js):
        dx, dz = (jf, js) if h == 0 else (js, jf)
        return lax.rem(self.mz + dz + 4, 4) * 4 + lax.rem(self.mx + dx + 4, 4)

    def copy(self, c, h, msg, jf, js, sub, axis, d):
        view = self.w[c].at[
            span(c, h, sub), pl.ds(pl.multiple_of(self.owner(h, jf, js) * SHARD, SHARD), SHARD)
        ]
        name = ("x", "z")[h] if axis == "f" else ("z", "x")[h]
        me = self.mx if name == "x" else self.mz
        return pltpu.make_async_remote_copy(
            src_ref=view,
            dst_ref=view,
            send_sem=self.send.at[c, h, msg],
            recv_sem=self.recv.at[c, h, msg],
            device_id={name: lax.rem(me + d + 4, 4)},
            device_id_type=MESH,
        )

    def m1(self, c, h, d):
        return self.copy(c, h, 0 if d > 0 else 1, 0, 0, None, "f", d)

    def r1(self, c, h, d):
        return self.copy(c, h, 0 if d > 0 else 1, -d, 0, None, "f", d)

    def m2(self, c, h, d):
        return self.copy(c, h, 2 if d > 0 else 3, -d, 0, 0 if d > 0 else 1, "f", d)

    def r2(self, c, h, d):
        return self.copy(c, h, 2 if d > 0 else 3, -2 * d, 0, 0 if d > 0 else 1, "f", d)

    def m3(self, c, h, j, d):
        return self.copy(c, h, 4 + 2 * (j % 4) + (0 if d > 0 else 1), j, 0, None, "s", d)

    def r3(self, c, h, j, d):
        return self.copy(c, h, 4 + 2 * (j % 4) + (0 if d > 0 else 1), j, -d, None, "s", d)

    def m4(self, c, h, j, d):
        return self.copy(c, h, 12 + 2 * (j % 4) + (0 if d > 0 else 1), j, -d, 0 if d > 0 else 1, "s", d)

    def r4(self, c, h, j, d):
        return self.copy(c, h, 12 + 2 * (j % 4) + (0 if d > 0 else 1), j, -2 * d, 0 if d > 0 else 1, "s", d)

    def t0(self, c):
        for h in (0, 1):
            for d in (1, -1):
                self.m1(c, h, d).start()
        for h in (0, 1):
            for d in (1, -1):
                self.m3(c, h, 0, d).start()

    def t1(self, c, h, d):
        self.r1(c, h, d).wait_recv()
        self.m2(c, h, d).start()
        for e in (1, -1):
            self.m3(c, h, -d, e).start()

    def t3(self, c, h):
        for d in (1, -1):
            self.r2(c, h, d).wait_recv()
        for e in (1, -1):
            self.m3(c, h, 2, e).start()

    def hand(self, c, h, j, d):
        self.r3(c, h, j, d).wait_recv()
        self.m4(c, h, j, d).start()

    def t6(self, c):
        for h in (0, 1):
            for j in (0, -1, 1, 2):
                for d in (1, -1):
                    self.r4(c, h, j, d).wait_recv()

    def drain(self, c):
        for h in (0, 1):
            for d in (1, -1):
                self.m1(c, h, d).wait_send()
                self.m2(c, h, d).wait_send()
                for j in (0, -1, 1, 2):
                    self.m3(c, h, j, d).wait_send()
                    self.m4(c, h, j, d).wait_send()


def greet(peers):
    barrier = pltpu.get_barrier_semaphore()
    for peer in peers:
        pl.semaphore_signal(barrier, inc=1, device_id=peer, device_id_type=MESH)
    pl.semaphore_wait(barrier, len(peers))


def ring_peers(names):
    peers = []
    for name in names:
        me = lax.axis_index(name)
        for d in (1, 3):
            peers.append({name: lax.rem(me + d, 4)})
    return peers


def nn(a, b):
    return jnp.dot(a, b, preferred_element_type=F32)


class Scatter:
    def __init__(self, g, r, send, recv, out):
        self.g, self.r = g, r
        self.send, self.recv, self.out = send, recv, out
        self.at = {"z": lax.axis_index("z"), "x": lax.axis_index("x")}

    def unit(self, c, h, jf, js=None, sub=None):
        fast, slow = (("x", "z"), ("z", "x"))[h]
        f = lax.rem(self.at[fast] + jf + 4, 4)
        s = slice(None) if js is None else lax.rem(self.at[slow] + js + 4, 4)
        where = (s, f) if h == 0 else (f, s)
        return self.g[c].at[(*where, span(c, h, sub), slice(None))]

    def landing(self, stage, c, h, i):
        return self.r[c][stage].at[h, i]

    def copy(self, stage, c, h, d, src):
        i = 0 if d > 0 else 1
        name = (("x", "z"), ("z", "x"))[h][stage // 2]
        m = stage * 2 + i
        return pltpu.make_async_remote_copy(
            src_ref=src,
            dst_ref=self.landing(stage, c, h, i),
            send_sem=self.send.at[c, h, m],
            recv_sem=self.recv.at[c, h, m],
            device_id={name: lax.rem(self.at[name] + d + 4, 4)},
            device_id_type=MESH,
        )

    def c1(self, c, h, d):
        return self.copy(0, c, h, d, self.unit(c, h, 2, None, 0 if d > 0 else 1))

    def c2(self, c, h, d):
        return self.copy(1, c, h, d, self.unit(c, h, d))

    def c3(self, c, h, d):
        return self.copy(2, c, h, d, self.unit(c, h, 0, 2, 0 if d > 0 else 1))

    def c4(self, c, h, d):
        return self.copy(3, c, h, d, self.unit(c, h, 0, d))

    def s1(self, c):
        for h in (0, 1):
            for d in (1, -1):
                self.c1(c, h, d).start()

    def a1(self, c, h, d):
        i = 0 if d > 0 else 1
        self.c1(c, h, d).wait_recv()
        part = self.unit(c, h, d, None, i)
        for k in range(4):
            part[k] = part[k] + self.landing(0, c, h, i)[k]
        self.c2(c, h, d).start()

    def a2(self, c, h):
        for d in (1, -1):
            self.c2(c, h, d).wait_recv()
        whole = self.unit(c, h, 0)
        for k in range(4):
            whole[k] = (
                whole[k].astype(F32)
                + self.landing(1, c, h, 0)[k].astype(F32)
                + self.landing(1, c, h, 1)[k].astype(F32)
            ).astype(BF)
        for d in (1, -1):
            self.c3(c, h, d).start()

    def a3(self, c, h, d):
        i = 0 if d > 0 else 1
        self.c3(c, h, d).wait_recv()
        part = self.unit(c, h, 0, d, i)
        part[...] = part[...] + self.landing(2, c, h, i)[...]
        self.c4(c, h, d).start()

    def a4(self, c, h):
        for d in (1, -1):
            self.c4(c, h, d).wait_recv()
        own = self.unit(c, h, 0, 0)
        done = (
            own[...].astype(F32)
            + self.landing(3, c, h, 0)[...].astype(F32)
            + self.landing(3, c, h, 1)[...].astype(F32)
        )
        n, size = half_of(c), SIZES[c]
        for k, out in enumerate(self.out):
            first, last = max(h * n, k * size), min((h + 1) * n, (k + 1) * size)
            if first < last:
                at = slice(STARTS[c] + first - k * size, STARTS[c] + last - k * size)
                out[at, :] = out[at, :] + done[first - h * n : last - h * n]

    def drain(self, c):
        for h in (0, 1):
            for d in (1, -1):
                for copy in (self.c1, self.c2, self.c3, self.c4):
                    copy(c, h, d).wait_send()


class TokenScatter:
    def __init__(self, t, p, buf, credit, send, recv):
        self.t, self.p, self.buf, self.credit = t, p, buf, credit
        self.send, self.recv = send, recv
        self.y, self.c = lax.axis_index("y"), lax.axis_index("c")

    def to(self, k):
        return lax.rem(self.y + k + 4, 4)

    def rows(self, k, core, sub=None):
        start, n = (self.to(k) * 2 + core) * SHARD, SHARD
        if sub is not None:
            start, n = start + sub * (SHARD // 2), SHARD // 2
        return self.p.at[pl.ds(pl.multiple_of(start, SHARD // 2), n), :]

    def landed(self, k):
        return self.buf.at[pl.ds(pl.multiple_of(self.to(k) * SHARD, SHARD), SHARD), :]

    def q1(self, i):
        start = 4 * SHARD + i * (SHARD // 2)
        return self.buf.at[start : start + SHARD // 2, :]

    def q2(self, i):
        start = (5 + i) * SHARD
        return self.buf.at[start : start + SHARD, :]

    def ready(self):
        for i, peer in enumerate(({"c": 1 - self.c}, {"y": self.to(-1)}, {"y": self.to(1)})):
            pl.semaphore_signal(self.credit.at[self.t, i], inc=1, device_id=peer, device_id_type=MESH)

    def pair(self, k):
        return pltpu.make_async_remote_copy(
            src_ref=self.rows(k, 1 - self.c),
            dst_ref=self.landed(k),
            send_sem=self.send.at[self.t, k % 4],
            recv_sem=self.recv.at[self.t, k % 4],
            device_id={"c": 1 - self.c},
            device_id_type=MESH,
        )

    def ring(self, src, dst, m, d):
        return pltpu.make_async_remote_copy(
            src_ref=src,
            dst_ref=dst,
            send_sem=self.send.at[self.t, m],
            recv_sem=self.recv.at[self.t, m],
            device_id={"y": self.to(d)},
            device_id_type=MESH,
        )

    def y1(self, d):
        i = 0 if d > 0 else 1
        return self.ring(self.rows(2, self.c, i), self.q1(i), 4 + i, d)

    def y2(self, d):
        i = 0 if d > 0 else 1
        return self.ring(self.rows(d, self.c), self.q2(i), 6 + i, d)

    def share(self, k):
        if k == 2:
            pl.semaphore_wait(self.credit.at[self.t, 0], 1)
        self.pair(k).start()

    def join(self, k):
        self.pair(k).wait_recv()
        mine = self.rows(k, self.c)
        mine[...] = mine[...] + self.landed(k)[...]

    def far(self):
        self.join(2)
        for d in (1, -1):
            pl.semaphore_wait(self.credit.at[self.t, 1 if d > 0 else 2], 1)
            self.y1(d).start()

    def near(self, d):
        i = 0 if d > 0 else 1
        self.join(d)
        self.y1(d).wait_recv()
        part = self.rows(d, self.c, i)
        part[...] = part[...] + self.q1(i)[...]
        self.y2(d).start()

    def finish(self):
        self.join(0)
        for d in (1, -1):
            self.y2(d).wait_recv()
        return (
            self.rows(0, self.c)[...].astype(F32) + self.q2(0)[...].astype(F32) + self.q2(1)[...].astype(F32)
        )

    def drain(self):
        for k in (0, 1, 2, -1):
            self.pair(k).wait_send()
        for d in (1, -1):
            self.y1(d).wait_send()
            self.y2(d).wait_send()


class GainSum:
    AXES = (("c", 2), ("x", 4), ("z", 4), ("y", 4))

    def __init__(self, rows, send, recv):
        self.rows, self.send, self.recv = rows, send, recv

    def copy(self, i, d, arriving):
        name, n = self.AXES[i]
        me = lax.axis_index(name)
        src = lax.rem(me + n - d, n) if arriving else me
        return pltpu.make_async_remote_copy(
            src_ref=self.rows.at[i, src],
            dst_ref=self.rows.at[i, src],
            send_sem=self.send.at[i, d],
            recv_sem=self.recv.at[i, d],
            device_id={name: lax.rem(me + d, n)},
            device_id_type=MESH,
        )

    def start(self, i, row):
        name, n = self.AXES[i]
        self.rows[i, lax.axis_index(name)] = row
        for d in range(1, n):
            self.copy(i, d, False).start()

    def end(self, i):
        n = self.AXES[i][1]
        for d in range(1, n):
            self.copy(i, d, True).wait_recv()
        row = self.rows[i, 0]
        for k in range(1, n):
            row = row + self.rows[i, k]
        return row

    def drain(self):
        for i, (_, n) in enumerate(self.AXES):
            for d in range(1, n):
                self.copy(i, d, False).wait_send()


def sublayer(
    later_in, earlier_in, cot_in, gate_w, up_w, down_w, gain, gate_sum, up_sum, down_sum,
    later_out, hidden_out, earlier_out, gate_new, up_new, down_new, gain_out,
    w, g, r, nl, ne, cot, nlt, net, cott, hl, dx, he, hb, xb, dn, lrow, crow, gacc, grows,
    in_sem, own_sem, wsend, wrecv, send, recv, tsend, trecv, gsend, grecv, credit, out_sem,
):
    tokens, width = nl.shape
    half = width // 2
    z, x, y, c_me = (lax.axis_index(n) for n in ALL)
    me = z * 4 + x
    own_rows = pl.ds(pl.multiple_of((y * 2 + c_me) * SHARD, SHARD), SHARD)
    mine = pl.ds(pl.multiple_of(me * SHARD, SHARD), SHARD)
    own = [
        pltpu.make_async_copy(
            ref.at[STARTS[c] : STARTS[c] + SIZES[c], :],
            w[c].at[k * SIZES[c] : (k + 1) * SIZES[c], mine],
            own_sem.at[c, k],
        )
        for c in range(N_CHUNK)
        for k, ref in enumerate((gate_w, up_w, down_w))
    ]
    pairs = [
        (later_in, nl), (earlier_in, ne), (cot_in, cot),
        (gate_sum, gate_new), (up_sum, up_new), (down_sum, down_new),
        (later_in.at[own_rows, :], lrow), (cot_in.at[own_rows, :], crow),
    ]
    ins = [pltpu.make_async_copy(a, b, in_sem.at[i]) for i, (a, b) in enumerate(pairs)]
    for copy in own:
        copy.start()
    for copy in ins[:3]:
        copy.start()
    across = [{n: lax.rem(lax.axis_index(n) + 2, 4)} for n in ("x", "z", "y")]
    greet(ring_peers(("x", "z", "y")) + [{"c": 1 - c_me}] + across)
    for copy in own:
        copy.wait()
    ring = Gather(w, wsend, wrecv)
    ring.t0(0)
    for copy in ins[3:]:
        copy.start()
    rs = Scatter(g, r, send, recv, (gate_new, up_new, down_new))
    later = TokenScatter(0, nl, nlt, credit, tsend, trecv)
    earlier = TokenScatter(1, ne, net, credit, tsend, trecv)
    total = GainSum(grows, gsend, grecv)

    gain_row = gain[...].astype(F32).reshape(1, width)

    def turn_block(turned, ref, i):
        rows = pl.ds(pl.multiple_of(i * 128, 128), 128)
        for j in (0, 1):
            at = pl.ds(pl.multiple_of(i * 128 + j * tokens, 128), 128)
            turned[:, at] = ref[rows, j * half : (j + 1) * half].T

    def tok(i):
        return pl.ds(pl.multiple_of(i * 256, 256), 256)

    def turned_cols(turned, i):
        return jnp.concatenate(
            [turned[:, pl.ds(pl.multiple_of(i * 256 + j * tokens, 256), 256)] for j in (0, 1)], axis=0
        )

    def norms(ref, first, last):
        @pl.loop(first, last)
        def _(i):
            rows = pl.ds(pl.multiple_of(i * 64, 64), 64)
            v = ref[rows, :].astype(F32)
            unit = v * lax.rsqrt(jnp.mean(v * v, axis=1, keepdims=True) + NORM_FLOOR)
            ref[rows, :] = (unit * gain_row).astype(BF)

    def turns(turned, ref, first, last):
        @pl.loop(first, last)
        def _(i):
            turn_block(turned, ref, i)

    blocks = tokens // 128

    def looped(item, c, first, count):
        @pl.loop(first, first + count)
        def _(i):
            item(c, i)

    def later_item(c, i):
        n = SIZES[c]
        pre = nn(w[c][: 2 * n, :], turned_cols(nlt, i))
        gate, up = pre[:n], pre[n:]
        hl[STARTS[c] : STARTS[c] + n, tok(i)] = (gate * jax.nn.sigmoid(gate) * up).astype(BF)

    def earlier_item(c, i):
        n = SIZES[c]
        pre = nn(w[c][: 2 * n, :], turned_cols(net, i))
        dh = 0.5 * nn(w[c][2 * n :, :], turned_cols(cott, i))
        gate, up = pre[:n], pre[n:]
        s = jax.nn.sigmoid(gate)
        act = gate * s
        he[:n, tok(i)] = (act * up).astype(BF)
        dx[c][:n, tok(i)] = (dh * up * s * (1.0 + gate * (1.0 - s))).astype(BF)
        dx[c][n:, tok(i)] = (dh * act).astype(BF)

    def grad_item(c, i):
        n = SIZES[c]
        for j in (0, 1):
            cols = pl.ds(pl.multiple_of(i * 512 + j * 256, 256), 256)
            both = nn(dx[c][...], ne[:, cols]).astype(BF)
            down = (0.5 * nn(he[:n, :], cot[:, cols])).astype(BF)
            for m in (0, 1):
                lanes = slice(m * SHARD, (m + 1) * SHARD)
                g[c][i, 2 * j + m, : 2 * n, :] = both[:, lanes]
                g[c][i, 2 * j + m, 2 * n :, :] = down[:, lanes]

    L = functools.partial(looped, later_item)
    E = functools.partial(looped, earlier_item)
    G = functools.partial(looped, grad_item)

    reload = pltpu.make_async_copy(earlier_in, cott, in_sem.at[8])
    hidden = pltpu.make_async_copy(hl, hidden_out, out_sem)

    def features(n):
        return pl.ds(pl.multiple_of(n * 512, 512), 512)

    def later_block(k):
        b = lax.rem(y + k + 4, 4)
        hb[...] = hl[:, tok(b)].T

        @pl.loop(0, width // 512)
        def _(n):
            f = features(n)
            rows = [w[c][2 * SIZES[c] :, f] for c in range(N_CHUNK)]
            nl[tok(b), f] = nn(hb[...], jnp.concatenate(rows, axis=0)).astype(BF)

        later.share(k)

    def earlier_block(k):
        b = lax.rem(y + k + 4, 4)
        for c in range(N_CHUNK):
            xb[:, 2 * STARTS[c] : 2 * (STARTS[c] + SIZES[c])] = dx[c][:, tok(b)].T

        @pl.loop(0, width // 512)
        def _(n):
            f = features(n)
            rows = [w[c][: 2 * SIZES[c], f] for c in range(N_CHUNK)]
            dn[:, f] = nn(xb[...], jnp.concatenate(rows, axis=0))

        @pl.loop(0, 16)
        def _(i):
            at = pl.ds(pl.multiple_of(b * 256 + i * 16, 16), 16)
            v = cott[at, :].astype(F32)
            scale = lax.rsqrt(jnp.mean(v * v, axis=1, keepdims=True) + NORM_FLOOR)
            unit = v * scale
            d = dn[pl.ds(pl.multiple_of(i * 16, 16), 16), :]
            terms = d * unit
            gacc[...] += terms[:8] + terms[8:]
            mean = jnp.mean(terms * gain_row, axis=1, keepdims=True)
            ne[at, :] = (scale * (d * gain_row - unit * mean)).astype(BF)

        earlier.share(k)

    def gain_step(i):
        row = total.end(i - 1) if i else jnp.sum(gacc[...], axis=0, keepdims=True)
        if i < 4:
            total.start(i, row)
        else:
            gain_out[...] = row

    def later_end():
        later_out[...] = (lrow[...].astype(F32) + 0.5 * later.finish()).astype(BF)

    def earlier_end():
        earlier_out[...] = (crow[...].astype(F32) + earlier.finish()).astype(BF)

    gacc[...] = jnp.zeros_like(gacc)
    ins[0].wait()
    norms(nl, 0, blocks)
    ins[1].wait()
    norms(ne, 0, blocks)
    norms(ne, blocks, 2 * blocks)
    ring.t1(0,0,1)
    ring.t1(0,0,-1)
    ring.t1(0,1,1)
    ring.t1(0,1,-1)
    turns(net, ne, 0, blocks // 2)
    ring.hand(0,0,0,1)
    ring.hand(0,0,0,-1)
    ring.hand(0,1,0,1)
    ring.hand(0,1,0,-1)
    turns(net, ne, blocks // 2, blocks)
    ring.t3(0,0)
    norms(nl, blocks, 2 * blocks)
    ring.hand(0,0,-1,1)
    ring.hand(0,0,-1,-1)
    ring.hand(0,1,-1,1)
    ring.hand(0,1,-1,-1)
    turns(nlt, nl, 0, blocks // 2)
    ring.t3(0,1)
    ring.t0(1)
    ring.hand(0,0,1,1)
    ring.hand(0,0,1,-1)
    ring.hand(0,1,1,1)
    ring.hand(0,1,1,-1)
    turns(nlt, nl, blocks // 2, blocks)
    ins[2].wait()
    turns(cott, cot, 0, blocks // 2)
    ring.hand(0,0,2,1)
    ring.hand(0,0,2,-1)
    turns(cott, cot, blocks // 2, blocks)
    ring.hand(0,1,2,1)
    ring.hand(0,1,2,-1)
    ring.t1(1,1,-1)
    ring.t1(1,1,1)
    ring.t1(1,0,-1)
    ring.t1(1,0,1)
    ring.hand(1,0,0,-1)
    ring.hand(1,0,0,1)
    ring.hand(1,1,0,-1)
    ring.hand(1,1,0,1)
    ring.t6(0)
    E(0, 3, 1)
    ring.t3(1,1)
    E(0, 1, 1)
    L(0, 0, 1)
    ring.hand(1,1,1,1)
    ring.hand(1,1,1,-1)
    E(0, 0, 1)
    ring.hand(1,0,1,1)
    ring.hand(1,0,1,-1)
    E(0, 2, 1)
    ring.hand(1,1,-1,1)
    ring.hand(1,1,-1,-1)
    L(0, 2, 1)
    ring.hand(1,0,-1,1)
    ring.hand(1,0,-1,-1)
    G(0, 2, 1)
    ring.t3(1,0)
    ring.t0(2)
    G(0, 0, 1)
    G(0, 3, 1)
    G(0, 1, 1)
    ring.hand(1,1,2,1)
    ring.hand(1,1,2,-1)
    L(0, 3, 1)
    L(0, 1, 1)
    ring.hand(1,0,2,1)
    ring.hand(1,0,2,-1)
    ring.t1(2,1,1)
    ring.t1(2,1,-1)
    ring.t1(2,0,-1)
    ring.t1(2,0,1)
    ring.hand(2,0,0,1)
    ring.hand(2,0,0,-1)
    ring.hand(2,1,0,-1)
    ring.hand(2,1,0,1)
    for copy in ins[3:]:
        copy.wait()
    ring.t6(1)
    E(1, 2, 1)
    ring.t3(2,1)
    ring.hand(2,1,-1,1)
    ring.hand(2,1,-1,-1)
    L(1, 0, 1)
    ring.hand(2,0,1,1)
    ring.hand(2,0,1,-1)
    ring.hand(2,1,1,1)
    ring.hand(2,1,1,-1)
    E(1, 1, 1)
    ring.t3(2,0)
    ring.hand(2,0,-1,1)
    ring.hand(2,0,-1,-1)
    rs.s1(0)
    L(1, 1, 2)
    ring.hand(2,1,2,1)
    ring.hand(2,1,2,-1)
    L(1, 3, 1)
    E(1, 3, 1)
    ring.hand(2,0,2,1)
    ring.hand(2,0,2,-1)
    E(1, 0, 1)
    G(1, 2, 1)
    rs.a1(0,0,1)
    rs.a1(0,0,-1)
    G(1, 3, 1)
    ring.t6(2)
    rs.a1(0,1,1)
    rs.a1(0,1,-1)
    L(2, 3, 1)
    L(2, 0, 1)
    L(2, 2, 1)
    L(2, 1, 1)
    later.ready()
    hidden.start()
    G(1, 0, 1)
    later_block(2)
    later_block(1)
    later_block(-1)
    later.far()
    G(1, 1, 1)
    rs.s1(1)
    E(2, 1, 2)
    rs.a2(0,0)
    E(2, 3, 1)
    E(2, 0, 1)
    rs.a2(0,1)
    earlier.ready()
    reload.start()
    G(2, 1, 1)
    G(2, 3, 1)
    G(2, 2, 1)
    G(2, 0, 1)
    later.near(1)
    later.near(-1)
    rs.s1(2)
    reload.wait()
    earlier_block(2)
    rs.a3(0,0,1)
    rs.a3(0,0,-1)
    rs.a3(0,1,1)
    rs.a3(0,1,-1)
    rs.a1(1,0,1)
    rs.a1(1,0,-1)
    rs.a1(1,1,1)
    rs.a1(1,1,-1)
    earlier.far()
    rs.a1(2,0,1)
    rs.a1(2,0,-1)
    rs.a1(2,1,1)
    rs.a1(2,1,-1)
    earlier_block(1)
    rs.a4(0,0)
    rs.a4(0,1)
    earlier_block(-1)
    earlier_block(0)
    earlier.near(1)
    earlier.near(-1)
    gain_step(0)
    rs.a2(1,0)
    gain_step(1)
    rs.a2(1,1)
    rs.a2(2,1)
    rs.a2(2,0)
    later_block(0)
    gain_step(2)
    rs.a3(1,0,1)
    rs.a3(1,0,-1)
    rs.a3(1,1,-1)
    rs.a3(1,1,1)
    rs.a3(2,1,-1)
    rs.a3(2,1,1)
    rs.a3(2,0,-1)
    rs.a3(2,0,1)
    later_end()
    gain_step(3)
    rs.a4(1,0)
    rs.a4(1,1)
    rs.a4(2,0)
    rs.a4(2,1)
    earlier_end()
    gain_step(4)
    for c in range(N_CHUNK):
        ring.drain(c)
        rs.drain(c)
    later.drain()
    earlier.drain()
    total.drain()
    hidden.wait()


def run(later_in, earlier_in, cot, gate_w, up_w, down_w, gain, gate_sum, up_sum, down_sum):
    tokens, width = later_in.shape
    cols, rows = gate_w.shape
    any_ = pl.BlockSpec(memory_space=pl.ANY)
    vm = pl.BlockSpec(memory_space=pltpu.VMEM)
    tok = (tokens, width)
    dma = pltpu.SemaphoreType.DMA
    return pl.pallas_call(
        sublayer,
        out_shape=[
            jax.ShapeDtypeStruct((tokens // 8, width), BF),
            jax.ShapeDtypeStruct((cols, tokens), BF),
            jax.ShapeDtypeStruct((tokens // 8, width), BF),
            jax.ShapeDtypeStruct((cols, rows), F32),
            jax.ShapeDtypeStruct((cols, rows), F32),
            jax.ShapeDtypeStruct((cols, rows), F32),
            jax.ShapeDtypeStruct((1, width), F32),
        ],
        in_specs=[any_] * 6 + [vm] + [any_] * 3,
        out_specs=[vm, any_] + [vm] * 5,
        scratch_shapes=[
            [pltpu.VMEM((3 * n, width), BF) for n in SIZES],
            [pltpu.VMEM((4, 4, 3 * n, SHARD), BF) for n in SIZES],
            [
                [
                    pltpu.VMEM((2, 2, 4, half_of(c) // 2, SHARD), BF),
                    pltpu.VMEM((2, 2, 4, half_of(c), SHARD), BF),
                    pltpu.VMEM((2, 2, half_of(c) // 2, SHARD), BF),
                    pltpu.VMEM((2, 2, half_of(c), SHARD), BF),
                ]
                for c in range(N_CHUNK)
            ],
            *[pltpu.VMEM(tok, BF)] * 6,
            pltpu.VMEM((cols, tokens), BF),
            [pltpu.VMEM((2 * n, tokens), BF) for n in SIZES],
            pltpu.VMEM((max(SIZES), tokens), BF),
            pltpu.VMEM((256, cols), BF),
            pltpu.VMEM((256, 2 * cols), BF),
            pltpu.VMEM((256, width), F32),
            pltpu.VMEM((SHARD, width), BF),
            pltpu.VMEM((SHARD, width), BF),
            pltpu.VMEM((8, width), F32),
            pltpu.VMEM((4, 4, 1, width), F32),
            dma((9,)),
            dma((N_CHUNK, 3)),
            dma((N_CHUNK, 2, 20)),
            dma((N_CHUNK, 2, 20)),
            dma((N_CHUNK, 2, 8)),
            dma((N_CHUNK, 2, 8)),
            dma((2, 8)),
            dma((2, 8)),
            dma((4, 4)),
            dma((4, 4)),
            pltpu.SemaphoreType.REGULAR((2, 3)),
            dma,
        ],
        compiler_params=pltpu.CompilerParams(
            collective_id=0, has_side_effects=True, vmem_limit_bytes=64 * 1024 * 1024 - 65536
        ),
        name="sublayer",
    )(later_in, earlier_in, cot, gate_w, up_w, down_w, gain, gate_sum, up_sum, down_sum)


def deliver_body(*refs):
    n = (len(refs) - 5) // 3
    srcs, (gain_sum, gain_total) = refs[:n], refs[n : n + 2]
    outs, gain_new = refs[n + 2 : 2 * n + 2], refs[2 * n + 2]
    bufs = refs[2 * n + 3 : 3 * n + 3]
    in_sem, out_sem = refs[-2:]
    ins = [pltpu.make_async_copy(a, b, in_sem.at[i]) for i, (a, b) in enumerate(zip(srcs, bufs))]
    for copy in ins:
        copy.start()
    puts = [pltpu.make_async_copy(a, b, out_sem.at[i]) for i, (a, b) in enumerate(zip(bufs, outs))]
    gain_new[...] = gain_sum[...] + gain_total[...].reshape(gain_sum.shape)
    for copy, put in zip(ins, puts):
        copy.wait()
        put.start()
    for put in puts:
        put.wait()


def deliver(arrays, gain_sum, gain_total):
    any_ = pl.BlockSpec(memory_space=pl.ANY)
    vm = pl.BlockSpec(memory_space=pltpu.VMEM)
    n = len(arrays)
    return pl.pallas_call(
        deliver_body,
        out_shape=[jax.ShapeDtypeStruct(a.shape, a.dtype) for a in (*arrays, gain_sum)],
        in_specs=[any_] * n + [vm] * 2,
        out_specs=[any_] * n + [vm],
        scratch_shapes=[pltpu.VMEM(a.shape, a.dtype) for a in arrays]
        + [pltpu.SemaphoreType.DMA((n,)), pltpu.SemaphoreType.DMA((n,))],
        compiler_params=pltpu.CompilerParams(vmem_limit_bytes=64 * 1024 * 1024 - 65536),
        name="deliver",
    )(*arrays, gain_sum, gain_total)


def local(later_in, earlier_in, cot, gate_w, up_w, down_w, gain, gate_sum, up_sum, down_sum, gain_sum):
    *parts, gain_total = run(
        later_in, earlier_in, cot, gate_w.T, up_w.T, down_w.T, gain, gate_sum.T, up_sum.T, down_sum.T
    )
    later_out, hidden, earlier_grad, gate_new, up_new, down_new, gain_new = deliver(
        parts, gain_sum, gain_total
    )
    return (
        later_out, hidden.T, earlier_grad,
        gate_new.T, up_new.T, down_new.T, gain_new,
    )


def solution(mesh):
    torus = Mesh(mesh.devices.reshape(4, 4, 4, 2), ALL)
    return jax.shard_map(
        local,
        mesh=torus,
        in_specs=(P(FS, None),) * 3 + (P(FS, TP),) * 3 + (P(),) + (P(FS, TP),) * 3 + (P(),),
        out_specs=(P(ALL, None), P(FS, TP), P(ALL, None), P(FS, TP), P(FS, TP), P(FS, TP), P()),
        check_vma=False,
    )
```
